32 devices in a mesh: rep: 2 (over x), fs: 8 (over z, y), tp: 2 (over core).
Axes of the slice: x: 2, y: 2, z: 4, core: 2. Of those that a mesh axis runs over, the one named last changes fastest.
Arguments:
- stream: bfloat16 [4096, 2048], P(('rep', 'fs'), 'tp'), may hold values from -6 to 6
- norm_gains: float32 [6, 2048], replicated, may hold values from 0.1 to 1.9
- w_gate: bfloat16 [2048, 5632], P('fs', 'tp'), may hold values from -0.125 to 0.125
- w_up: bfloat16 [2048, 5632], P('fs', 'tp'), may hold values from -0.125 to 0.125
- w_down: bfloat16 [5632, 2048], P('tp', 'fs'), may hold values from -0.109375 to 0.109375
- w_inner: bfloat16 [2048, 1024], P('fs', 'tp'), may hold values from -0.125 to 0.125
- w_bgate: bfloat16 [2048, 1024], P('fs', 'tp'), may hold values from -0.125 to 0.125
- w_cgate: bfloat16 [2048, 1024], P('fs', 'tp'), may hold values from -0.125 to 0.125
- conv_taps: float32 [3, 1024], P(None, 'tp'), may hold values from -3.5 to 3.5
- w_out: bfloat16 [1024, 2048], P('tp', 'fs'), may hold values from -0.25 to 0.25
Outputs:
- mixed: bfloat16 [4096, 2048], P(('rep', 'fs'), 'tp')
The draws below stay inside these ranges and needn't reach their ends.
All inputs are finite; a program needn't handle non-finite values.
Results may differ from the reference program's by a relative error of at most 0.02.
Values may be sent and summed in bfloat16 or wider, within the bound.
A program may use at most 128 MiB of HBM per device.

```python
import jax
import jax.numpy as jnp
from jax import lax

D = 2048
FF = 5632
CW = 1024
TAPS = 3
SEQ_LEN = 2048
TOKENS = 4096
N_TP = 2


def strengthened(values, rng, source, target, shards_of, factor):
    def block_of(position):
        return (jnp.arange(values.shape[position]) // (values.shape[position] // shards_of)).reshape((-1,) + (1,) * (values.ndim - 1 - position))

    one_side = jax.random.permutation(rng, shards_of)[block_of(target)]
    second = (block_of(target) + shards_of // 2) % shards_of
    return jnp.where((block_of(source) == one_side) | (block_of(source) == second), factor * values, values)


def levels(key, extent, pieces, least, largest):
    level, own = 1.0, jax.random.fold_in(key, 6)
    for dim, blocks in pieces:
        draws = jnp.exp(jax.random.uniform(jax.random.fold_in(own, dim), (blocks,), jnp.float32, least / len(pieces), largest / len(pieces)))
        level = level * jnp.repeat(draws, extent[dim] // blocks).reshape([-1 if axis == dim else 1 for axis in range(len(extent))])
    return level


def normal_values(rng, dims, width, limit, cuts=(), held_as=jnp.bfloat16):
    array = jax.random.normal(rng, dims, jnp.float32) * width
    if len(cuts) > 0:
        array = levels(rng, dims, cuts, -0.22, 0.18) * array
    return jnp.clip(array, min=-limit, max=limit).astype(held_as)


def noise_with(rng, extent, deviation, most, shards, heavy, dtype=jnp.bfloat16):
    values = deviation * jax.random.normal(rng, extent, jnp.float32)
    if shards:
        values = values * levels(rng, extent, shards, -0.22, 0.18)
    return jnp.clip(strengthened(values, jax.random.fold_in(rng, 3), *heavy), -most, most).astype(dtype)


def setup_inputs(seed: int = 0) -> dict:
    key_list = jax.random.split(jax.random.key(seed), 11)
    return {
        "stream": normal_values(key_list[0], (TOKENS, D), 1.0, 6.0, ((0, 16), (1, 2))),
        "norm_gains": jnp.clip(1.0 + 0.18 * jax.random.normal(key_list[1], (6, D), jnp.float32), 0.1, 1.9),
        "w_gate": normal_values(key_list[2], (D, FF), D ** -0.5, 0.125, ((0, 8), (1, 2))),
        "w_up": normal_values(key_list[3], (D, FF), D ** -0.5, 0.125, ((0, 8), (1, 2))),
        "w_down": noise_with(key_list[4], (FF, D), FF ** -0.5, 0.109375, ((0, 2), (1, 8)), (0, 1, 8, 2.0)),
        "w_inner": normal_values(key_list[5], (D, CW), D ** -0.5, 0.125, ((0, 8), (1, 2))),
        "w_bgate": normal_values(key_list[6], (D, CW), D ** -0.5, 0.125, ((0, 8), (1, 2))),
        "w_cgate": normal_values(key_list[7], (D, CW), D ** -0.5, 0.125, ((0, 8), (1, 2))),
        "conv_taps": normal_values(key_list[8], (TAPS, CW), TAPS ** -0.5, 3.5, ((1, 2),), jnp.float32),
        "w_out": noise_with(key_list[9], (CW, D), CW ** -0.5, 0.25, ((0, 2), (1, 8)), (0, 1, 8, 2.0)),
    }


EPSILON = 1e-06

def rms_scale(values):
    return values * lax.rsqrt(lax.optimization_barrier(jnp.mean(values * values, axis=1, keepdims=True)) + EPSILON)

def norm_input(current, gain):
    return (rms_scale(current.astype(jnp.float32)) * gain).astype(jnp.bfloat16)

def split_sum(hidden, weight, groups):
    columns = hidden.shape[1] // groups
    result = jnp.zeros((hidden.shape[0], weight.shape[1]), jnp.float32)
    for group in range(groups):
        partial_term = jnp.dot(hidden[:, group * columns:(group + 1) * columns], weight[group * columns:(group + 1) * columns], preferred_element_type=jnp.float32)
        rounded = lax.optimization_barrier(partial_term.astype(jnp.bfloat16))
        result = result + rounded.astype(jnp.float32)
    return result

def settle(current, branch_sum, gain, weight):
    return (current.astype(jnp.float32) + weight * (rms_scale(branch_sum) * gain)).astype(jnp.bfloat16)

def feed_forward(current, gain_in, gain_out, w_gate, w_up, w_down):
    normed = norm_input(current, gain_in)
    gate_vals = jnp.dot(normed, w_gate, preferred_element_type=jnp.float32)
    upward = jnp.dot(normed, w_up, preferred_element_type=jnp.float32)
    hidden = (jax.nn.silu(gate_vals) * upward).astype(jnp.bfloat16)
    return settle(current, split_sum(hidden, w_down, N_TP), gain_out, 0.5)

def reference(stream, norm_gains, w_gate, w_up, w_down, w_inner, w_bgate, w_cgate, conv_taps, w_out):
    first = feed_forward(stream, norm_gains[0], norm_gains[1], w_gate, w_up, w_down)
    normed = norm_input(first, norm_gains[2])
    inner = jnp.dot(normed, w_inner, preferred_element_type=jnp.float32)
    bgate = jnp.dot(normed, w_bgate, preferred_element_type=jnp.float32)
    cgate = jnp.dot(normed, w_cgate, preferred_element_type=jnp.float32)
    conv_input = (cgate * inner).reshape(-1, SEQ_LEN, CW)
    padded = jnp.pad(conv_input, ((0, 0), (TAPS - 1, 0), (0, 0)))
    conv = conv_taps[0] * padded[:, 0:SEQ_LEN]
    for tap in range(1, TAPS):
        conv = conv + conv_taps[tap] * padded[:, tap:tap + SEQ_LEN]
    gated = (bgate * conv.reshape(-1, CW)).astype(jnp.bfloat16)
    second = settle(first, split_sum(gated, w_out, N_TP), norm_gains[3], 1.0)
    return feed_forward(second, norm_gains[4], norm_gains[5], w_gate, w_up, w_down)
```

```python
import functools

import jax
import jax.numpy as jnp
from jax import lax
from jax.experimental import pallas as pl
from jax.experimental.pallas import tpu as pltpu
from jax.sharding import PartitionSpec as P

TAPS = 3
EPSILON = 1e-06


def ring_order(count):
    return list(range(0, count, 2)) + list(range(1, count, 2))[::-1]


def swap(x, axis):
    return lax.ppermute(x, axis, [(0, 1), (1, 0)])


def copy_blocks(count, size, starts, source, target):
    for i in range(count):
        begin = pl.multiple_of(starts[i] * size, size)
        target[:, i * size : (i + 1) * size] = source[:, pl.ds(begin, size)]


def permuted(x, starts, size):
    return pl.pallas_call(
        functools.partial(copy_blocks, len(starts), size),
        in_specs=[
            pl.BlockSpec(memory_space=pltpu.SMEM),
            pl.BlockSpec(memory_space=pltpu.VMEM),
        ],
        out_specs=pl.BlockSpec(memory_space=pltpu.VMEM),
        out_shape=jax.ShapeDtypeStruct(x.shape, x.dtype),
        cost_estimate=pl.CostEstimate(flops=0, bytes_accessed=2 * x.size * x.dtype.itemsize, transcendentals=0),
        compiler_params=pltpu.CompilerParams(vmem_limit_bytes=3 * x.size * x.dtype.itemsize),
    )(jnp.stack(starts), x)


class Ring:
    def __init__(self, own, after=None):
        count = lax.axis_size("fs")
        order = ring_order(count)
        onward = [(order[i], order[(i + 1) % count]) for i in range(count)]
        back = [(b, a) for a, b in onward]
        half = count // 2
        first, second = own, own
        if after is not None:
            first, _ = lax.optimization_barrier((own, after[0]))
            second, _ = lax.optimization_barrier((own, after[1]))
        rows = own.shape[0] // 2
        self.shards = {0: own}
        self.arrived = self.early = (own, own)
        for step in range(1, half):
            first = lax.ppermute(first, "fs", onward)
            second = lax.ppermute(second, "fs", back)
            self.shards[step] = first
            self.shards[count - step] = second
            self.arrived = (first, second)
            if step == 1:
                self.early = self.arrived
        self.last = (
            lax.ppermute(first[:rows], "fs", onward),
            lax.ppermute(second[rows:], "fs", back),
        )
        self.shards[half] = jnp.concatenate(self.last, axis=0)
        self.sequence = [0]
        for step in range(1, half):
            self.sequence += [step, count - step]
        self.sequence += [half]

    def lined_up(self, axis):
        return jnp.concatenate([self.shards[d] for d in range(len(self.shards))], axis=axis)


def shards(stream, norm_gains, w_gate, w_up, w_down, w_inner, w_bgate, w_cgate, conv_taps, w_out):
    count, tp = lax.axis_size("fs"), lax.axis_size("tp")
    tp_index, rep_index, fs_index = lax.axis_index("tp"), lax.axis_index("rep"), lax.axis_index("fs")
    rows, width = stream.shape
    model_width = width * tp
    order = ring_order(count)
    places = [order.index(i) for i in range(count)]
    place = jnp.array(places, jnp.int32)[fs_index]
    origin = [
        jnp.array(order, jnp.int32)[lax.rem(place - d + count, count)] for d in range(count)
    ]

    behind = [
        lax.rem(place - places[i] + count, count) for i in range(count)
    ]

    def blocks(x, starts):
        size = x.shape[1] // count
        if size % 128 == 0:
            return permuted(x, starts, size)
        return jnp.concatenate(
            [lax.dynamic_slice_in_dim(x, start * size, size, 1) for start in starts], axis=1
        )

    def rep_part(w, axis):
        size = w.shape[axis] // lax.axis_size("rep")
        return lax.dynamic_slice_in_dim(w, rep_index * size, size, axis)

    def whole_features(x):
        if tp != 2:
            return lax.all_gather(x, "tp", axis=1, tiled=True)
        other = swap(x, "tp")
        mine = tp_index == 0
        return jnp.concatenate([jnp.where(mine, x, other), jnp.where(mine, other, x)], axis=1)

    def own_features(x):
        return lax.dynamic_slice_in_dim(x, tp_index * width, width, 1)

    def feature_sum(partials):
        rounded = blocks(partials.astype(jnp.bfloat16), behind)
        if tp != 2:
            return lax.psum_scatter(rounded, "tp", scatter_dimension=1, tiled=True).astype(jnp.float32)
        theirs = lax.dynamic_slice_in_dim(rounded, (1 - tp_index) * width, width, 1)
        received = swap(theirs, "tp").astype(jnp.float32)
        return own_features(rounded).astype(jnp.float32) + received

    def norm_own(current, row):
        values = current.astype(jnp.float32)
        scaled = values * lax.rsqrt(jnp.mean(values * values, axis=1, keepdims=True) + EPSILON)
        return (scaled * norm_gains[row]).astype(jnp.bfloat16)

    def norm_other(normed):
        return whole_features(swap(own_features(normed), "rep"))

    def settle(current, own_sum, other_sum, row, weight):
        received = swap(other_sum.astype(jnp.bfloat16), "rep").astype(jnp.float32)
        branch = whole_features(own_sum + received)
        scaled = branch * lax.rsqrt(jnp.mean(branch * branch, axis=1, keepdims=True) + EPSILON)
        return (current.astype(jnp.float32) + weight * (scaled * norm_gains[row])).astype(
            jnp.bfloat16
        )

    def dot(a, b):
        return jnp.dot(a, b, preferred_element_type=jnp.float32)

    def activate(gate_vals, upward):
        return (jax.nn.silu(gate_vals) * upward).astype(jnp.bfloat16)

    current = whole_features(stream)
    normed = norm_own(current, 0)
    normed = jnp.concatenate([normed, norm_other(normed)], axis=0)

    gate_ring = Ring(rep_part(w_gate, 1))
    up_ring = Ring(rep_part(w_up, 1))
    down_own = rep_part(w_down, 0)
    down_ring = Ring(down_own, gate_ring.arrived)
    mix_own = jnp.concatenate([rep_part(w, 1) for w in (w_inner, w_bgate, w_cgate)], axis=1)
    out_own = rep_part(w_out, 0)
    mix_width = mix_own.shape[1]
    mix_ring = Ring(
        jnp.concatenate([mix_own, out_own.reshape(mix_own.shape[0], -1)], axis=1), down_ring.early
    )

    def by_shards(ring):
        size = ring.shards[0].shape[0]
        total = None
        for d in ring.sequence:
            term = dot(lax.dynamic_slice_in_dim(normed, origin[d] * size, size, 1), ring.shards[d])
            total = term if total is None else total + term
        return total

    hidden = activate(by_shards(gate_ring), by_shards(up_ring))
    down_blocks = {d: dot(hidden, down_ring.shards[d]).astype(jnp.bfloat16) for d in down_ring.sequence}
    sums = feature_sum(jnp.concatenate([down_blocks[d] for d in range(count)], axis=1))
    first = settle(current, sums[:rows], sums[rows:], 1, 0.5)

    mix_whole = mix_ring.lined_up(0)[:, :mix_width]
    out_whole = jnp.concatenate(
        [mix_ring.shards[d][:, mix_width:].reshape(out_own.shape) for d in range(count)], axis=1
    )
    channels = mix_width // 3
    taps = rep_part(conv_taps, 1)

    def mix_in(normed_mix):
        product = dot(blocks(normed_mix, origin), mix_whole)
        inner, bgate, cgate = (product[:, i * channels : (i + 1) * channels] for i in range(3))
        return cgate * inner, bgate

    def mix_out(conv_input, bgate, earlier):
        padded = jnp.concatenate([earlier, conv_input], axis=0)
        conv = taps[0] * padded[0:rows]
        for tap in range(1, TAPS):
            conv = conv + taps[tap] * padded[tap : tap + rows]
        return feature_sum(dot((bgate * conv).astype(jnp.bfloat16), out_whole))

    normed_mix = norm_own(first, 2)
    other_mix = norm_other(normed_mix)
    own_in, own_bgate = mix_in(normed_mix)
    other_in, other_bgate = mix_in(other_mix)
    tails = jnp.concatenate([own_in[rows - (TAPS - 1) :], other_in[rows - (TAPS - 1) :]], axis=0)
    earlier = lax.ppermute(tails, "fs", [(i, i + 1) for i in range(count - 1)])
    other_sum = mix_out(other_in, other_bgate, earlier[TAPS - 1 :])
    own_sum = mix_out(own_in, own_bgate, earlier[: TAPS - 1])
    second = settle(first, own_sum, other_sum, 3, 1.0)

    gate_whole, up_whole = gate_ring.lined_up(0), up_ring.lined_up(0)
    down_whole = down_ring.lined_up(1)

    def units(normed_rows):
        lined = blocks(normed_rows, origin)
        return activate(dot(lined, gate_whole), dot(lined, up_whole))

    normed = norm_own(second, 4)
    other_normed = norm_other(normed)
    own_units = units(normed)
    other_sum = feature_sum(dot(units(other_normed), down_whole))
    own_sum = feature_sum(dot(own_units, down_whole))
    return own_features(settle(second, own_sum, other_sum, 5, 0.5))


MESH = pl.DeviceIdType.MESH
GATE, UP, DOWN, MIX = range(4)
Z, X, Y, PART_A, PART_B = range(5)


def aligned(value, to):
    return pl.multiple_of(value, to)


def layer_kernel(
    planes,
    stream, gains, w_gate, w_up, w_down, w_mix, taps, out,
    gate_buf, up_buf, down_buf, mix_buf, raw, normed, hidden, partials, from_core, summed,
    from_pair, current, conv_in, bgates, gated, result, other_half,
    local_sem, piece_send, piece_recv, raw_send, raw_recv, core_send, core_recv,
    pair_send, pair_recv, gather_send, gather_recv, halo_send, halo_recv, out_send, out_recv,
):
    x, place, core = lax.axis_index("rep"), lax.axis_index("fs"), lax.axis_index("tp")
    z, y = place // 2, place % 2
    pair, member = z // 2, z % 2
    pairs = planes // 2
    rows, width = stream.shape
    own_rows = rows // 2
    model_width = 2 * width
    units, channels, mix_width = gate_buf.shape[1], gated.shape[1], mix_buf.shape[1]
    out_cols = mix_width - 3 * channels
    weight_rows = w_gate.shape[0]
    down_cols = w_down.shape[1]
    plane_cols = 2 * down_cols
    buffers = (gate_buf, up_buf, down_buf, mix_buf)
    halves = (weight_rows // 2, weight_rows // 2, units // 2, weight_rows // 2)

    def device(to_x, to_z, to_y, to_core):
        return (to_x, to_z * 2 + to_y, to_core)

    order = [2 * ((pair + j // 2) % pairs) + (member + j) % 2 for j in range(planes)]
    partner = order[1]
    core_peer = device(x, z, y, 1 - core)
    pair_peer = device(x, partner, y, core)
    x_peer, y_peer = device(1 - x, z, y, core), device(x, z, 1 - y, core)

    pending = []

    def send(source, target, send_sem, recv_sem, to):
        copy = pltpu.make_async_remote_copy(
            src_ref=source, dst_ref=target, send_sem=send_sem, recv_sem=recv_sem,
            device_id=to, device_id_type=MESH,
        )
        copy.start()
        pending.append(copy)

    def arrive(target, send_sem, recv_sem):
        pltpu.make_async_remote_copy(
            src_ref=target, dst_ref=target, send_sem=send_sem, recv_sem=recv_sem,
            device_id=core_peer, device_id_type=MESH,
        ).wait_recv()

    def piece(kind, of_z, of_y, of_x, part=None):
        half = halves[kind]
        count, offset = (half, 0) if part is None else (half // 2, part * (half // 2))
        if kind == DOWN:
            return down_buf.at[of_z * 2 + of_y, pl.ds(aligned(of_x * half + offset, 16), count), :]
        start = ((of_z * 2 + of_y) * 2 + of_x) * half + offset
        return buffers[kind].at[pl.ds(aligned(start, 16), count), :]

    def own_source(kind, side, start, count):
        if kind == DOWN:
            return w_down.at[pl.ds(aligned(side * units + start, 16), count), :]
        cols = mix_width if kind == MIX else units
        source = (w_gate, w_up, None, w_mix)[kind]
        return source.at[pl.ds(aligned(start, 16), count), pl.ds(aligned(side * cols, 128), cols)]

    def piece_copy(source, kind, route, of_z, of_y, of_x, to, part=None, index=None, recv_index=None):
        index = of_z if index is None else index
        send(
            source, piece(kind, of_z, of_y, of_x, part),
            piece_send.at[kind, route, index], piece_recv.at[kind, route, of_z], to,
        )

    def wait_piece(kind, route, of_z, of_y, of_x, part=None):
        arrive(
            piece(kind, of_z, of_y, of_x, part),
            piece_send.at[kind, route, of_z], piece_recv.at[kind, route, of_z],
        )

    def send_planes(kind, j):
        to = order[j]
        piece_copy(
            own_source(kind, to % 2, x * halves[kind], halves[kind]),
            kind, Z, z, y, x, device(x, to, y, core), index=to,
        )

    def send_own(kind):
        piece_copy(own_source(kind, member, x * halves[kind], halves[kind]), kind, Y, z, y, x, y_peer)

    def pass_own(kind):
        wait_piece(kind, Y, z, 1 - y, x)
        piece_copy(piece(kind, z, 1 - y, x), kind, X, z, 1 - y, x, x_peer)

    def spread(kind, j):
        of = order[j]
        wait_piece(kind, Z, of, y, x)
        piece_copy(piece(kind, of, y, x), kind, X, of, y, x, x_peer)
        piece_copy(piece(kind, of, y, x), kind, Y, of, y, x, y_peer)

    def relay(kind, j):
        of = order[j]
        wait_piece(kind, X, of, y, 1 - x)
        piece_copy(piece(kind, of, y, 1 - x, 0), kind, PART_A, of, y, 1 - x, y_peer, part=0)
        wait_piece(kind, Y, of, 1 - y, x)
        piece_copy(piece(kind, of, 1 - y, x, 1), kind, PART_B, of, 1 - y, x, x_peer, part=1)

    def local_copy(kind):
        count = units if kind == DOWN else weight_rows
        if kind == DOWN:
            target = down_buf.at[z * 2 + y]
        else:
            target = buffers[kind].at[pl.ds(aligned((z * 2 + y) * weight_rows, 16), count), :]
        return pltpu.make_async_copy(own_source(kind, member, 0, count), target, local_sem.at[kind])

    def complete(kind, j):
        if j == 0:
            local_copy(kind).wait()
            wait_piece(kind, X, z, 1 - y, 1 - x)
        else:
            wait_piece(kind, PART_A, order[j], 1 - y, 1 - x, 0)
            wait_piece(kind, PART_B, order[j], 1 - y, 1 - x, 1)

    barrier = pltpu.get_barrier_semaphore()
    greeted = [core_peer, x_peer, y_peer]
    greeted += [device(x, order[j], y, core) for j in range(1, planes)]
    greeted += [device(x, (z + s) % planes, 1 - y, core) for s in sorted({2, planes - 2})]
    for peer in greeted:
        pl.semaphore_signal(barrier, inc=1, device_id=peer, device_id_type=MESH)
    pl.semaphore_wait(barrier, len(greeted))

    for j in range(1, planes):
        send_planes(GATE, j)
    send_own(GATE)
    own_raw = raw.at[pl.ds(aligned(member * rows, 16), rows), pl.ds(aligned(core * width, 128), width)]
    send(stream, own_raw, raw_send.at[0], raw_recv.at[0], core_peer)
    send(stream, own_raw, raw_send.at[1], raw_recv.at[1], pair_peer)
    for kind in (UP, DOWN, MIX):
        for j in range(1, planes):
            send_planes(kind, j)
    send_own(UP)
    raw_copy = pltpu.make_async_copy(stream, own_raw, local_sem.at[4])
    raw_copy.start()
    for kind in range(4):
        local_copy(kind).start()

    def rms(values):
        return values * lax.rsqrt(jnp.mean(values * values, axis=1, keepdims=True) + EPSILON)

    step_rows = 16

    def norm_all():
        @pl.loop(0, 2 * rows // step_rows)
        def _(i):
            at = pl.ds(aligned(i * step_rows, 16), step_rows)
            values = raw[at, :].astype(jnp.float32)
            normed[0, at, :] = (rms(values) * gains[0:1, :]).astype(jnp.bfloat16)

    def dot(a, b):
        return jnp.dot(a, b, preferred_element_type=jnp.float32)

    tile = 256

    def hidden_rows(which, start):
        at = pl.ds(aligned(start, 128), rows)

        def columns(begin, count):
            cols = pl.ds(aligned(begin, 128), count)
            gate = dot(normed[which, at, :], gate_buf[:, cols])
            up = dot(normed[which, at, :], up_buf[:, cols])
            hidden[at, cols] = (gate / (1.0 + jnp.exp(-gate)) * up).astype(jnp.bfloat16)

        @pl.loop(0, units // tile)
        def _(n):
            columns(n * tile, tile)

        if units % tile:
            columns(units - units % tile, units % tile)

    def down_rows(phase, start, of_z):
        at = pl.ds(aligned(start, 128), rows)

        @pl.loop(0, 2)
        def _(s):
            cols = pl.ds(aligned((of_z * 2 + s) * down_cols, 128), down_cols)
            partials[phase, at, cols] = dot(hidden[at, :], down_buf[of_z * 2 + s]).astype(jnp.bfloat16)

    def block(of_member, of_core):
        return pl.ds(aligned((of_member * 2 + of_core) * own_rows, 16), own_rows)

    def plane_of(of_z):
        return pl.ds(aligned(of_z * plane_cols, 128), plane_cols)

    def send_core(phase, of_member, of_z):
        send(
            partials.at[phase, block(of_member, 1 - core), plane_of(of_z)],
            from_core.at[phase, of_member, :, plane_of(of_z)],
            core_send.at[phase, of_member, of_z], core_recv.at[phase, of_member, of_z], core_peer,
        )

    def wait_core(phase, of_member, of_z):
        arrive(
            from_core.at[phase, of_member, :, plane_of(of_z)],
            core_send.at[phase, of_member, of_z], core_recv.at[phase, of_member, of_z],
        )

    def send_pair(phase, of_z):
        wait_core(phase, 1 - member, of_z)
        cols = plane_of(of_z)
        mine = partials[phase, block(1 - member, core), cols].astype(jnp.float32)
        theirs = from_core[phase, 1 - member, :, cols].astype(jnp.float32)
        summed[phase, :, cols] = (mine + theirs).astype(jnp.bfloat16)
        send(
            summed.at[phase, :, cols], from_pair.at[phase, :, cols],
            pair_send.at[phase, of_z], pair_recv.at[phase, of_z], pair_peer,
        )

    def wait_pair(phase, j):
        of_z = order[j]
        wait_core(phase, member, of_z)
        arrive(
            from_pair.at[phase, :, plane_of(of_z)],
            pair_send.at[phase, of_z], pair_recv.at[phase, of_z],
        )

    def settle(phase, gain, weight, source, source_start, target, next_gain):
        @pl.loop(0, own_rows // step_rows)
        def _(i):
            at = pl.ds(aligned(i * step_rows, 16), step_rows)
            mine = pl.ds(
                aligned((member * 2 + core) * own_rows + i * step_rows, 16), step_rows
            )
            branch = (
                partials[phase, mine, :].astype(jnp.float32)
                + from_core[phase, member, at, :].astype(jnp.float32)
                + from_pair[phase, at, :].astype(jnp.float32)
            )
            before = source[pl.ds(aligned(source_start + i * step_rows, 16), step_rows), :]
            after = before.astype(jnp.float32) + weight * (rms(branch) * gains[gain : gain + 1, :])
            rounded = after.astype(jnp.bfloat16)
            target[at, :] = rounded
            if next_gain is not None:
                scaled = rms(rounded.astype(jnp.float32)) * gains[next_gain : next_gain + 1, :]
                normed[phase + 1, mine, :] = scaled.astype(jnp.bfloat16)

    def gather_ref(which, of_member, of_core):
        return normed.at[which, block(of_member, of_core), :]

    def gather_start(which):
        mine = gather_ref(which, member, core)
        send(mine, mine, gather_send.at[which, 1], gather_recv.at[which, 1], pair_peer)
        send(mine, mine, gather_send.at[which, 0], gather_recv.at[which, 0], core_peer)

    def gather_own(which):
        arrive(gather_ref(which, member, 1 - core), gather_send.at[which, 0], gather_recv.at[which, 0])

    def gather_pair(which):
        theirs = gather_ref(which, 1 - member, core)
        arrive(theirs, gather_send.at[which, 1], gather_recv.at[which, 1])
        send(theirs, theirs, gather_send.at[which, 2], gather_recv.at[which, 2], core_peer)
        arrive(
            gather_ref(which, 1 - member, 1 - core),
            gather_send.at[which, 2], gather_recv.at[which, 2],
        )

    spread(GATE, 1)
    pass_own(GATE)
    for j in range(2, planes):
        spread(GATE, j)
    raw_copy.wait()
    other_raw = raw.at[
        pl.ds(aligned(member * rows, 16), rows), pl.ds(aligned((1 - core) * width, 128), width)
    ]
    arrive(other_raw, raw_send.at[0], raw_recv.at[0])
    pair_raw = raw.at[
        pl.ds(aligned((1 - member) * rows, 16), rows), pl.ds(aligned(core * width, 128), width)
    ]
    arrive(pair_raw, raw_send.at[1], raw_recv.at[1])
    send(pair_raw, pair_raw, raw_send.at[2], raw_recv.at[2], core_peer)
    for j in range(1, planes):
        relay(GATE, j)
        spread(UP, j)
    pass_own(UP)
    send_own(DOWN)
    last_raw = raw.at[
        pl.ds(aligned((1 - member) * rows, 16), rows), pl.ds(aligned((1 - core) * width, 128), width)
    ]
    arrive(last_raw, raw_send.at[2], raw_recv.at[2])
    norm_all()
    for j in range(1, planes):
        relay(UP, j)
        spread(DOWN, j)
    pass_own(DOWN)
    send_own(MIX)
    for kind in (GATE, UP):
        for j in range(planes):
            complete(kind, j)

    @pl.loop(0, 2)
    def _(r):
        hidden_rows(0, r * rows)

    for j in range(1, planes):
        relay(DOWN, j)
        spread(MIX, j)
    pass_own(MIX)
    for j in range(planes):
        complete(DOWN, j)

        @pl.loop(0, 2)
        def _(r):
            down_rows(0, r * rows, order[j])

        send_core(0, 1 - member, order[j])
        send_core(0, member, order[j])
        if j > 0:
            send_pair(0, order[j - 1])
    send_pair(0, order[planes - 1])
    for j in range(1, planes):
        relay(MIX, j)
    for j in range(planes):
        wait_pair(0, j)
    own_start = (member * 2 + core) * own_rows
    settle(0, 1, 0.5, raw, own_start, current, 2)
    gather_start(1)
    gather_own(1)
    gather_pair(1)
    for j in range(planes):
        complete(MIX, j)

    head = 8

    def mix_in(s):
        at = pl.ds(aligned(s * rows, 128), rows)
        inner = dot(normed[1, at, :], mix_buf[:, 0:channels])
        cgate = dot(normed[1, at, :], mix_buf[:, 2 * channels : 3 * channels])
        conv_in[s, head : head + rows, :] = cgate * inner
        bgates[s] = dot(normed[1, at, :], mix_buf[:, channels : 2 * channels])

    @pl.loop(0, 2)
    def _(s):
        mix_in(s)

    first_segment = (y == 0) & (pair == 0)
    last_segment = (y == 1) & (pair == pairs - 1)

    def halo(source, target, to):
        return pltpu.make_async_remote_copy(
            src_ref=conv_in.at[source, rows : rows + head, :],
            dst_ref=conv_in.at[target, 0:head, :],
            send_sem=halo_send.at[source], recv_sem=halo_recv.at[target],
            device_id=to, device_id_type=MESH,
        )

    tail_here = halo(0, y, y_peer)
    tail_near = halo(1, 1, y_peer)
    tail_far = halo(1, 0, device(x, (z + 2) % planes, 0, core))
    tail_here.start()

    @pl.when(y == 0)
    def _():
        tail_near.start()

    @pl.when((y == 1) & (pair < pairs - 1))
    def _():
        tail_far.start()

    @pl.when(first_segment)
    def _():
        conv_in[0, 0:head, :] = jnp.zeros((head, channels), jnp.float32)

    @pl.when(jnp.logical_not(first_segment))
    def _():
        halo(0, 0, y_peer).wait_recv()

    halo(1, 1, y_peer).wait_recv()

    @pl.loop(0, 2)
    def _(s):
        total = None
        for tap in range(TAPS):
            shifted = conv_in[s, head - TAPS + 1 + tap : head - TAPS + 1 + tap + rows, :]
            scale = taps[tap : tap + 1, pl.ds(aligned(member * channels, 128), channels)]
            total = scale * shifted if total is None else total + scale * shifted
        gated[pl.ds(aligned(s * rows, 128), rows), :] = (bgates[s] * total).astype(jnp.bfloat16)

    for j in range(planes):
        of_z = order[j]

        @pl.loop(0, 2)
        def _(s):
            index = of_z * 2 + s
            cols = pl.ds(aligned(index * out_cols, 128), out_cols)
            weight = mix_buf[pl.ds(aligned(index * weight_rows, 128), channels), 3 * channels :]
            partials[1, :, cols] = dot(gated[...], weight).astype(jnp.bfloat16)

        send_core(1, 1 - member, of_z)
        send_core(1, member, of_z)
        if j > 0:
            send_pair(1, order[j - 1])
    send_pair(1, order[planes - 1])
    for j in range(planes):
        wait_pair(1, j)
    settle(1, 3, 1.0, current, 0, current, 4)
    gather_start(2)
    gather_own(2)
    hidden_rows(2, member * rows)
    for j in range(planes):
        down_rows(2, member * rows, order[j])
        send_core(2, member, order[j])
    gather_pair(2)
    hidden_rows(2, (1 - member) * rows)
    for j in range(planes):
        down_rows(2, (1 - member) * rows, order[j])
        send_core(2, 1 - member, order[j])
        if j > 0:
            send_pair(2, order[j - 1])
    send_pair(2, order[planes - 1])
    for j in range(planes):
        wait_pair(2, j)
    settle(2, 5, 0.5, current, 0, result, None)
    send(
        result.at[:, pl.ds(aligned((1 - core) * width, 128), width)], other_half,
        out_send.at[0], out_recv.at[0], core_peer,
    )
    out[pl.ds(aligned(core * own_rows, 16), own_rows), :] = result[
        :, pl.ds(aligned(core * width, 128), width)
    ]
    arrive(other_half, out_send.at[0], out_recv.at[0])
    out[pl.ds(aligned((1 - core) * own_rows, 16), own_rows), :] = other_half[...]

    for copy in pending:
        copy.wait_send()
    tail_here.wait_send()

    @pl.when(y == 0)
    def _():
        tail_near.wait_send()

    @pl.when((y == 1) & (pair < pairs - 1))
    def _():
        tail_far.wait_send()


def fits_kernel(mesh, stream, w_gate, w_down, w_inner, w_out):
    planes = mesh.shape["fs"] // 2
    return (
        mesh.shape["tp"] == 2
        and mesh.shape["rep"] == 2
        and mesh.shape["fs"] % 4 == 0
        and planes >= 4
        and w_gate.shape[0] == w_inner.shape[0] == w_out.shape[0] // 2
        and stream.shape[0] % 64 == 0
        and w_gate.shape[1] % 256 == 0
        and w_inner.shape[1] % 256 == 0
        and w_down.shape[1] % 128 == 0
    )


def fused(stream, norm_gains, w_gate, w_up, w_down, w_inner, w_bgate, w_cgate, conv_taps, w_out):
    count = lax.axis_size("fs")
    planes = count // 2
    rows, width = stream.shape
    model_width = 2 * width
    weight_rows, units = w_gate.shape[0], w_gate.shape[1] // 2
    channels, down_cols, out_cols = w_inner.shape[1] // 2, w_down.shape[1], w_out.shape[1]
    own_rows = rows // 2
    sides = []
    for side in range(2):
        at = slice(side * channels, (side + 1) * channels)
        sides += [w_inner[:, at], w_bgate[:, at], w_cgate[:, at], w_out[at, :]]
    w_mix = jnp.concatenate(sides, axis=1)
    bf16, f32 = jnp.bfloat16, jnp.float32
    vmem, dma = pltpu.VMEM, pltpu.SemaphoreType.DMA
    anywhere = pl.BlockSpec(memory_space=pl.ANY)
    inside = pl.BlockSpec(memory_space=pltpu.VMEM)
    flops = 2 * 2 * rows * (6 * model_width * units + 4 * model_width * channels)
    return pl.pallas_call(
        functools.partial(layer_kernel, planes),
        out_shape=jax.ShapeDtypeStruct((rows, width), bf16),
        in_specs=[anywhere, inside, anywhere, anywhere, anywhere, anywhere, inside],
        out_specs=inside,
        scratch_shapes=[
            vmem((model_width, units), bf16),
            vmem((model_width, units), bf16),
            vmem((count, units, down_cols), bf16),
            vmem((model_width, 3 * channels + out_cols), bf16),
            vmem((2 * rows, model_width), bf16),
            vmem((3, 2 * rows, model_width), bf16),
            vmem((2 * rows, units), bf16),
            vmem((3, 2 * rows, model_width), bf16),
            vmem((3, 2, own_rows, model_width), bf16),
            vmem((3, own_rows, model_width), bf16),
            vmem((3, own_rows, model_width), bf16),
            vmem((own_rows, model_width), bf16),
            vmem((2, 8 + rows, channels), f32),
            vmem((2, rows, channels), f32),
            vmem((2 * rows, channels), bf16),
            vmem((own_rows, model_width), bf16),
            vmem((own_rows, width), bf16),
            dma((5,)),
            dma((4, 5, planes)),
            dma((4, 5, planes)),
            dma((3,)),
            dma((3,)),
            dma((3, 2, planes)),
            dma((3, 2, planes)),
            dma((3, planes)),
            dma((3, planes)),
            dma((3, 3)),
            dma((3, 3)),
            dma((2,)),
            dma((2,)),
            dma((1,)),
            dma((1,)),
        ],
        cost_estimate=pl.CostEstimate(
            flops=flops, bytes_accessed=4 * w_gate.size * 2, transcendentals=4 * rows * units
        ),
        compiler_params=pltpu.CompilerParams(
            collective_id=0, has_side_effects=True, vmem_limit_bytes=60 * 1024 * 1024
        ),
        name="layer",
    )(stream, norm_gains, w_gate, w_up, w_down, w_mix, conv_taps)


def solution(mesh):
    def body(stream, norm_gains, w_gate, w_up, w_down, w_inner, w_bgate, w_cgate, conv_taps, w_out):
        arguments = (stream, norm_gains, w_gate, w_up, w_down, w_inner, w_bgate, w_cgate, conv_taps, w_out)
        if fits_kernel(mesh, stream, w_gate, w_down, w_inner, w_out):
            return fused(*arguments)
        return shards(*arguments)

    return jax.shard_map(
        body,
        mesh=mesh,
        in_specs=(
            P(("rep", "fs"), "tp"),
            P(),
            P("fs", "tp"),
            P("fs", "tp"),
            P("tp", "fs"),
            P("fs", "tp"),
            P("fs", "tp"),
            P("fs", "tp"),
            P(None, "tp"),
            P("tp", "fs"),
        ),
        out_specs=P(("rep", "fs"), "tp"),
        check_vma=False,
    )
```

```python
import functools

import jax
import jax.numpy as jnp
from jax import lax
from jax.experimental import pallas as pl
from jax.experimental.pallas import tpu as pltpu
from jax.sharding import PartitionSpec as P

TAPS = 3
EPSILON = 1e-06


def ring_order(count):
    return list(range(0, count, 2)) + list(range(1, count, 2))[::-1]


def swap(x, axis):
    return lax.ppermute(x, axis, [(0, 1), (1, 0)])


def copy_blocks(count, size, starts, source, target):
    for i in range(count):
        begin = pl.multiple_of(starts[i] * size, size)
        target[:, i * size : (i + 1) * size] = source[:, pl.ds(begin, size)]


def permuted(x, starts, size):
    return pl.pallas_call(
        functools.partial(copy_blocks, len(starts), size),
        in_specs=[
            pl.BlockSpec(memory_space=pltpu.SMEM),
            pl.BlockSpec(memory_space=pltpu.VMEM),
        ],
        out_specs=pl.BlockSpec(memory_space=pltpu.VMEM),
        out_shape=jax.ShapeDtypeStruct(x.shape, x.dtype),
        cost_estimate=pl.CostEstimate(flops=0, bytes_accessed=2 * x.size * x.dtype.itemsize, transcendentals=0),
        compiler_params=pltpu.CompilerParams(vmem_limit_bytes=3 * x.size * x.dtype.itemsize),
    )(jnp.stack(starts), x)


class Ring:
    def __init__(self, own, after=None):
        count = lax.axis_size("fs")
        order = ring_order(count)
        onward = [(order[i], order[(i + 1) % count]) for i in range(count)]
        back = [(b, a) for a, b in onward]
        half = count // 2
        first, second = own, own
        if after is not None:
            first, _ = lax.optimization_barrier((own, after[0]))
            second, _ = lax.optimization_barrier((own, after[1]))
        rows = own.shape[0] // 2
        self.shards = {0: own}
        self.arrived = self.early = (own, own)
        for step in range(1, half):
            first = lax.ppermute(first, "fs", onward)
            second = lax.ppermute(second, "fs", back)
            self.shards[step] = first
            self.shards[count - step] = second
            self.arrived = (first, second)
            if step == 1:
                self.early = self.arrived
        self.last = (
            lax.ppermute(first[:rows], "fs", onward),
            lax.ppermute(second[rows:], "fs", back),
        )
        self.shards[half] = jnp.concatenate(self.last, axis=0)
        self.sequence = [0]
        for step in range(1, half):
            self.sequence += [step, count - step]
        self.sequence += [half]

    def lined_up(self, axis):
        return jnp.concatenate([self.shards[d] for d in range(len(self.shards))], axis=axis)


def shards(stream, norm_gains, w_gate, w_up, w_down, w_inner, w_bgate, w_cgate, conv_taps, w_out):
    count, tp = lax.axis_size("fs"), lax.axis_size("tp")
    tp_index, rep_index, fs_index = lax.axis_index("tp"), lax.axis_index("rep"), lax.axis_index("fs")
    rows, width = stream.shape
    model_width = width * tp
    order = ring_order(count)
    places = [order.index(i) for i in range(count)]
    place = jnp.array(places, jnp.int32)[fs_index]
    origin = [
        jnp.array(order, jnp.int32)[lax.rem(place - d + count, count)] for d in range(count)
    ]

    behind = [
        lax.rem(place - places[i] + count, count) for i in range(count)
    ]

    def blocks(x, starts):
        size = x.shape[1] // count
        if size % 128 == 0:
            return permuted(x, starts, size)
        return jnp.concatenate(
            [lax.dynamic_slice_in_dim(x, start * size, size, 1) for start in starts], axis=1
        )

    def rep_part(w, axis):
        size = w.shape[axis] // lax.axis_size("rep")
        return lax.dynamic_slice_in_dim(w, rep_index * size, size, axis)

    def whole_features(x):
        if tp != 2:
            return lax.all_gather(x, "tp", axis=1, tiled=True)
        other = swap(x, "tp")
        mine = tp_index == 0
        return jnp.concatenate([jnp.where(mine, x, other), jnp.where(mine, other, x)], axis=1)

    def own_features(x):
        return lax.dynamic_slice_in_dim(x, tp_index * width, width, 1)

    def feature_sum(partials):
        rounded = blocks(partials.astype(jnp.bfloat16), behind)
        if tp != 2:
            return lax.psum_scatter(rounded, "tp", scatter_dimension=1, tiled=True).astype(jnp.float32)
        theirs = lax.dynamic_slice_in_dim(rounded, (1 - tp_index) * width, width, 1)
        received = swap(theirs, "tp").astype(jnp.float32)
        return own_features(rounded).astype(jnp.float32) + received

    def norm_own(current, row):
        values = current.astype(jnp.float32)
        scaled = values * lax.rsqrt(jnp.mean(values * values, axis=1, keepdims=True) + EPSILON)
        return (scaled * norm_gains[row]).astype(jnp.bfloat16)

    def norm_other(normed):
        return whole_features(swap(own_features(normed), "rep"))

    def settle(current, own_sum, other_sum, row, weight):
        received = swap(other_sum.astype(jnp.bfloat16), "rep").astype(jnp.float32)
        branch = whole_features(own_sum + received)
        scaled = branch * lax.rsqrt(jnp.mean(branch * branch, axis=1, keepdims=True) + EPSILON)
        return (current.astype(jnp.float32) + weight * (scaled * norm_gains[row])).astype(
            jnp.bfloat16
        )

    def dot(a, b):
        return jnp.dot(a, b, preferred_element_type=jnp.float32)

    def activate(gate_vals, upward):
        return (jax.nn.silu(gate_vals) * upward).astype(jnp.bfloat16)

    current = whole_features(stream)
    normed = norm_own(current, 0)
    normed = jnp.concatenate([normed, norm_other(normed)], axis=0)

    gate_ring = Ring(rep_part(w_gate, 1))
    up_ring = Ring(rep_part(w_up, 1))
    down_own = rep_part(w_down, 0)
    down_ring = Ring(down_own, gate_ring.arrived)
    mix_own = jnp.concatenate([rep_part(w, 1) for w in (w_inner, w_bgate, w_cgate)], axis=1)
    out_own = rep_part(w_out, 0)
    mix_width = mix_own.shape[1]
    mix_ring = Ring(
        jnp.concatenate([mix_own, out_own.reshape(mix_own.shape[0], -1)], axis=1), down_ring.early
    )

    def by_shards(ring):
        size = ring.shards[0].shape[0]
        total = None
        for d in ring.sequence:
            term = dot(lax.dynamic_slice_in_dim(normed, origin[d] * size, size, 1), ring.shards[d])
            total = term if total is None else total + term
        return total

    hidden = activate(by_shards(gate_ring), by_shards(up_ring))
    down_blocks = {d: dot(hidden, down_ring.shards[d]).astype(jnp.bfloat16) for d in down_ring.sequence}
    sums = feature_sum(jnp.concatenate([down_blocks[d] for d in range(count)], axis=1))
    first = settle(current, sums[:rows], sums[rows:], 1, 0.5)

    mix_whole = mix_ring.lined_up(0)[:, :mix_width]
    out_whole = jnp.concatenate(
        [mix_ring.shards[d][:, mix_width:].reshape(out_own.shape) for d in range(count)], axis=1
    )
    channels = mix_width // 3
    taps = rep_part(conv_taps, 1)

    def mix_in(normed_mix):
        product = dot(blocks(normed_mix, origin), mix_whole)
        inner, bgate, cgate = (product[:, i * channels : (i + 1) * channels] for i in range(3))
        return cgate * inner, bgate

    def mix_out(conv_input, bgate, earlier):
        padded = jnp.concatenate([earlier, conv_input], axis=0)
        conv = taps[0] * padded[0:rows]
        for tap in range(1, TAPS):
            conv = conv + taps[tap] * padded[tap : tap + rows]
        return feature_sum(dot((bgate * conv).astype(jnp.bfloat16), out_whole))

    normed_mix = norm_own(first, 2)
    other_mix = norm_other(normed_mix)
    own_in, own_bgate = mix_in(normed_mix)
    other_in, other_bgate = mix_in(other_mix)
    tails = jnp.concatenate([own_in[rows - (TAPS - 1) :], other_in[rows - (TAPS - 1) :]], axis=0)
    earlier = lax.ppermute(tails, "fs", [(i, i + 1) for i in range(count - 1)])
    other_sum = mix_out(other_in, other_bgate, earlier[TAPS - 1 :])
    own_sum = mix_out(own_in, own_bgate, earlier[: TAPS - 1])
    second = settle(first, own_sum, other_sum, 3, 1.0)

    gate_whole, up_whole = gate_ring.lined_up(0), up_ring.lined_up(0)
    down_whole = down_ring.lined_up(1)

    def units(normed_rows):
        lined = blocks(normed_rows, origin)
        return activate(dot(lined, gate_whole), dot(lined, up_whole))

    normed = norm_own(second, 4)
    other_normed = norm_other(normed)
    own_units = units(normed)
    other_sum = feature_sum(dot(units(other_normed), down_whole))
    own_sum = feature_sum(dot(own_units, down_whole))
    return own_features(settle(second, own_sum, other_sum, 5, 0.5))


MESH = pl.DeviceIdType.MESH
GATE, UP, DOWN, MIX = range(4)
Z, X, Y, PART_A, PART_B, Z_OTHER = range(6)


def aligned(value, to):
    return pl.multiple_of(value, to)


def layer_kernel(
    planes,
    stream, all_gains, w_gate, w_up, w_down, w_inner, w_bgate, w_cgate, all_taps, w_out, out,
    gains, taps, w_mix,
    gate_buf, up_buf, down_buf, mix_buf, raw, normed, hidden, partials, from_core, summed,
    from_pair, current, conv_in, bgates, gated, result,
    local_sem, pack_sem, piece_send, piece_recv, raw_send, raw_recv, core_send, core_recv,
    pair_send, pair_recv, gather_send, gather_recv, halo_send, halo_recv, out_send, out_recv, store_sem,
):
    x, place, core = lax.axis_index("rep"), lax.axis_index("fs"), lax.axis_index("tp")
    z, y = place // 2, place % 2
    pair, member = z // 2, z % 2
    pairs = planes // 2
    rows, width = stream.shape
    quarter = rows // 4
    model_width = 2 * width
    units, channels, mix_width = gate_buf.shape[1], gated.shape[1], mix_buf.shape[1]
    out_cols = mix_width - 3 * channels
    weight_rows = w_gate.shape[0]
    down_cols = w_down.shape[1]
    plane_cols = 2 * down_cols
    buffers = (gate_buf, up_buf, down_buf, mix_buf)
    halves = (weight_rows // 2, weight_rows // 2, units // 2, weight_rows // 2)

    def device(to_x, to_z, to_y, to_core):
        return (to_x, to_z * 2 + to_y, to_core)

    order = [2 * ((pair + j // 2) % pairs) + (member + j) % 2 for j in range(planes)]
    partner = order[1]
    core_peer = device(x, z, y, 1 - core)
    pair_peer = device(x, partner, y, core)
    x_peer, y_peer = device(1 - x, z, y, core), device(x, z, 1 - y, core)

    pending = []

    def send(source, target, send_sem, recv_sem, to):
        copy = pltpu.make_async_remote_copy(
            src_ref=source, dst_ref=target, send_sem=send_sem, recv_sem=recv_sem,
            device_id=to, device_id_type=MESH,
        )
        copy.start()
        pending.append(copy)

    def arrive(target, send_sem, recv_sem):
        pltpu.make_async_remote_copy(
            src_ref=target, dst_ref=target, send_sem=send_sem, recv_sem=recv_sem,
            device_id=core_peer, device_id_type=MESH,
        ).wait_recv()

    def piece(kind, of_z, of_y, of_x, begin=0, end=None):
        half = halves[kind]
        count = (half if end is None else end) - begin
        if kind == DOWN:
            return down_buf.at[of_z * 2 + of_y, pl.ds(aligned(of_x * half + begin, 16), count), :]
        start = ((of_z * 2 + of_y) * 2 + of_x) * half + begin
        return buffers[kind].at[pl.ds(aligned(start, 16), count), :]

    def own_source(kind, side, start, count):
        if kind == DOWN:
            return w_down.at[pl.ds(aligned(side * units + start, 16), count), :]
        cols = mix_width if kind == MIX else units
        source = (w_gate, w_up, None, w_mix)[kind]
        return source.at[pl.ds(aligned(start, 16), count), pl.ds(aligned(side * cols, 128), cols)]

    def piece_copy(source, target, kind, route, of_z, to, index=None):
        index = of_z if index is None else index
        send(source, target, piece_send.at[kind, route, index], piece_recv.at[kind, route, of_z], to)

    def wait_piece(target, kind, route, of_z):
        arrive(target, piece_send.at[kind, route, of_z], piece_recv.at[kind, route, of_z])

    def direct(kind, j):
        half = halves[kind]
        if kind == MIX:
            return half if j == 1 else half // 2
        if j > 1:
            return 0
        return half // 2 if kind == UP else half

    def split(kind):
        half = halves[kind]
        return half - (half // 8 if kind == MIX else (half * 3 // 8 + 15) // 16 * 16)

    def send_planes(kind, j):
        to, half = order[j], halves[kind]
        piece_copy(
            own_source(kind, to % 2, x * half, half), piece(kind, z, y, x),
            kind, Z, z, device(x, to, y, core), index=to,
        )

    def send_direct(kind, j):
        to, count = order[j], direct(kind, j)
        if count == 0:
            return
        piece_copy(
            own_source(kind, to % 2, (1 - x) * halves[kind], count), piece(kind, z, y, 1 - x, 0, count),
            kind, Z_OTHER, z, device(x, to, y, core), index=to,
        )

    def own_part(kind, i):
        half = halves[kind] // 2
        return i * half, (i + 1) * half

    def send_own(kind):
        for i, route in enumerate((Y, PART_A)):
            begin, end = own_part(kind, i)
            piece_copy(
                own_source(kind, member, x * halves[kind] + begin, end - begin),
                piece(kind, z, y, x, begin, end), kind, route, z, y_peer,
            )

    def pass_own(kind, i):
        part = piece(kind, z, 1 - y, x, *own_part(kind, i))
        wait_piece(part, kind, (Y, PART_A)[i], z)
        piece_copy(part, part, kind, (X, PART_B)[i], z, x_peer)

    def spread(kind, j):
        of = order[j]
        whole = piece(kind, of, y, x)
        wait_piece(whole, kind, Z, of)
        piece_copy(whole, whole, kind, Y, of, y_peer)
        if direct(kind, j) < halves[kind]:
            rest = piece(kind, of, y, x, direct(kind, j), None)
            piece_copy(rest, rest, kind, X, of, x_peer)

    def relay(kind, j):
        of = order[j]
        if direct(kind, j) == halves[kind]:
            wait_piece(piece(kind, of, y, 1 - x), kind, Z_OTHER, of)
        else:
            wait_piece(piece(kind, of, y, 1 - x, direct(kind, j), None), kind, X, of)
        part = piece(kind, of, y, 1 - x, split(kind), None)
        piece_copy(part, part, kind, PART_A, of, y_peer)
        wait_piece(piece(kind, of, 1 - y, x), kind, Y, of)
        part = piece(kind, of, 1 - y, x, 0, split(kind))
        piece_copy(part, part, kind, PART_B, of, x_peer)

    def local_copy(kind):
        count = units if kind == DOWN else weight_rows
        if kind == DOWN:
            target = down_buf.at[z * 2 + y]
        else:
            target = buffers[kind].at[pl.ds(aligned((z * 2 + y) * weight_rows, 16), count), :]
        return pltpu.make_async_copy(own_source(kind, member, 0, count), target, local_sem.at[kind])

    def complete(kind, j):
        of = order[j]
        if j == 0:
            local_copy(kind).wait()
            for i, route in enumerate((X, PART_B)):
                wait_piece(piece(kind, z, 1 - y, 1 - x, *own_part(kind, i)), kind, route, z)
        else:
            if 0 < direct(kind, j) < halves[kind]:
                wait_piece(piece(kind, of, y, 1 - x, 0, direct(kind, j)), kind, Z_OTHER, of)
            wait_piece(piece(kind, of, 1 - y, 1 - x, split(kind), None), kind, PART_A, of)
            wait_piece(piece(kind, of, 1 - y, 1 - x, 0, split(kind)), kind, PART_B, of)

    own_raw = raw.at[pl.ds(aligned(member * rows, 16), rows), pl.ds(aligned(core * width, 128), width)]
    packs = []
    for side in range(2):
        base = side * mix_width
        for n, weight in enumerate((w_inner, w_bgate, w_cgate)):
            packs.append((
                weight.at[:, side * channels : (side + 1) * channels],
                w_mix.at[:, base + n * channels : base + (n + 1) * channels],
            ))
        packs.append((
            w_out.at[side * channels : (side + 1) * channels, :],
            w_mix.at[:, base + 3 * channels : base + mix_width],
        ))
    packs += [(all_gains, gains), (all_taps, taps)]
    packs = [pltpu.make_async_copy(a, b, pack_sem.at[n]) for n, (a, b) in enumerate(packs)]
    for copy in packs:
        copy.start()
    raw_copy = pltpu.make_async_copy(stream, own_raw, local_sem.at[4])
    raw_copy.start()
    for kind in (GATE, UP, DOWN):
        local_copy(kind).start()

    first_segment = (y == 0) & (pair == 0)

    @pl.when(first_segment)
    def _():
        conv_in[0, 0:8, :] = jnp.zeros((8, channels), jnp.float32)

    barrier = pltpu.get_barrier_semaphore()
    greeted = [core_peer, x_peer, y_peer]
    greeted += [device(x, order[j], y, core) for j in range(1, planes)]
    greeted += [device(x, (z + s) % planes, 1 - y, core) for s in sorted({2, planes - 2})]
    for peer in greeted:
        pl.semaphore_signal(barrier, inc=1, device_id=peer, device_id_type=MESH)
    pl.semaphore_wait(barrier, len(greeted))

    others = range(1, planes)
    send_own(GATE)
    for j in others:
        send_planes(GATE, j)
    send_own(UP)
    send_own(DOWN)
    send(stream, own_raw, raw_send.at[0], raw_recv.at[0], core_peer)
    for j in others:
        send_direct(GATE, j)
    for copy in packs:
        copy.wait()
    local_copy(MIX).start()

    def rms(values):
        return values * lax.rsqrt(jnp.mean(values * values, axis=1, keepdims=True) + EPSILON)

    step_rows = 16

    def norm_all():
        @pl.loop(0, 2 * rows // step_rows)
        def _(i):
            at = pl.ds(aligned(i * step_rows, 16), step_rows)
            values = raw[at, :].astype(jnp.float32)
            normed[0, at, :] = (rms(values) * gains[0:1, :]).astype(jnp.bfloat16)

    def dot(a, b):
        return jnp.dot(a, b, preferred_element_type=jnp.float32)

    tile = 256

    def hidden_rows(which, start, row_count):
        at = pl.ds(aligned(start, 128), row_count)

        def columns(begin, count):
            cols = pl.ds(aligned(begin, 128), count)
            gate = dot(normed[which, at, :], gate_buf[:, cols])
            up = dot(normed[which, at, :], up_buf[:, cols])
            hidden[at, cols] = (gate / (1.0 + jnp.exp(-gate)) * up).astype(jnp.bfloat16)

        @pl.loop(0, units // tile)
        def _(n):
            columns(n * tile, tile)

        if units % tile:
            columns(units - units % tile, units % tile)

    def down_rows(phase, start, row_count, of_z):
        at = pl.ds(aligned(start, 128), row_count)

        @pl.loop(0, 2)
        def _(s):
            cols = pl.ds(aligned((of_z * 2 + s) * down_cols, 128), down_cols)
            partials[phase, at, cols] = dot(hidden[at, :], down_buf[of_z * 2 + s]).astype(jnp.bfloat16)

    def owned(of_member, of_core, part):
        return of_member * rows + part * 2 * quarter + of_core * quarter

    def owned_rows(of_member, of_core, part):
        return pl.ds(aligned(owned(of_member, of_core, part), 16), quarter)

    def local_rows(part):
        return pl.ds(part * quarter, quarter)

    def plane_of(of_z):
        return pl.ds(aligned(of_z * plane_cols, 128), plane_cols)

    def send_core(phase, of_member, part, of_z):
        send(
            partials.at[phase, owned_rows(of_member, 1 - core, part), plane_of(of_z)],
            from_core.at[phase, of_member, local_rows(part), plane_of(of_z)],
            core_send.at[phase, of_member, part, of_z], core_recv.at[phase, of_member, part, of_z],
            core_peer,
        )

    def wait_core(phase, of_member, part, of_z):
        arrive(
            from_core.at[phase, of_member, local_rows(part), plane_of(of_z)],
            core_send.at[phase, of_member, part, of_z], core_recv.at[phase, of_member, part, of_z],
        )

    def send_pair(phase, part, of_z):
        wait_core(phase, 1 - member, part, of_z)
        at, cols = local_rows(part), plane_of(of_z)
        mine = partials[phase, owned_rows(1 - member, core, part), cols].astype(jnp.float32)
        theirs = from_core[phase, 1 - member, at, cols].astype(jnp.float32)
        summed[phase, at, cols] = (mine + theirs).astype(jnp.bfloat16)
        send(
            summed.at[phase, at, cols], from_pair.at[phase, at, cols],
            pair_send.at[phase, part, of_z], pair_recv.at[phase, part, of_z], pair_peer,
        )

    def wait_pair(phase, part):
        for of_z in order:
            wait_core(phase, member, part, of_z)
            arrive(
                from_pair.at[phase, local_rows(part), plane_of(of_z)],
                pair_send.at[phase, part, of_z], pair_recv.at[phase, part, of_z],
            )

    def settle(phase, gain, weight, source, target, next_gain, part):
        @pl.loop(0, quarter // step_rows)
        def _(i):
            at = pl.ds(aligned(part * quarter + i * step_rows, 16), step_rows)
            mine = pl.ds(aligned(owned(member, core, part) + i * step_rows, 16), step_rows)
            branch = (
                partials[phase, mine, :].astype(jnp.float32)
                + from_core[phase, member, at, :].astype(jnp.float32)
                + from_pair[phase, at, :].astype(jnp.float32)
            )
            before = source[mine if phase == 0 else at, :]
            after = before.astype(jnp.float32) + weight * (rms(branch) * gains[gain : gain + 1, :])
            rounded = after.astype(jnp.bfloat16)
            target[at, :] = rounded
            if next_gain is not None:
                scaled = rms(rounded.astype(jnp.float32)) * gains[next_gain : next_gain + 1, :]
                normed[phase + 1, mine, :] = scaled.astype(jnp.bfloat16)

    def gather_ref(which, of_member, of_core, part):
        return normed.at[which, owned_rows(of_member, of_core, part), :]

    def gather_start(which, part):
        mine = gather_ref(which, member, core, part)
        send(mine, mine, gather_send.at[which, 1, part], gather_recv.at[which, 1, part], pair_peer)
        send(mine, mine, gather_send.at[which, 0, part], gather_recv.at[which, 0, part], core_peer)

    def gather_own(which, part):
        arrive(
            gather_ref(which, member, 1 - core, part),
            gather_send.at[which, 0, part], gather_recv.at[which, 0, part],
        )

    def gather_pass(which, part):
        theirs = gather_ref(which, 1 - member, core, part)
        arrive(theirs, gather_send.at[which, 1, part], gather_recv.at[which, 1, part])
        send(theirs, theirs, gather_send.at[which, 2, part], gather_recv.at[which, 2, part], core_peer)

    def gather_pair(which, part):
        arrive(
            gather_ref(which, 1 - member, 1 - core, part),
            gather_send.at[which, 2, part], gather_recv.at[which, 2, part],
        )

    head = 8

    def mix_in(s, begin, count):
        at = pl.ds(aligned(s * rows + begin, 128), count)
        inner = dot(normed[1, at, :], mix_buf[:, 0:channels])
        cgate = dot(normed[1, at, :], mix_buf[:, 2 * channels : 3 * channels])
        conv_in[s, head + begin : head + begin + count, :] = cgate * inner
        bgates[s, begin : begin + count, :] = dot(
            normed[1, at, :], mix_buf[:, channels : 2 * channels]
        )

    def halo(source, target, to):
        return pltpu.make_async_remote_copy(
            src_ref=conv_in.at[source, rows : rows + head, :],
            dst_ref=conv_in.at[target, 0:head, :],
            send_sem=halo_send.at[source], recv_sem=halo_recv.at[target],
            device_id=to, device_id_type=MESH,
        )

    def near_tail(s):
        return halo(s, y + s * (1 - y), y_peer)

    def far_tail(s):
        return halo(s, 0, device(x, (z + 2) % planes, 0, core))

    def tails(s, act):
        @pl.when((s == 0) | (y == 0))
        def _():
            act(near_tail(s))

        @pl.when((s == 1) & (y == 1) & (pair < pairs - 1))
        def _():
            act(far_tail(s))

    def mix_gate(s):
        @pl.when(jnp.logical_not(first_segment & (s == 0)))
        def _():
            near_tail_recv = halo(s, s, y_peer)
            near_tail_recv.wait_recv()

        total = None
        for tap in range(TAPS):
            begin = head - TAPS + 1 + tap
            shifted = conv_in[s, begin : begin + rows, :]
            scale = taps[tap : tap + 1, pl.ds(aligned(member * channels, 128), channels)]
            total = scale * shifted if total is None else total + scale * shifted
        gated[pl.ds(aligned(s * rows, 128), rows), :] = (bgates[s] * total).astype(jnp.bfloat16)

    def mix_out(s, part, of_z):
        at = pl.ds(aligned(s * rows + part * 2 * quarter, 128), 2 * quarter)

        @pl.loop(0, 2)
        def _(n):
            index = of_z * 2 + n
            cols = pl.ds(aligned(index * out_cols, 128), out_cols)
            weight = mix_buf[pl.ds(aligned(index * weight_rows, 128), channels), 3 * channels :]
            partials[1, at, cols] = dot(gated[at, :], weight).astype(jnp.bfloat16)

    def core_parts(phase, of_member, part):
        for of_z in order:
            send_core(phase, of_member, part, of_z)

    def pair_parts(phase, part):
        for of_z in order:
            send_pair(phase, part, of_z)

    for kind, i in ((GATE, 0), (GATE, 1), (UP, 0), (UP, 1)):
        pass_own(kind, i)
    for j in others:
        spread(GATE, j)
        send_planes(UP, j)
        if j <= 2:
            pass_own(DOWN, j - 1)
    send(stream, own_raw, raw_send.at[1], raw_recv.at[1], pair_peer)
    for j in others:
        send_direct(UP, j)
    for j in others:
        relay(GATE, j)
        spread(UP, j)
        send_planes(DOWN, j)
    for j in others:
        send_direct(DOWN, j)
    for j in others:
        relay(UP, j)
        spread(DOWN, j)
        send_planes(MIX, j)
    for j in others:
        send_direct(MIX, j)
    raw_copy.wait()

    def raw_at(of_member, of_core):
        return raw.at[
            pl.ds(aligned(of_member * rows, 16), rows), pl.ds(aligned(of_core * width, 128), width)
        ]

    arrive(raw_at(member, 1 - core), raw_send.at[0], raw_recv.at[0])
    pair_raw = raw_at(1 - member, core)
    arrive(pair_raw, raw_send.at[1], raw_recv.at[1])
    send(pair_raw, pair_raw, raw_send.at[2], raw_recv.at[2], core_peer)
    arrive(raw_at(1 - member, 1 - core), raw_send.at[2], raw_recv.at[2])
    norm_all()
    for kind in (GATE, UP):
        for j in range(planes):
            complete(kind, j)
    hidden_rows(0, 0, rows)
    relay(DOWN, 1)
    relay(DOWN, 2)
    hidden_rows(0, rows, rows)
    for j in range(3, planes):
        relay(DOWN, j)
    send_own(MIX)
    for j in others:
        spread(MIX, j)
    for j in range(planes):
        complete(DOWN, j)

        @pl.loop(0, 2)
        def _(r):
            down_rows(0, r * rows, rows, order[j])

        for of_member in (1 - member, member):
            for part in (1, 0):
                send_core(0, of_member, part, order[j])
        if j > 0:
            for part in (1, 0):
                send_pair(0, part, order[j - 1])
    for part in (1, 0):
        send_pair(0, part, order[planes - 1])
    pass_own(MIX, 0)
    pass_own(MIX, 1)
    relay(MIX, 1)
    for part in (1, 0):
        wait_pair(0, part)
        settle(0, 1, 0.5, raw, current, 2, part)
        gather_start(1, part)
    for j in range(2, planes):
        relay(MIX, j)
    gather_own(1, 1)
    gather_own(1, 0)
    gather_pass(1, 1)
    for j in range(planes):
        complete(MIX, j)
    mix_in(member, 0, rows)
    tails(member, lambda copy: copy.start())
    gather_pass(1, 0)
    gather_pair(1, 1)
    mix_in(1 - member, 2 * quarter, 2 * quarter)
    tails(1 - member, lambda copy: copy.start())
    gather_pair(1, 0)
    mix_in(1 - member, 0, 2 * quarter)
    mix_gate(1 - member)
    for part in range(2):
        for of_z in order:
            mix_out(1 - member, part, of_z)
        core_parts(1, 1 - member, part)
    mix_gate(member)
    pair_parts(1, 0)
    for of_z in order:
        mix_out(member, 0, of_z)
    core_parts(1, member, 0)
    pair_parts(1, 1)
    for of_z in order:
        mix_out(member, 1, of_z)
    core_parts(1, member, 1)
    for part in range(2):
        wait_pair(1, part)
        settle(1, 3, 1.0, current, current, 4, part)
        gather_start(2, part)
    gather_own(2, 0)
    gather_own(2, 1)
    hidden_rows(2, member * rows, rows)
    for of_z in order:
        down_rows(2, member * rows, rows, of_z)
    for part in range(2):
        core_parts(2, member, part)
    for part in range(2):
        gather_pass(2, part)
        gather_pair(2, part)
        start = (1 - member) * rows + part * 2 * quarter
        hidden_rows(2, start, 2 * quarter)
        for j in range(planes):
            down_rows(2, start, 2 * quarter, order[j])
            send_core(2, 1 - member, part, order[j])
            if j > 0:
                send_pair(2, part, order[j - 1])
        send_pair(2, part, order[planes - 1])
    stores = []
    for part in range(2):
        wait_pair(2, part)
        settle(2, 5, 0.5, current, result, None, part)
        there = pl.ds(aligned(part * 2 * quarter + core * quarter, 16), quarter)
        send(
            result.at[local_rows(part), pl.ds(aligned((1 - core) * width, 128), width)],
            out.at[there, :], out_send.at[part], out_recv.at[part], core_peer,
        )
        store = pltpu.make_async_copy(
            result.at[local_rows(part), pl.ds(aligned(core * width, 128), width)],
            out.at[there, :], store_sem.at[part],
        )
        store.start()
        stores.append(store)
    for part in range(2):
        stores[part].wait()
        theirs = pl.ds(aligned(part * 2 * quarter + (1 - core) * quarter, 16), quarter)
        arrive(out.at[theirs, :], out_send.at[part], out_recv.at[part])
    for copy in pending:
        copy.wait_send()
    for s in range(2):
        tails(s, lambda copy: copy.wait_send())


def fits_kernel(mesh, stream, w_gate, w_down, w_inner, w_out):
    planes = mesh.shape["fs"] // 2
    return (
        mesh.shape["tp"] == 2
        and mesh.shape["rep"] == 2
        and mesh.shape["fs"] % 4 == 0
        and planes >= 4
        and w_gate.shape[0] == w_inner.shape[0] == w_out.shape[0] // 2
        and stream.shape[0] % 256 == 0
        and w_gate.shape[0] % 256 == 0
        and w_gate.shape[1] % 256 == 0
        and w_inner.shape[1] % 256 == 0
        and w_down.shape[1] % 128 == 0
    )


def fused(stream, norm_gains, w_gate, w_up, w_down, w_inner, w_bgate, w_cgate, conv_taps, w_out):
    count = lax.axis_size("fs")
    planes = count // 2
    rows, width = stream.shape
    model_width = 2 * width
    weight_rows, units = w_gate.shape[0], w_gate.shape[1] // 2
    channels, down_cols, out_cols = w_inner.shape[1] // 2, w_down.shape[1], w_out.shape[1]
    own_rows = rows // 2
    mix_width = 3 * channels + out_cols
    bf16, f32 = jnp.bfloat16, jnp.float32
    vmem, dma = pltpu.VMEM, pltpu.SemaphoreType.DMA
    anywhere = pl.BlockSpec(memory_space=pl.ANY)
    flops = 2 * 2 * rows * (6 * model_width * units + 4 * model_width * channels)
    return pl.pallas_call(
        functools.partial(layer_kernel, planes),
        out_shape=jax.ShapeDtypeStruct((rows, width), bf16),
        in_specs=[anywhere] * 10,
        out_specs=anywhere,
        scratch_shapes=[
            vmem(norm_gains.shape, f32),
            vmem(conv_taps.shape, f32),
            vmem((weight_rows, 2 * mix_width), bf16),
            vmem((model_width, units), bf16),
            vmem((model_width, units), bf16),
            vmem((count, units, down_cols), bf16),
            vmem((model_width, mix_width), bf16),
            vmem((2 * rows, model_width), bf16),
            vmem((3, 2 * rows, model_width), bf16),
            vmem((2 * rows, units), bf16),
            vmem((3, 2 * rows, model_width), bf16),
            vmem((3, 2, own_rows, model_width), bf16),
            vmem((3, own_rows, model_width), bf16),
            vmem((3, own_rows, model_width), bf16),
            vmem((own_rows, model_width), bf16),
            vmem((2, 8 + rows, channels), f32),
            vmem((2, rows, channels), f32),
            vmem((2 * rows, channels), bf16),
            vmem((own_rows, model_width), bf16),
            dma((5,)),
            dma((10,)),
            dma((4, 6, planes)),
            dma((4, 6, planes)),
            dma((3,)),
            dma((3,)),
            dma((3, 2, 2, planes)),
            dma((3, 2, 2, planes)),
            dma((3, 2, planes)),
            dma((3, 2, planes)),
            dma((3, 3, 2)),
            dma((3, 3, 2)),
            dma((2,)),
            dma((2,)),
            dma((2,)),
            dma((2,)),
            dma((2,)),
        ],
        cost_estimate=pl.CostEstimate(
            flops=flops, bytes_accessed=4 * w_gate.size * 2, transcendentals=4 * rows * units
        ),
        compiler_params=pltpu.CompilerParams(
            collective_id=0, has_side_effects=True, vmem_limit_bytes=60 * 1024 * 1024
        ),
        name="layer",
    )(stream, norm_gains, w_gate, w_up, w_down, w_inner, w_bgate, w_cgate, conv_taps, w_out)


def solution(mesh):
    def body(stream, norm_gains, w_gate, w_up, w_down, w_inner, w_bgate, w_cgate, conv_taps, w_out):
        arguments = (stream, norm_gains, w_gate, w_up, w_down, w_inner, w_bgate, w_cgate, conv_taps, w_out)
        if fits_kernel(mesh, stream, w_gate, w_down, w_inner, w_out):
            return fused(*arguments)
        return shards(*arguments)

    return jax.shard_map(
        body,
        mesh=mesh,
        in_specs=(
            P(("rep", "fs"), "tp"),
            P(),
            P("fs", "tp"),
            P("fs", "tp"),
            P("tp", "fs"),
            P("fs", "tp"),
            P("fs", "tp"),
            P("fs", "tp"),
            P(None, "tp"),
            P("tp", "fs"),
        ),
        out_specs=P(("rep", "fs"), "tp"),
        check_vma=False,
    )
```

```python
import functools

import jax
import jax.numpy as jnp
from jax import lax
from jax.experimental import pallas as pl
from jax.experimental.pallas import tpu as pltpu
from jax.sharding import PartitionSpec as P

TAPS = 3
EPSILON = 1e-06


def ring_order(count):
    return list(range(0, count, 2)) + list(range(1, count, 2))[::-1]


def swap(x, axis):
    return lax.ppermute(x, axis, [(0, 1), (1, 0)])


def copy_blocks(count, size, starts, source, target):
    for i in range(count):
        begin = pl.multiple_of(starts[i] * size, size)
        target[:, i * size : (i + 1) * size] = source[:, pl.ds(begin, size)]


def permuted(x, starts, size):
    return pl.pallas_call(
        functools.partial(copy_blocks, len(starts), size),
        in_specs=[
            pl.BlockSpec(memory_space=pltpu.SMEM),
            pl.BlockSpec(memory_space=pltpu.VMEM),
        ],
        out_specs=pl.BlockSpec(memory_space=pltpu.VMEM),
        out_shape=jax.ShapeDtypeStruct(x.shape, x.dtype),
        cost_estimate=pl.CostEstimate(flops=0, bytes_accessed=2 * x.size * x.dtype.itemsize, transcendentals=0),
        compiler_params=pltpu.CompilerParams(vmem_limit_bytes=3 * x.size * x.dtype.itemsize),
    )(jnp.stack(starts), x)


class Ring:
    def __init__(self, own, after=None):
        count = lax.axis_size("fs")
        order = ring_order(count)
        onward = [(order[i], order[(i + 1) % count]) for i in range(count)]
        back = [(b, a) for a, b in onward]
        half = count // 2
        first, second = own, own
        if after is not None:
            first, _ = lax.optimization_barrier((own, after[0]))
            second, _ = lax.optimization_barrier((own, after[1]))
        rows = own.shape[0] // 2
        self.shards = {0: own}
        self.arrived = self.early = (own, own)
        for step in range(1, half):
            first = lax.ppermute(first, "fs", onward)
            second = lax.ppermute(second, "fs", back)
            self.shards[step] = first
            self.shards[count - step] = second
            self.arrived = (first, second)
            if step == 1:
                self.early = self.arrived
        self.last = (
            lax.ppermute(first[:rows], "fs", onward),
            lax.ppermute(second[rows:], "fs", back),
        )
        self.shards[half] = jnp.concatenate(self.last, axis=0)
        self.sequence = [0]
        for step in range(1, half):
            self.sequence += [step, count - step]
        self.sequence += [half]

    def lined_up(self, axis):
        return jnp.concatenate([self.shards[d] for d in range(len(self.shards))], axis=axis)


def shards(stream, norm_gains, w_gate, w_up, w_down, w_inner, w_bgate, w_cgate, conv_taps, w_out):
    count, tp = lax.axis_size("fs"), lax.axis_size("tp")
    tp_index, rep_index, fs_index = lax.axis_index("tp"), lax.axis_index("rep"), lax.axis_index("fs")
    rows, width = stream.shape
    model_width = width * tp
    order = ring_order(count)
    places = [order.index(i) for i in range(count)]
    place = jnp.array(places, jnp.int32)[fs_index]
    origin = [
        jnp.array(order, jnp.int32)[lax.rem(place - d + count, count)] for d in range(count)
    ]

    behind = [
        lax.rem(place - places[i] + count, count) for i in range(count)
    ]

    def blocks(x, starts):
        size = x.shape[1] // count
        if size % 128 == 0:
            return permuted(x, starts, size)
        return jnp.concatenate(
            [lax.dynamic_slice_in_dim(x, start * size, size, 1) for start in starts], axis=1
        )

    def rep_part(w, axis):
        size = w.shape[axis] // lax.axis_size("rep")
        return lax.dynamic_slice_in_dim(w, rep_index * size, size, axis)

    def whole_features(x):
        if tp != 2:
            return lax.all_gather(x, "tp", axis=1, tiled=True)
        other = swap(x, "tp")
        mine = tp_index == 0
        return jnp.concatenate([jnp.where(mine, x, other), jnp.where(mine, other, x)], axis=1)

    def own_features(x):
        return lax.dynamic_slice_in_dim(x, tp_index * width, width, 1)

    def feature_sum(partials):
        rounded = blocks(partials.astype(jnp.bfloat16), behind)
        if tp != 2:
            return lax.psum_scatter(rounded, "tp", scatter_dimension=1, tiled=True).astype(jnp.float32)
        theirs = lax.dynamic_slice_in_dim(rounded, (1 - tp_index) * width, width, 1)
        received = swap(theirs, "tp").astype(jnp.float32)
        return own_features(rounded).astype(jnp.float32) + received

    def norm_own(current, row):
        values = current.astype(jnp.float32)
        scaled = values * lax.rsqrt(jnp.mean(values * values, axis=1, keepdims=True) + EPSILON)
        return (scaled * norm_gains[row]).astype(jnp.bfloat16)

    def norm_other(normed):
        return whole_features(swap(own_features(normed), "rep"))

    def settle(current, own_sum, other_sum, row, weight):
        received = swap(other_sum.astype(jnp.bfloat16), "rep").astype(jnp.float32)
        branch = whole_features(own_sum + received)
        scaled = branch * lax.rsqrt(jnp.mean(branch * branch, axis=1, keepdims=True) + EPSILON)
        return (current.astype(jnp.float32) + weight * (scaled * norm_gains[row])).astype(
            jnp.bfloat16
        )

    def dot(a, b):
        return jnp.dot(a, b, preferred_element_type=jnp.float32)

    def activate(gate_vals, upward):
        return (jax.nn.silu(gate_vals) * upward).astype(jnp.bfloat16)

    current = whole_features(stream)
    normed = norm_own(current, 0)
    normed = jnp.concatenate([normed, norm_other(normed)], axis=0)

    gate_ring = Ring(rep_part(w_gate, 1))
    up_ring = Ring(rep_part(w_up, 1))
    down_own = rep_part(w_down, 0)
    down_ring = Ring(down_own, gate_ring.arrived)
    mix_own = jnp.concatenate([rep_part(w, 1) for w in (w_inner, w_bgate, w_cgate)], axis=1)
    out_own = rep_part(w_out, 0)
    mix_width = mix_own.shape[1]
    mix_ring = Ring(
        jnp.concatenate([mix_own, out_own.reshape(mix_own.shape[0], -1)], axis=1), down_ring.early
    )

    def by_shards(ring):
        size = ring.shards[0].shape[0]
        total = None
        for d in ring.sequence:
            term = dot(lax.dynamic_slice_in_dim(normed, origin[d] * size, size, 1), ring.shards[d])
            total = term if total is None else total + term
        return total

    hidden = activate(by_shards(gate_ring), by_shards(up_ring))
    down_blocks = {d: dot(hidden, down_ring.shards[d]).astype(jnp.bfloat16) for d in down_ring.sequence}
    sums = feature_sum(jnp.concatenate([down_blocks[d] for d in range(count)], axis=1))
    first = settle(current, sums[:rows], sums[rows:], 1, 0.5)

    mix_whole = mix_ring.lined_up(0)[:, :mix_width]
    out_whole = jnp.concatenate(
        [mix_ring.shards[d][:, mix_width:].reshape(out_own.shape) for d in range(count)], axis=1
    )
    channels = mix_width // 3
    taps = rep_part(conv_taps, 1)

    def mix_in(normed_mix):
        product = dot(blocks(normed_mix, origin), mix_whole)
        inner, bgate, cgate = (product[:, i * channels : (i + 1) * channels] for i in range(3))
        return cgate * inner, bgate

    def mix_out(conv_input, bgate, earlier):
        padded = jnp.concatenate([earlier, conv_input], axis=0)
        conv = taps[0] * padded[0:rows]
        for tap in range(1, TAPS):
            conv = conv + taps[tap] * padded[tap : tap + rows]
        return feature_sum(dot((bgate * conv).astype(jnp.bfloat16), out_whole))

    normed_mix = norm_own(first, 2)
    other_mix = norm_other(normed_mix)
    own_in, own_bgate = mix_in(normed_mix)
    other_in, other_bgate = mix_in(other_mix)
    tails = jnp.concatenate([own_in[rows - (TAPS - 1) :], other_in[rows - (TAPS - 1) :]], axis=0)
    earlier = lax.ppermute(tails, "fs", [(i, i + 1) for i in range(count - 1)])
    other_sum = mix_out(other_in, other_bgate, earlier[TAPS - 1 :])
    own_sum = mix_out(own_in, own_bgate, earlier[: TAPS - 1])
    second = settle(first, own_sum, other_sum, 3, 1.0)

    gate_whole, up_whole = gate_ring.lined_up(0), up_ring.lined_up(0)
    down_whole = down_ring.lined_up(1)

    def units(normed_rows):
        lined = blocks(normed_rows, origin)
        return activate(dot(lined, gate_whole), dot(lined, up_whole))

    normed = norm_own(second, 4)
    other_normed = norm_other(normed)
    own_units = units(normed)
    other_sum = feature_sum(dot(units(other_normed), down_whole))
    own_sum = feature_sum(dot(own_units, down_whole))
    return own_features(settle(second, own_sum, other_sum, 5, 0.5))


MESH = pl.DeviceIdType.MESH
GATE, UP, DOWN, MIX = range(4)
Z, X, Y, PART_A, PART_B, Z_OTHER = range(6)
DIRECT = ((8, 0), (4, 0), (8, 0), (8, 0))
BY_Y = (3, 3, 3, 3)
TILE = 512


def aligned(value, to):
    return pl.multiple_of(value, to)


def layer_kernel(
    planes,
    stream, all_gains, w_gate, w_up, w_down, w_inner, w_bgate, w_cgate, all_taps, w_out, out,
    gains, taps, w_mix,
    gate_buf, up_buf, down_buf, mix_buf, raw, normed, hidden, partials, from_core, summed,
    from_pair, current, conv_in, bgates, gated, result,
    local_sem, pack_sem, piece_send, piece_recv, raw_send, raw_recv, core_send, core_recv,
    pair_send, pair_recv, gather_send, gather_recv, halo_send, halo_recv, out_send, out_recv, store_sem,
):
    x, place, core = lax.axis_index("rep"), lax.axis_index("fs"), lax.axis_index("tp")
    z, y = place // 2, place % 2
    pair, member = z // 2, z % 2
    pairs = planes // 2
    rows, width = stream.shape
    quarter = rows // 4
    model_width = 2 * width
    units, channels, mix_width = gate_buf.shape[1], gated.shape[1], mix_buf.shape[1]
    out_cols = mix_width - 3 * channels
    weight_rows = w_gate.shape[0]
    down_cols = w_down.shape[1]
    plane_cols = 2 * down_cols
    buffers = (gate_buf, up_buf, down_buf, mix_buf)
    halves = (weight_rows // 2, weight_rows // 2, units // 2, weight_rows // 2)

    def device(to_x, to_z, to_y, to_core):
        return (to_x, to_z * 2 + to_y, to_core)

    order = [2 * ((pair + j // 2) % pairs) + (member + j) % 2 for j in range(planes)]
    partner = order[1]
    core_peer = device(x, z, y, 1 - core)
    pair_peer = device(x, partner, y, core)
    x_peer, y_peer = device(1 - x, z, y, core), device(x, z, 1 - y, core)

    pending = []

    def send(source, target, send_sem, recv_sem, to):
        copy = pltpu.make_async_remote_copy(
            src_ref=source, dst_ref=target, send_sem=send_sem, recv_sem=recv_sem,
            device_id=to, device_id_type=MESH,
        )
        copy.start()
        pending.append(copy)

    def arrive(target, send_sem, recv_sem):
        pltpu.make_async_remote_copy(
            src_ref=target, dst_ref=target, send_sem=send_sem, recv_sem=recv_sem,
            device_id=core_peer, device_id_type=MESH,
        ).wait_recv()

    def piece(kind, of_z, of_y, of_x, begin=0, end=None):
        half = halves[kind]
        count = (half if end is None else end) - begin
        if kind == DOWN:
            return down_buf.at[of_z * 2 + of_y, pl.ds(aligned(of_x * half + begin, 16), count), :]
        start = ((of_z * 2 + of_y) * 2 + of_x) * half + begin
        return buffers[kind].at[pl.ds(aligned(start, 16), count), :]

    def own_source(kind, side, start, count):
        if kind == DOWN:
            return w_down.at[pl.ds(aligned(side * units + start, 16), count), :]
        cols = mix_width if kind == MIX else units
        source = (w_gate, w_up, None, w_mix)[kind]
        return source.at[pl.ds(aligned(start, 16), count), pl.ds(aligned(side * cols, 128), cols)]

    def piece_copy(source, target, kind, route, of_z, to, index=None):
        index = of_z if index is None else index
        send(source, target, piece_send.at[kind, route, index], piece_recv.at[kind, route, of_z], to)

    def wait_piece(target, kind, route, of_z):
        arrive(target, piece_send.at[kind, route, of_z], piece_recv.at[kind, route, of_z])

    def eighths(half, count):
        return min(half, (half * count // 8 + 15) // 16 * 16)

    def direct(kind, j):
        return eighths(halves[kind], DIRECT[kind][0 if j == 1 else 1])

    def split(kind):
        return halves[kind] - eighths(halves[kind], BY_Y[kind])

    def send_planes(kind, j):
        to, half = order[j], halves[kind]
        piece_copy(
            own_source(kind, to % 2, x * half, half), piece(kind, z, y, x),
            kind, Z, z, device(x, to, y, core), index=to,
        )

    def send_direct(kind, j):
        to, count = order[j], direct(kind, j)
        if count == 0:
            return
        piece_copy(
            own_source(kind, to % 2, (1 - x) * halves[kind], count), piece(kind, z, y, 1 - x, 0, count),
            kind, Z_OTHER, z, device(x, to, y, core), index=to,
        )

    def own_part(kind, i):
        half = halves[kind] // 2
        return i * half, (i + 1) * half

    def send_own(kind):
        for i, route in enumerate((Y, PART_A)):
            begin, end = own_part(kind, i)
            piece_copy(
                own_source(kind, member, x * halves[kind] + begin, end - begin),
                piece(kind, z, y, x, begin, end), kind, route, z, y_peer,
            )

    def pass_own(kind, i):
        part = piece(kind, z, 1 - y, x, *own_part(kind, i))
        wait_piece(part, kind, (Y, PART_A)[i], z)
        piece_copy(part, part, kind, (X, PART_B)[i], z, x_peer)

    def spread(kind, j):
        of = order[j]
        whole = piece(kind, of, y, x)
        wait_piece(whole, kind, Z, of)
        piece_copy(whole, whole, kind, Y, of, y_peer)
        if direct(kind, j) < halves[kind]:
            rest = piece(kind, of, y, x, direct(kind, j), None)
            piece_copy(rest, rest, kind, X, of, x_peer)

    def relay(kind, j):
        of = order[j]
        if direct(kind, j) == halves[kind]:
            wait_piece(piece(kind, of, y, 1 - x), kind, Z_OTHER, of)
        else:
            wait_piece(piece(kind, of, y, 1 - x, direct(kind, j), None), kind, X, of)
        part = piece(kind, of, y, 1 - x, split(kind), None)
        piece_copy(part, part, kind, PART_A, of, y_peer)
        wait_piece(piece(kind, of, 1 - y, x), kind, Y, of)
        part = piece(kind, of, 1 - y, x, 0, split(kind))
        piece_copy(part, part, kind, PART_B, of, x_peer)

    def local_copy(kind):
        count = units if kind == DOWN else weight_rows
        if kind == DOWN:
            target = down_buf.at[z * 2 + y]
        else:
            target = buffers[kind].at[pl.ds(aligned((z * 2 + y) * weight_rows, 16), count), :]
        return pltpu.make_async_copy(own_source(kind, member, 0, count), target, local_sem.at[kind])

    def complete(kind, j):
        of = order[j]
        if j == 0:
            local_copy(kind).wait()
            for i, route in enumerate((X, PART_B)):
                wait_piece(piece(kind, z, 1 - y, 1 - x, *own_part(kind, i)), kind, route, z)
        else:
            if 0 < direct(kind, j) < halves[kind]:
                wait_piece(piece(kind, of, y, 1 - x, 0, direct(kind, j)), kind, Z_OTHER, of)
            wait_piece(piece(kind, of, 1 - y, 1 - x, split(kind), None), kind, PART_A, of)
            wait_piece(piece(kind, of, 1 - y, 1 - x, 0, split(kind)), kind, PART_B, of)

    own_raw = raw.at[pl.ds(aligned(member * rows, 16), rows), pl.ds(aligned(core * width, 128), width)]
    packs = []
    for side in range(2):
        base = side * mix_width
        for n, weight in enumerate((w_inner, w_bgate, w_cgate)):
            packs.append((
                weight.at[:, side * channels : (side + 1) * channels],
                w_mix.at[:, base + n * channels : base + (n + 1) * channels],
            ))
        packs.append((
            w_out.at[side * channels : (side + 1) * channels, :],
            w_mix.at[:, base + 3 * channels : base + mix_width],
        ))
    packs += [(all_gains, gains), (all_taps, taps)]
    packs = [pltpu.make_async_copy(a, b, pack_sem.at[n]) for n, (a, b) in enumerate(packs)]
    for copy in packs:
        copy.start()
    raw_copy = pltpu.make_async_copy(stream, own_raw, local_sem.at[4])
    raw_copy.start()
    for kind in (GATE, UP, DOWN):
        local_copy(kind).start()

    first_segment = (y == 0) & (pair == 0)

    @pl.when(first_segment)
    def _():
        conv_in[0, 0:8, :] = jnp.zeros((8, channels), jnp.float32)

    barrier = pltpu.get_barrier_semaphore()
    greeted = [core_peer, x_peer, y_peer]
    greeted += [device(x, order[j], y, core) for j in range(1, planes)]
    greeted += [device(x, (z + s) % planes, 1 - y, core) for s in sorted({2, planes - 2})]
    for peer in greeted:
        pl.semaphore_signal(barrier, inc=1, device_id=peer, device_id_type=MESH)
    pl.semaphore_wait(barrier, len(greeted))

    others = range(1, planes)
    send_own(GATE)
    for j in others:
        send_planes(GATE, j)
    send_own(UP)
    send_own(DOWN)
    send(stream, own_raw, raw_send.at[0], raw_recv.at[0], core_peer)
    for j in others:
        send_direct(GATE, j)
    for copy in packs:
        copy.wait()
    local_copy(MIX).start()
    send_own(MIX)

    def rms(values):
        return values * lax.rsqrt(jnp.mean(values * values, axis=1, keepdims=True) + EPSILON)

    step_rows = 16

    def norm_all():
        @pl.loop(0, 2 * rows // step_rows)
        def _(i):
            at = pl.ds(aligned(i * step_rows, 16), step_rows)
            values = raw[at, :].astype(jnp.float32)
            normed[0, at, :] = (rms(values) * gains[0:1, :]).astype(jnp.bfloat16)

    def dot(a, b):
        return jnp.dot(a, b, preferred_element_type=jnp.float32)

    tile = TILE

    def hidden_tiles(which, start, row_count, first, last):
        at = pl.ds(aligned(start, 128), row_count)

        def columns(begin, count):
            cols = pl.ds(aligned(begin, 128), count)
            gate = dot(normed[which, at, :], gate_buf[:, cols])
            up = dot(normed[which, at, :], up_buf[:, cols])
            hidden[at, cols] = (gate / (1.0 + jnp.exp(-gate)) * up).astype(jnp.bfloat16)

        whole = min(last, units // tile)

        @pl.loop(first, whole)
        def _(n):
            columns(n * tile, tile)

        if whole < last:
            columns(whole * tile, units - whole * tile)

    tiles = pl.cdiv(units, tile)

    def hidden_rows(which, start, row_count):
        hidden_tiles(which, start, row_count, 0, tiles)

    def down_rows(phase, start, row_count, of_z):
        at = pl.ds(aligned(start, 128), row_count)

        for s in range(2):
            cols = pl.ds(aligned((of_z * 2 + s) * down_cols, 128), down_cols)
            partials[phase, at, cols] = dot(hidden[at, :], down_buf[of_z * 2 + s]).astype(jnp.bfloat16)

    def owned(of_member, of_core, part):
        return of_member * rows + part * 2 * quarter + of_core * quarter

    def owned_rows(of_member, of_core, part):
        return pl.ds(aligned(owned(of_member, of_core, part), 16), quarter)

    def local_rows(part):
        return pl.ds(part * quarter, quarter)

    def plane_of(of_z):
        return pl.ds(aligned(of_z * plane_cols, 128), plane_cols)

    def send_core(phase, of_member, part, of_z):
        send(
            partials.at[phase, owned_rows(of_member, 1 - core, part), plane_of(of_z)],
            from_core.at[phase, of_member, local_rows(part), plane_of(of_z)],
            core_send.at[phase, of_member, part, of_z], core_recv.at[phase, of_member, part, of_z],
            core_peer,
        )

    def wait_core(phase, of_member, part, of_z):
        arrive(
            from_core.at[phase, of_member, local_rows(part), plane_of(of_z)],
            core_send.at[phase, of_member, part, of_z], core_recv.at[phase, of_member, part, of_z],
        )

    def send_pair(phase, part, of_z):
        wait_core(phase, 1 - member, part, of_z)
        at, cols = local_rows(part), plane_of(of_z)
        mine = partials[phase, owned_rows(1 - member, core, part), cols].astype(jnp.float32)
        theirs = from_core[phase, 1 - member, at, cols].astype(jnp.float32)
        summed[phase, at, cols] = (mine + theirs).astype(jnp.bfloat16)
        send(
            summed.at[phase, at, cols], from_pair.at[phase, at, cols],
            pair_send.at[phase, part, of_z], pair_recv.at[phase, part, of_z], pair_peer,
        )

    def wait_pair(phase, part):
        for of_z in order:
            wait_core(phase, member, part, of_z)
            arrive(
                from_pair.at[phase, local_rows(part), plane_of(of_z)],
                pair_send.at[phase, part, of_z], pair_recv.at[phase, part, of_z],
            )

    def settle(phase, gain, weight, source, target, next_gain, part):
        @pl.loop(0, quarter // step_rows)
        def _(i):
            at = pl.ds(aligned(part * quarter + i * step_rows, 16), step_rows)
            mine = pl.ds(aligned(owned(member, core, part) + i * step_rows, 16), step_rows)
            branch = (
                partials[phase, mine, :].astype(jnp.float32)
                + from_core[phase, member, at, :].astype(jnp.float32)
                + from_pair[phase, at, :].astype(jnp.float32)
            )
            before = source[mine if phase == 0 else at, :]
            after = before.astype(jnp.float32) + weight * (rms(branch) * gains[gain : gain + 1, :])
            rounded = after.astype(jnp.bfloat16)
            target[at, :] = rounded
            if next_gain is not None:
                scaled = rms(rounded.astype(jnp.float32)) * gains[next_gain : next_gain + 1, :]
                normed[phase + 1, mine, :] = scaled.astype(jnp.bfloat16)

    def gather_ref(which, of_member, of_core, part):
        return normed.at[which, owned_rows(of_member, of_core, part), :]

    def gather_start(which, part):
        mine = gather_ref(which, member, core, part)
        send(mine, mine, gather_send.at[which, 1, part], gather_recv.at[which, 1, part], pair_peer)
        send(mine, mine, gather_send.at[which, 0, part], gather_recv.at[which, 0, part], core_peer)

    def gather_own(which, part):
        arrive(
            gather_ref(which, member, 1 - core, part),
            gather_send.at[which, 0, part], gather_recv.at[which, 0, part],
        )

    def gather_pass(which, part):
        theirs = gather_ref(which, 1 - member, core, part)
        arrive(theirs, gather_send.at[which, 1, part], gather_recv.at[which, 1, part])
        send(theirs, theirs, gather_send.at[which, 2, part], gather_recv.at[which, 2, part], core_peer)

    def gather_pair(which, part):
        arrive(
            gather_ref(which, 1 - member, 1 - core, part),
            gather_send.at[which, 2, part], gather_recv.at[which, 2, part],
        )

    head = 8

    def mix_in(s, begin, count):
        at = pl.ds(aligned(s * rows + begin, 128), count)
        inner = dot(normed[1, at, :], mix_buf[:, 0:channels])
        cgate = dot(normed[1, at, :], mix_buf[:, 2 * channels : 3 * channels])
        conv_in[s, head + begin : head + begin + count, :] = cgate * inner
        bgates[s, begin : begin + count, :] = dot(
            normed[1, at, :], mix_buf[:, channels : 2 * channels]
        )

    def halo(source, target, to):
        return pltpu.make_async_remote_copy(
            src_ref=conv_in.at[source, rows : rows + head, :],
            dst_ref=conv_in.at[target, 0:head, :],
            send_sem=halo_send.at[source], recv_sem=halo_recv.at[target],
            device_id=to, device_id_type=MESH,
        )

    def near_tail(s):
        return halo(s, y + s * (1 - y), y_peer)

    def far_tail(s):
        return halo(s, 0, device(x, (z + 2) % planes, 0, core))

    def tails(s, act):
        @pl.when((s == 0) | (y == 0))
        def _():
            act(near_tail(s))

        @pl.when((s == 1) & (y == 1) & (pair < pairs - 1))
        def _():
            act(far_tail(s))

    def mix_gate(s, part):
        if part == 0:
            @pl.when(jnp.logical_not(first_segment & (s == 0)))
            def _():
                halo(s, s, y_peer).wait_recv()

        count = 2 * quarter
        total = None
        for tap in range(TAPS):
            begin = head - TAPS + 1 + tap + part * count
            shifted = conv_in[s, begin : begin + count, :]
            scale = taps[tap : tap + 1, pl.ds(aligned(member * channels, 128), channels)]
            total = scale * shifted if total is None else total + scale * shifted
        bgate = bgates[s, part * count : (part + 1) * count, :]
        at = pl.ds(aligned(s * rows + part * count, 128), count)
        gated[at, :] = (bgate * total).astype(jnp.bfloat16)

    def mix_out(s, part, of_z):
        at = pl.ds(aligned(s * rows + part * 2 * quarter, 128), 2 * quarter)

        for n in range(2):
            index = of_z * 2 + n
            cols = pl.ds(aligned(index * out_cols, 128), out_cols)
            weight = mix_buf[pl.ds(aligned(index * weight_rows, 128), channels), 3 * channels :]
            partials[1, at, cols] = dot(gated[at, :], weight).astype(jnp.bfloat16)

    def core_parts(phase, of_member, part):
        for of_z in order:
            send_core(phase, of_member, part, of_z)

    for kind, i in ((GATE, 0), (GATE, 1), (UP, 0), (UP, 1)):
        pass_own(kind, i)
    for j in others:
        spread(GATE, j)
        send_planes(UP, j)
        if j <= 2:
            pass_own(DOWN, j - 1)
    pass_own(MIX, 0)
    pass_own(MIX, 1)
    send(stream, own_raw, raw_send.at[1], raw_recv.at[1], pair_peer)
    for j in others:
        send_direct(UP, j)
    for j in others:
        relay(GATE, j)
    for j in others:
        spread(UP, j)
        send_planes(DOWN, j)
    for j in others:
        send_direct(DOWN, j)
    relay(UP, 1)
    raw_copy.wait()

    def raw_at(of_member, of_core):
        return raw.at[
            pl.ds(aligned(of_member * rows, 16), rows), pl.ds(aligned(of_core * width, 128), width)
        ]

    arrive(raw_at(member, 1 - core), raw_send.at[0], raw_recv.at[0])
    pair_raw = raw_at(1 - member, core)
    arrive(pair_raw, raw_send.at[1], raw_recv.at[1])
    send(pair_raw, pair_raw, raw_send.at[2], raw_recv.at[2], core_peer)
    for j in range(2, planes):
        relay(UP, j)
    for j in others:
        spread(DOWN, j)
        send_planes(MIX, j)
    for j in others:
        send_direct(MIX, j)
    arrive(raw_at(1 - member, 1 - core), raw_send.at[2], raw_recv.at[2])
    norm_all()
    for kind in (GATE, UP):
        for j in range(planes):
            complete(kind, j)
    for j in others:
        hidden_tiles(0, 0, 2 * rows, tiles * (j - 1) // (planes - 1), tiles * j // (planes - 1))
        relay(DOWN, j)
    for j in range(planes):
        if j > 0:
            spread(MIX, j)
        complete(DOWN, j)

        @pl.loop(0, 2)
        def _(r):
            down_rows(0, r * rows, rows, order[j])

        for of_member in (1 - member, member):
            for part in (1, 0):
                send_core(0, of_member, part, order[j])
        if j > 0:
            for part in (1, 0):
                send_pair(0, part, order[j - 1])
    for part in (1, 0):
        send_pair(0, part, order[planes - 1])
    for part in (1, 0):
        wait_pair(0, part)
        settle(0, 1, 0.5, raw, current, 2, part)
        gather_start(1, part)
    for j in others:
        relay(MIX, j)
    gather_own(1, 1)
    gather_own(1, 0)
    gather_pass(1, 1)
    for j in range(planes):
        complete(MIX, j)
    mix_in(member, 0, rows)
    tails(member, lambda copy: copy.start())
    gather_pass(1, 0)
    gather_pair(1, 1)
    mix_in(1 - member, 2 * quarter, 2 * quarter)
    tails(1 - member, lambda copy: copy.start())
    gather_pair(1, 0)
    mix_in(1 - member, 0, 2 * quarter)
    mix_gate(1 - member, 1)
    for of_z in order:
        mix_out(1 - member, 1, of_z)
        send_core(1, 1 - member, 1, of_z)
    mix_gate(1 - member, 0)
    for of_z in order:
        mix_out(1 - member, 0, of_z)
        send_core(1, 1 - member, 0, of_z)
        send_pair(1, 1, of_z)
    mix_gate(member, 1)
    for of_z in order:
        mix_out(member, 1, of_z)
        send_core(1, member, 1, of_z)
        send_pair(1, 0, of_z)
    mix_gate(member, 0)
    for of_z in order:
        mix_out(member, 0, of_z)
        send_core(1, member, 0, of_z)
    for part in (1, 0):
        wait_pair(1, part)
        settle(1, 3, 1.0, current, current, 4, part)
        gather_start(2, part)
        gather_own(2, part)
        hidden_rows(2, member * rows + part * 2 * quarter, 2 * quarter)
    gather_pass(2, 1)
    down_rows(2, member * rows, rows, order[0])
    gather_pair(2, 1)
    start = (1 - member) * rows
    hidden_rows(2, start + 2 * quarter, 2 * quarter)
    gather_pass(2, 0)
    for j in range(planes):
        down_rows(2, start + 2 * quarter, 2 * quarter, order[j])
        send_core(2, 1 - member, 1, order[j])
        if j > 1:
            send_pair(2, 1, order[j - 2])
    gather_pair(2, 0)
    hidden_rows(2, start, 2 * quarter)
    for j in range(2):
        send_pair(2, 1, order[planes - 2 + j])
    for j in range(planes):
        down_rows(2, start, 2 * quarter, order[j])
        send_core(2, 1 - member, 0, order[j])
        if j > 1:
            send_pair(2, 0, order[j - 2])
    down_rows(2, member * rows, rows, order[1])
    for j in range(2):
        send_pair(2, 0, order[planes - 2 + j])
    for j in range(2, planes):
        down_rows(2, member * rows, rows, order[j])
    for part in (1, 0):
        core_parts(2, member, part)
    stores = [None, None]
    for part in (1, 0):
        wait_pair(2, part)
        settle(2, 5, 0.5, current, result, None, part)
        there = pl.ds(aligned(part * 2 * quarter + core * quarter, 16), quarter)
        send(
            result.at[local_rows(part), pl.ds(aligned((1 - core) * width, 128), width)],
            out.at[there, :], out_send.at[part], out_recv.at[part], core_peer,
        )
        store = pltpu.make_async_copy(
            result.at[local_rows(part), pl.ds(aligned(core * width, 128), width)],
            out.at[there, :], store_sem.at[part],
        )
        store.start()
        stores[part] = store
    for part in range(2):
        stores[part].wait()
        theirs = pl.ds(aligned(part * 2 * quarter + (1 - core) * quarter, 16), quarter)
        arrive(out.at[theirs, :], out_send.at[part], out_recv.at[part])
    for copy in pending:
        copy.wait_send()
    for s in range(2):
        tails(s, lambda copy: copy.wait_send())


def fits_kernel(mesh, stream, w_gate, w_down, w_inner, w_out):
    planes = mesh.shape["fs"] // 2
    return (
        mesh.shape["tp"] == 2
        and mesh.shape["rep"] == 2
        and mesh.shape["fs"] % 4 == 0
        and planes >= 4
        and w_gate.shape[0] == w_inner.shape[0] == w_out.shape[0] // 2
        and stream.shape[0] % 256 == 0
        and w_gate.shape[0] % 256 == 0
        and w_gate.shape[1] % 256 == 0
        and w_inner.shape[1] % 256 == 0
        and w_down.shape[1] % 128 == 0
    )


def fused(stream, norm_gains, w_gate, w_up, w_down, w_inner, w_bgate, w_cgate, conv_taps, w_out):
    count = lax.axis_size("fs")
    planes = count // 2
    rows, width = stream.shape
    model_width = 2 * width
    weight_rows, units = w_gate.shape[0], w_gate.shape[1] // 2
    channels, down_cols, out_cols = w_inner.shape[1] // 2, w_down.shape[1], w_out.shape[1]
    own_rows = rows // 2
    mix_width = 3 * channels + out_cols
    bf16, f32 = jnp.bfloat16, jnp.float32
    vmem, dma = pltpu.VMEM, pltpu.SemaphoreType.DMA
    anywhere = pl.BlockSpec(memory_space=pl.ANY)
    flops = 2 * 2 * rows * (6 * model_width * units + 4 * model_width * channels)
    return pl.pallas_call(
        functools.partial(layer_kernel, planes),
        out_shape=jax.ShapeDtypeStruct((rows, width), bf16),
        in_specs=[anywhere] * 10,
        out_specs=anywhere,
        scratch_shapes=[
            vmem(norm_gains.shape, f32),
            vmem(conv_taps.shape, f32),
            vmem((weight_rows, 2 * mix_width), bf16),
            vmem((model_width, units), bf16),
            vmem((model_width, units), bf16),
            vmem((count, units, down_cols), bf16),
            vmem((model_width, mix_width), bf16),
            vmem((2 * rows, model_width), bf16),
            vmem((3, 2 * rows, model_width), bf16),
            vmem((2 * rows, units), bf16),
            vmem((3, 2 * rows, model_width), bf16),
            vmem((3, 2, own_rows, model_width), bf16),
            vmem((3, own_rows, model_width), bf16),
            vmem((3, own_rows, model_width), bf16),
            vmem((own_rows, model_width), bf16),
            vmem((2, 8 + rows, channels), f32),
            vmem((2, rows, channels), f32),
            vmem((2 * rows, channels), bf16),
            vmem((own_rows, model_width), bf16),
            dma((5,)),
            dma((10,)),
            dma((4, 6, planes)),
            dma((4, 6, planes)),
            dma((3,)),
            dma((3,)),
            dma((3, 2, 2, planes)),
            dma((3, 2, 2, planes)),
            dma((3, 2, planes)),
            dma((3, 2, planes)),
            dma((3, 3, 2)),
            dma((3, 3, 2)),
            dma((2,)),
            dma((2,)),
            dma((2,)),
            dma((2,)),
            dma((2,)),
        ],
        cost_estimate=pl.CostEstimate(
            flops=flops, bytes_accessed=4 * w_gate.size * 2, transcendentals=4 * rows * units
        ),
        compiler_params=pltpu.CompilerParams(
            collective_id=0, has_side_effects=True, vmem_limit_bytes=60 * 1024 * 1024
        ),
        name="layer",
    )(stream, norm_gains, w_gate, w_up, w_down, w_inner, w_bgate, w_cgate, conv_taps, w_out)


def solution(mesh):
    def body(stream, norm_gains, w_gate, w_up, w_down, w_inner, w_bgate, w_cgate, conv_taps, w_out):
        arguments = (stream, norm_gains, w_gate, w_up, w_down, w_inner, w_bgate, w_cgate, conv_taps, w_out)
        if fits_kernel(mesh, stream, w_gate, w_down, w_inner, w_out):
            return fused(*arguments)
        return shards(*arguments)

    return jax.shard_map(
        body,
        mesh=mesh,
        in_specs=(
            P(("rep", "fs"), "tp"),
            P(),
            P("fs", "tp"),
            P("fs", "tp"),
            P("tp", "fs"),
            P("fs", "tp"),
            P("fs", "tp"),
            P("fs", "tp"),
            P(None, "tp"),
            P("tp", "fs"),
        ),
        out_specs=P(("rep", "fs"), "tp"),
        check_vma=False,
    )
```

```python
import functools

import jax
import jax.numpy as jnp
from jax import lax
from jax.experimental import pallas as pl
from jax.experimental.pallas import tpu as pltpu
from jax.sharding import PartitionSpec as P

TAPS = 3
EPSILON = 1e-06


def ring_order(count):
    return list(range(0, count, 2)) + list(range(1, count, 2))[::-1]


def swap(x, axis):
    return lax.ppermute(x, axis, [(0, 1), (1, 0)])


def copy_blocks(count, size, starts, source, target):
    for i in range(count):
        begin = pl.multiple_of(starts[i] * size, size)
        target[:, i * size : (i + 1) * size] = source[:, pl.ds(begin, size)]


def permuted(x, starts, size):
    return pl.pallas_call(
        functools.partial(copy_blocks, len(starts), size),
        in_specs=[
            pl.BlockSpec(memory_space=pltpu.SMEM),
            pl.BlockSpec(memory_space=pltpu.VMEM),
        ],
        out_specs=pl.BlockSpec(memory_space=pltpu.VMEM),
        out_shape=jax.ShapeDtypeStruct(x.shape, x.dtype),
        cost_estimate=pl.CostEstimate(flops=0, bytes_accessed=2 * x.size * x.dtype.itemsize, transcendentals=0),
        compiler_params=pltpu.CompilerParams(vmem_limit_bytes=3 * x.size * x.dtype.itemsize),
    )(jnp.stack(starts), x)


class Ring:
    def __init__(self, own, after=None):
        count = lax.axis_size("fs")
        order = ring_order(count)
        onward = [(order[i], order[(i + 1) % count]) for i in range(count)]
        back = [(b, a) for a, b in onward]
        half = count // 2
        first, second = own, own
        if after is not None:
            first, _ = lax.optimization_barrier((own, after[0]))
            second, _ = lax.optimization_barrier((own, after[1]))
        rows = own.shape[0] // 2
        self.shards = {0: own}
        self.arrived = self.early = (own, own)
        for step in range(1, half):
            first = lax.ppermute(first, "fs", onward)
            second = lax.ppermute(second, "fs", back)
            self.shards[step] = first
            self.shards[count - step] = second
            self.arrived = (first, second)
            if step == 1:
                self.early = self.arrived
        self.last = (
            lax.ppermute(first[:rows], "fs", onward),
            lax.ppermute(second[rows:], "fs", back),
        )
        self.shards[half] = jnp.concatenate(self.last, axis=0)
        self.sequence = [0]
        for step in range(1, half):
            self.sequence += [step, count - step]
        self.sequence += [half]

    def lined_up(self, axis):
        return jnp.concatenate([self.shards[d] for d in range(len(self.shards))], axis=axis)


def shards(stream, norm_gains, w_gate, w_up, w_down, w_inner, w_bgate, w_cgate, conv_taps, w_out):
    count, tp = lax.axis_size("fs"), lax.axis_size("tp")
    tp_index, rep_index, fs_index = lax.axis_index("tp"), lax.axis_index("rep"), lax.axis_index("fs")
    rows, width = stream.shape
    model_width = width * tp
    order = ring_order(count)
    places = [order.index(i) for i in range(count)]
    place = jnp.array(places, jnp.int32)[fs_index]
    origin = [
        jnp.array(order, jnp.int32)[lax.rem(place - d + count, count)] for d in range(count)
    ]

    behind = [
        lax.rem(place - places[i] + count, count) for i in range(count)
    ]

    def blocks(x, starts):
        size = x.shape[1] // count
        if size % 128 == 0:
            return permuted(x, starts, size)
        return jnp.concatenate(
            [lax.dynamic_slice_in_dim(x, start * size, size, 1) for start in starts], axis=1
        )

    def rep_part(w, axis):
        size = w.shape[axis] // lax.axis_size("rep")
        return lax.dynamic_slice_in_dim(w, rep_index * size, size, axis)

    def whole_features(x):
        if tp != 2:
            return lax.all_gather(x, "tp", axis=1, tiled=True)
        other = swap(x, "tp")
        mine = tp_index == 0
        return jnp.concatenate([jnp.where(mine, x, other), jnp.where(mine, other, x)], axis=1)

    def own_features(x):
        return lax.dynamic_slice_in_dim(x, tp_index * width, width, 1)

    def feature_sum(partials):
        rounded = blocks(partials.astype(jnp.bfloat16), behind)
        if tp != 2:
            return lax.psum_scatter(rounded, "tp", scatter_dimension=1, tiled=True).astype(jnp.float32)
        theirs = lax.dynamic_slice_in_dim(rounded, (1 - tp_index) * width, width, 1)
        received = swap(theirs, "tp").astype(jnp.float32)
        return own_features(rounded).astype(jnp.float32) + received

    def norm_own(current, row):
        values = current.astype(jnp.float32)
        scaled = values * lax.rsqrt(jnp.mean(values * values, axis=1, keepdims=True) + EPSILON)
        return (scaled * norm_gains[row]).astype(jnp.bfloat16)

    def norm_other(normed):
        return whole_features(swap(own_features(normed), "rep"))

    def settle(current, own_sum, other_sum, row, weight):
        received = swap(other_sum.astype(jnp.bfloat16), "rep").astype(jnp.float32)
        branch = whole_features(own_sum + received)
        scaled = branch * lax.rsqrt(jnp.mean(branch * branch, axis=1, keepdims=True) + EPSILON)
        return (current.astype(jnp.float32) + weight * (scaled * norm_gains[row])).astype(
            jnp.bfloat16
        )

    def dot(a, b):
        return jnp.dot(a, b, preferred_element_type=jnp.float32)

    def activate(gate_vals, upward):
        return (jax.nn.silu(gate_vals) * upward).astype(jnp.bfloat16)

    current = whole_features(stream)
    normed = norm_own(current, 0)
    normed = jnp.concatenate([normed, norm_other(normed)], axis=0)

    gate_ring = Ring(rep_part(w_gate, 1))
    up_ring = Ring(rep_part(w_up, 1))
    down_own = rep_part(w_down, 0)
    down_ring = Ring(down_own, gate_ring.arrived)
    mix_own = jnp.concatenate([rep_part(w, 1) for w in (w_inner, w_bgate, w_cgate)], axis=1)
    out_own = rep_part(w_out, 0)
    mix_width = mix_own.shape[1]
    mix_ring = Ring(
        jnp.concatenate([mix_own, out_own.reshape(mix_own.shape[0], -1)], axis=1), down_ring.early
    )

    def by_shards(ring):
        size = ring.shards[0].shape[0]
        total = None
        for d in ring.sequence:
            term = dot(lax.dynamic_slice_in_dim(normed, origin[d] * size, size, 1), ring.shards[d])
            total = term if total is None else total + term
        return total

    hidden = activate(by_shards(gate_ring), by_shards(up_ring))
    down_blocks = {d: dot(hidden, down_ring.shards[d]).astype(jnp.bfloat16) for d in down_ring.sequence}
    sums = feature_sum(jnp.concatenate([down_blocks[d] for d in range(count)], axis=1))
    first = settle(current, sums[:rows], sums[rows:], 1, 0.5)

    mix_whole = mix_ring.lined_up(0)[:, :mix_width]
    out_whole = jnp.concatenate(
        [mix_ring.shards[d][:, mix_width:].reshape(out_own.shape) for d in range(count)], axis=1
    )
    channels = mix_width // 3
    taps = rep_part(conv_taps, 1)

    def mix_in(normed_mix):
        product = dot(blocks(normed_mix, origin), mix_whole)
        inner, bgate, cgate = (product[:, i * channels : (i + 1) * channels] for i in range(3))
        return cgate * inner, bgate

    def mix_out(conv_input, bgate, earlier):
        padded = jnp.concatenate([earlier, conv_input], axis=0)
        conv = taps[0] * padded[0:rows]
        for tap in range(1, TAPS):
            conv = conv + taps[tap] * padded[tap : tap + rows]
        return feature_sum(dot((bgate * conv).astype(jnp.bfloat16), out_whole))

    normed_mix = norm_own(first, 2)
    other_mix = norm_other(normed_mix)
    own_in, own_bgate = mix_in(normed_mix)
    other_in, other_bgate = mix_in(other_mix)
    tails = jnp.concatenate([own_in[rows - (TAPS - 1) :], other_in[rows - (TAPS - 1) :]], axis=0)
    earlier = lax.ppermute(tails, "fs", [(i, i + 1) for i in range(count - 1)])
    other_sum = mix_out(other_in, other_bgate, earlier[TAPS - 1 :])
    own_sum = mix_out(own_in, own_bgate, earlier[: TAPS - 1])
    second = settle(first, own_sum, other_sum, 3, 1.0)

    gate_whole, up_whole = gate_ring.lined_up(0), up_ring.lined_up(0)
    down_whole = down_ring.lined_up(1)

    def units(normed_rows):
        lined = blocks(normed_rows, origin)
        return activate(dot(lined, gate_whole), dot(lined, up_whole))

    normed = norm_own(second, 4)
    other_normed = norm_other(normed)
    own_units = units(normed)
    other_sum = feature_sum(dot(units(other_normed), down_whole))
    own_sum = feature_sum(dot(own_units, down_whole))
    return own_features(settle(second, own_sum, other_sum, 5, 0.5))


MESH = pl.DeviceIdType.MESH
GATE, UP, DOWN, MIX = range(4)
Z, X, Y, PART_A, PART_B, Z_OTHER = range(6)
DIRECT = ((8, 0), (4, 0), (8, 0), (8, 0))
BY_Y = (3, 3, 3, 3)
TILE = 512
LATE = 1


def aligned(value, to):
    return pl.multiple_of(value, to)


def layer_kernel(
    planes,
    stream, all_gains, w_gate, w_up, w_down, w_inner, w_bgate, w_cgate, all_taps, w_out, out,
    gains, taps, w_mix,
    gate_buf, up_buf, down_buf, mix_buf, raw, normed, hidden, partials, from_core, summed,
    from_pair, current, conv_in, mix_sum, gated, result,
    local_sem, pack_sem, piece_send, piece_recv, raw_send, raw_recv, core_send, core_recv,
    pair_send, pair_recv, gather_send, gather_recv, halo_send, halo_recv, out_send, out_recv, store_sem,
):
    x, place, core = lax.axis_index("rep"), lax.axis_index("fs"), lax.axis_index("tp")
    z, y = place // 2, place % 2
    pair, member = z // 2, z % 2
    pairs = planes // 2
    rows, width = stream.shape
    quarter = rows // 4
    model_width = 2 * width
    units, channels, mix_width = gate_buf.shape[1], gated.shape[1], mix_buf.shape[1]
    out_cols = mix_width - 3 * channels
    weight_rows = w_gate.shape[0]
    down_cols = w_down.shape[1]
    plane_cols = 2 * down_cols
    buffers = (gate_buf, up_buf, down_buf, mix_buf)
    halves = (weight_rows // 2, weight_rows // 2, units // 2, weight_rows // 2)

    def device(to_x, to_z, to_y, to_core):
        return (to_x, to_z * 2 + to_y, to_core)

    order = [2 * ((pair + j // 2) % pairs) + (member + j) % 2 for j in range(planes)]
    ranks = {id(of_z): j for j, of_z in enumerate(order)}
    partner = order[1]
    core_peer = device(x, z, y, 1 - core)
    pair_peer = device(x, partner, y, core)
    x_peer, y_peer = device(1 - x, z, y, core), device(x, z, 1 - y, core)

    pending = {}

    def send(source, target, sems, slot, recv_sem, to):
        key = (id(sems),) + slot
        if key in pending:
            pending[key].wait_send()
        send_sem = sems.at[slot]
        copy = pltpu.make_async_remote_copy(
            src_ref=source, dst_ref=target, send_sem=send_sem, recv_sem=recv_sem,
            device_id=to, device_id_type=MESH,
        )
        copy.start()
        pending[key] = copy

    def arrive(target, recv_sem):
        pltpu.make_async_remote_copy(
            src_ref=target, dst_ref=target, send_sem=raw_send.at[0], recv_sem=recv_sem,
            device_id=core_peer, device_id_type=MESH,
        ).wait_recv()

    def piece(kind, of_z, of_y, of_x, begin=0, end=None):
        half = halves[kind]
        count = (half if end is None else end) - begin
        if kind == DOWN:
            return down_buf.at[of_z * 2 + of_y, pl.ds(aligned(of_x * half + begin, 16), count), :]
        start = ((of_z * 2 + of_y) * 2 + of_x) * half + begin
        return buffers[kind].at[pl.ds(aligned(start, 16), count), :]

    def own_source(kind, side, start, count):
        if kind == DOWN:
            return w_down.at[pl.ds(aligned(side * units + start, 16), count), :]
        cols = mix_width if kind == MIX else units
        source = (w_gate, w_up, None, w_mix)[kind]
        return source.at[pl.ds(aligned(start, 16), count), pl.ds(aligned(side * cols, 128), cols)]

    def piece_copy(source, target, kind, route, j, of_z, to):
        send(source, target, piece_send, (kind % 2, route, j), piece_recv.at[kind, route, of_z], to)

    def wait_piece(target, kind, route, of_z):
        arrive(target, piece_recv.at[kind, route, of_z])

    def eighths(half, count):
        return min(half, (half * count // 8 + 15) // 16 * 16)

    def direct(kind, j):
        return eighths(halves[kind], DIRECT[kind][0 if j == 1 else 1])

    def split(kind):
        return halves[kind] - eighths(halves[kind], BY_Y[kind])

    def send_planes(kind, j):
        to, half = order[j], halves[kind]
        piece_copy(
            own_source(kind, to % 2, x * half, half), piece(kind, z, y, x),
            kind, Z, j, z, device(x, to, y, core),
        )

    def send_direct(kind, j):
        to, count = order[j], direct(kind, j)
        if count == 0:
            return
        piece_copy(
            own_source(kind, to % 2, (1 - x) * halves[kind], count), piece(kind, z, y, 1 - x, 0, count),
            kind, Z_OTHER, j, z, device(x, to, y, core),
        )

    def own_part(kind, i):
        half = halves[kind] // 2
        return i * half, (i + 1) * half

    def send_own(kind):
        for i, route in enumerate((Y, PART_A)):
            begin, end = own_part(kind, i)
            piece_copy(
                own_source(kind, member, x * halves[kind] + begin, end - begin),
                piece(kind, z, y, x, begin, end), kind, route, 0, z, y_peer,
            )

    def pass_own(kind, i):
        part = piece(kind, z, 1 - y, x, *own_part(kind, i))
        wait_piece(part, kind, (Y, PART_A)[i], z)
        piece_copy(part, part, kind, (X, PART_B)[i], 0, z, x_peer)

    def spread(kind, j):
        of = order[j]
        whole = piece(kind, of, y, x)
        wait_piece(whole, kind, Z, of)
        piece_copy(whole, whole, kind, Y, j, of, y_peer)
        if direct(kind, j) < halves[kind]:
            rest = piece(kind, of, y, x, direct(kind, j), None)
            piece_copy(rest, rest, kind, X, j, of, x_peer)

    def relay(kind, j):
        of = order[j]
        if direct(kind, j) == halves[kind]:
            wait_piece(piece(kind, of, y, 1 - x), kind, Z_OTHER, of)
        else:
            wait_piece(piece(kind, of, y, 1 - x, direct(kind, j), None), kind, X, of)
        part = piece(kind, of, y, 1 - x, split(kind), None)
        piece_copy(part, part, kind, PART_A, j, of, y_peer)
        wait_piece(piece(kind, of, 1 - y, x), kind, Y, of)
        part = piece(kind, of, 1 - y, x, 0, split(kind))
        piece_copy(part, part, kind, PART_B, j, of, x_peer)

    def local_copy(kind):
        count = units if kind == DOWN else weight_rows
        if kind == DOWN:
            target = down_buf.at[z * 2 + y]
        else:
            target = buffers[kind].at[pl.ds(aligned((z * 2 + y) * weight_rows, 16), count), :]
        return pltpu.make_async_copy(own_source(kind, member, 0, count), target, local_sem.at[kind])

    def complete(kind, j):
        of = order[j]
        if j == 0:
            local_copy(kind).wait()
            for i, route in enumerate((X, PART_B)):
                wait_piece(piece(kind, z, 1 - y, 1 - x, *own_part(kind, i)), kind, route, z)
        else:
            if 0 < direct(kind, j) < halves[kind]:
                wait_piece(piece(kind, of, y, 1 - x, 0, direct(kind, j)), kind, Z_OTHER, of)
            wait_piece(piece(kind, of, 1 - y, 1 - x, split(kind), None), kind, PART_A, of)
            wait_piece(piece(kind, of, 1 - y, 1 - x, 0, split(kind)), kind, PART_B, of)

    own_raw = raw.at[pl.ds(aligned(member * rows, 16), rows), pl.ds(aligned(core * width, 128), width)]
    packs = []
    for side in range(2):
        base = side * mix_width
        for n, weight in enumerate((w_inner, w_bgate, w_cgate)):
            packs.append((
                weight.at[:, side * channels : (side + 1) * channels],
                w_mix.at[:, base + n * channels : base + (n + 1) * channels],
            ))
        packs.append((
            w_out.at[side * channels : (side + 1) * channels, :],
            w_mix.at[:, base + 3 * channels : base + mix_width],
        ))
    packs += [(all_gains, gains), (all_taps, taps)]
    packs = [pltpu.make_async_copy(a, b, pack_sem.at[n]) for n, (a, b) in enumerate(packs)]
    for copy in packs:
        copy.start()
    raw_copy = pltpu.make_async_copy(stream, own_raw, local_sem.at[4])
    raw_copy.start()
    for kind in (GATE, UP, DOWN):
        local_copy(kind).start()

    first_segment = (y == 0) & (pair == 0)

    @pl.when(first_segment)
    def _():
        conv_in[0, 0:8, :] = jnp.zeros((8, channels), jnp.float32)

    barrier = pltpu.get_barrier_semaphore()
    greeted = [core_peer, x_peer, y_peer]
    greeted += [device(x, order[j], y, core) for j in range(1, planes)]
    greeted += [device(x, (z + s) % planes, 1 - y, core) for s in sorted({2, planes - 2})]
    for peer in greeted:
        pl.semaphore_signal(barrier, inc=1, device_id=peer, device_id_type=MESH)
    pl.semaphore_wait(barrier, len(greeted))

    others = range(1, planes)
    send_own(GATE)
    for j in others:
        send_planes(GATE, j)
    send_own(UP)
    send_own(DOWN)
    send(stream, own_raw, raw_send, (0,), raw_recv.at[0], core_peer)
    for j in others:
        send_direct(GATE, j)
    for copy in packs:
        copy.wait()
    local_copy(MIX).start()
    if not LATE:
        send_own(MIX)

    def rms(values):
        return values * lax.rsqrt(jnp.mean(values * values, axis=1, keepdims=True) + EPSILON)

    step_rows = 16

    def norm_all():
        @pl.loop(0, 2 * rows // step_rows)
        def _(i):
            at = pl.ds(aligned(i * step_rows, 16), step_rows)
            values = raw[at, :].astype(jnp.float32)
            normed[0, at, :] = (rms(values) * gains[0:1, :]).astype(jnp.bfloat16)

    def dot(a, b):
        return jnp.dot(a, b, preferred_element_type=jnp.float32)

    tile = TILE

    def hidden_tiles(which, start, row_count, first, last):
        at = pl.ds(aligned(start, 128), row_count)

        def columns(begin, count):
            cols = pl.ds(aligned(begin, 128), count)
            gate = dot(normed[which, at, :], gate_buf[:, cols])
            up = dot(normed[which, at, :], up_buf[:, cols])
            hidden[at, cols] = (gate / (1.0 + jnp.exp(-gate)) * up).astype(jnp.bfloat16)

        whole = min(last, units // tile)

        @pl.loop(first, whole)
        def _(n):
            columns(n * tile, tile)

        if whole < last:
            columns(whole * tile, units - whole * tile)

    tiles = pl.cdiv(units, tile)

    def hidden_rows(which, start, row_count):
        hidden_tiles(which, start, row_count, 0, tiles)

    def down_rows(phase, start, row_count, of_z):
        at = pl.ds(aligned(start, 128), row_count)

        for s in range(2):
            cols = pl.ds(aligned((of_z * 2 + s) * down_cols, 128), down_cols)
            partials[phase, at, cols] = dot(hidden[at, :], down_buf[of_z * 2 + s]).astype(jnp.bfloat16)

    def owned(of_member, of_core, part):
        return of_member * rows + part * 2 * quarter + of_core * quarter

    def owned_rows(of_member, of_core, part):
        return pl.ds(aligned(owned(of_member, of_core, part), 16), quarter)

    def local_rows(part):
        return pl.ds(part * quarter, quarter)

    def plane_of(of_z):
        return pl.ds(aligned(of_z * plane_cols, 128), plane_cols)

    def send_core(phase, of_member, part, of_z):
        send(
            partials.at[phase, owned_rows(of_member, 1 - core, part), plane_of(of_z)],
            from_core.at[phase, of_member, local_rows(part), plane_of(of_z)],
            core_send, (int(of_member is not member), part, ranks[id(of_z)]),
            core_recv.at[phase, of_member, part, of_z], core_peer,
        )

    def wait_core(phase, of_member, part, of_z):
        arrive(
            from_core.at[phase, of_member, local_rows(part), plane_of(of_z)],
            core_recv.at[phase, of_member, part, of_z],
        )

    def send_pair(phase, part, of_z):
        wait_core(phase, 1 - member, part, of_z)
        at, cols = local_rows(part), plane_of(of_z)
        mine = partials[phase, owned_rows(1 - member, core, part), cols].astype(jnp.float32)
        theirs = from_core[phase, 1 - member, at, cols].astype(jnp.float32)
        summed[phase, at, cols] = (mine + theirs).astype(jnp.bfloat16)
        send(
            summed.at[phase, at, cols], from_pair.at[phase, at, cols],
            pair_send, (part, ranks[id(of_z)]), pair_recv.at[phase, part, of_z], pair_peer,
        )

    def wait_pair(phase, part):
        for of_z in order:
            wait_core(phase, member, part, of_z)
            arrive(
                from_pair.at[phase, local_rows(part), plane_of(of_z)],
                pair_recv.at[phase, part, of_z],
            )

    def settle(phase, gain, weight, source, target, next_gain, part):
        @pl.loop(0, quarter // step_rows)
        def _(i):
            at = pl.ds(aligned(part * quarter + i * step_rows, 16), step_rows)
            mine = pl.ds(aligned(owned(member, core, part) + i * step_rows, 16), step_rows)
            branch = (
                partials[phase, mine, :].astype(jnp.float32)
                + from_core[phase, member, at, :].astype(jnp.float32)
                + from_pair[phase, at, :].astype(jnp.float32)
            )
            before = source[mine if phase == 0 else at, :]
            after = before.astype(jnp.float32) + weight * (rms(branch) * gains[gain : gain + 1, :])
            rounded = after.astype(jnp.bfloat16)
            target[at, :] = rounded
            if next_gain is not None:
                scaled = rms(rounded.astype(jnp.float32)) * gains[next_gain : next_gain + 1, :]
                normed[phase + 1, mine, :] = scaled.astype(jnp.bfloat16)

    def gather_ref(which, of_member, of_core, part):
        return normed.at[which, owned_rows(of_member, of_core, part), :]

    def gather_start(which, part):
        mine = gather_ref(which, member, core, part)
        send(mine, mine, gather_send, (1, part), gather_recv.at[which, 1, part], pair_peer)
        send(mine, mine, gather_send, (0, part), gather_recv.at[which, 0, part], core_peer)

    def gather_own(which, part):
        arrive(
            gather_ref(which, member, 1 - core, part),
            gather_recv.at[which, 0, part],
        )

    def gather_pass(which, part):
        theirs = gather_ref(which, 1 - member, core, part)
        arrive(theirs, gather_recv.at[which, 1, part])
        send(theirs, theirs, gather_send, (2, part), gather_recv.at[which, 2, part], core_peer)

    def gather_pair(which, part):
        arrive(
            gather_ref(which, 1 - member, 1 - core, part),
            gather_recv.at[which, 2, part],
        )

    head = 8

    def mix_in(s, begin, count, js):
        at = pl.ds(aligned(s * rows + begin, 128), count)
        deep = 2 * weight_rows
        total = None if 0 in js else mix_sum[at, :]
        for j in js:
            along = pl.ds(aligned(order[j] * deep, 128), deep)
            term = dot(normed[1, at, along], mix_buf[along, 0 : 3 * channels])
            total = term if total is None else total + term
        mix_sum[at, :] = total
        if planes - 1 in js:
            conv_in[s, head + begin : head + begin + count, :] = (
                total[:, 2 * channels : 3 * channels] * total[:, 0:channels]
            )

    def halo(source, target, to):
        return pltpu.make_async_remote_copy(
            src_ref=conv_in.at[source, rows : rows + head, :],
            dst_ref=conv_in.at[target, 0:head, :],
            send_sem=halo_send.at[source], recv_sem=halo_recv.at[target],
            device_id=to, device_id_type=MESH,
        )

    def near_tail(s):
        return halo(s, y + s * (1 - y), y_peer)

    def far_tail(s):
        return halo(s, 0, device(x, (z + 2) % planes, 0, core))

    def tails(s, act):
        @pl.when((s == 0) | (y == 0))
        def _():
            act(near_tail(s))

        @pl.when((s == 1) & (y == 1) & (pair < pairs - 1))
        def _():
            act(far_tail(s))

    def mix_gate(s, part):
        if part == 0:
            @pl.when(jnp.logical_not(first_segment & (s == 0)))
            def _():
                halo(s, s, y_peer).wait_recv()

        count = 2 * quarter
        total = None
        for tap in range(TAPS):
            begin = head - TAPS + 1 + tap + part * count
            shifted = conv_in[s, begin : begin + count, :]
            scale = taps[tap : tap + 1, pl.ds(aligned(member * channels, 128), channels)]
            total = scale * shifted if total is None else total + scale * shifted
        at = pl.ds(aligned(s * rows + part * count, 128), count)
        bgate = mix_sum[at, channels : 2 * channels]
        gated[at, :] = (bgate * total).astype(jnp.bfloat16)

    def mix_out(s, part, of_z):
        at = pl.ds(aligned(s * rows + part * 2 * quarter, 128), 2 * quarter)

        for n in range(2):
            index = of_z * 2 + n
            cols = pl.ds(aligned(index * out_cols, 128), out_cols)
            weight = mix_buf[pl.ds(aligned(index * weight_rows, 128), channels), 3 * channels :]
            partials[1, at, cols] = dot(gated[at, :], weight).astype(jnp.bfloat16)

    def core_parts(phase, of_member, part):
        for of_z in order:
            send_core(phase, of_member, part, of_z)

    for kind, i in ((GATE, 0), (GATE, 1), (UP, 0), (UP, 1)):
        pass_own(kind, i)
    for j in others:
        spread(GATE, j)
        send_planes(UP, j)
        if j <= 2:
            pass_own(DOWN, j - 1)
    if not LATE:
        pass_own(MIX, 0)
        pass_own(MIX, 1)
    send(stream, own_raw, raw_send, (1,), raw_recv.at[1], pair_peer)
    for j in others:
        send_direct(UP, j)
    for j in others:
        relay(GATE, j)
    for j in others:
        spread(UP, j)
        send_planes(DOWN, j)
    for j in others:
        send_direct(DOWN, j)
    relay(UP, 1)
    raw_copy.wait()

    def raw_at(of_member, of_core):
        return raw.at[
            pl.ds(aligned(of_member * rows, 16), rows), pl.ds(aligned(of_core * width, 128), width)
        ]

    arrive(raw_at(member, 1 - core), raw_recv.at[0])
    pair_raw = raw_at(1 - member, core)
    arrive(pair_raw, raw_recv.at[1])
    send(pair_raw, pair_raw, raw_send, (2,), raw_recv.at[2], core_peer)
    for j in range(2, planes):
        relay(UP, j)
    for j in others:
        spread(DOWN, j)
        send_planes(MIX, j)
    for j in others:
        send_direct(MIX, j)
    arrive(raw_at(1 - member, 1 - core), raw_recv.at[2])
    norm_all()
    for kind in (GATE, UP):
        for j in range(planes):
            complete(kind, j)
    for j in others:
        hidden_tiles(0, 0, 2 * rows, tiles * (j - 1) // (planes - 1), tiles * j // (planes - 1))
        relay(DOWN, j)
    if LATE:
        send_own(MIX)
    for j in range(planes):
        if j > 0:
            spread(MIX, j)
        complete(DOWN, j)

        @pl.loop(0, 2)
        def _(r):
            down_rows(0, r * rows, rows, order[j])

        for of_member in (1 - member, member):
            for part in (1, 0):
                send_core(0, of_member, part, order[j])
        if j > 0:
            for part in (1, 0):
                send_pair(0, part, order[j - 1])
    for part in (1, 0):
        send_pair(0, part, order[planes - 1])
    if LATE:
        pass_own(MIX, 0)
        pass_own(MIX, 1)
    for part in (1, 0):
        wait_pair(0, part)
        settle(0, 1, 0.5, raw, current, 2, part)
        gather_start(1, part)
    for j in others:
        relay(MIX, j)
    gather_own(1, 1)
    gather_own(1, 0)
    last = planes - 1
    half_rows = 2 * quarter
    for j in range(last):
        complete(MIX, j)
        mix_in(member, 0, rows, (j,))
    gather_pass(1, 1)
    gather_pair(1, 1)
    mix_in(1 - member, half_rows, half_rows, range(last))
    gather_pass(1, 0)
    complete(MIX, last)
    mix_in(1 - member, half_rows, half_rows, (last,))
    tails(1 - member, lambda copy: copy.start())
    mix_in(member, 0, rows, (last,))
    tails(member, lambda copy: copy.start())
    gather_pair(1, 0)
    mix_in(1 - member, 0, half_rows, range(planes))
    mix_gate(1 - member, 1)
    for of_z in order:
        mix_out(1 - member, 1, of_z)
        send_core(1, 1 - member, 1, of_z)
    mix_gate(1 - member, 0)
    for of_z in order:
        mix_out(1 - member, 0, of_z)
        send_core(1, 1 - member, 0, of_z)
        send_pair(1, 1, of_z)
    mix_gate(member, 1)
    for of_z in order:
        mix_out(member, 1, of_z)
        send_core(1, member, 1, of_z)
        send_pair(1, 0, of_z)
    mix_gate(member, 0)
    for of_z in order:
        mix_out(member, 0, of_z)
        send_core(1, member, 0, of_z)
    for part in (1, 0):
        wait_pair(1, part)
        settle(1, 3, 1.0, current, current, 4, part)
        gather_start(2, part)
        gather_own(2, part)
        hidden_rows(2, member * rows + part * 2 * quarter, 2 * quarter)
    gather_pass(2, 1)
    down_rows(2, member * rows, rows, order[0])
    gather_pair(2, 1)
    start = (1 - member) * rows
    hidden_rows(2, start + 2 * quarter, 2 * quarter)
    for j in range(planes):
        down_rows(2, start + 2 * quarter, 2 * quarter, order[j])
        send_core(2, 1 - member, 1, order[j])
        if j > 1:
            send_pair(2, 1, order[j - 2])
    gather_pass(2, 0)
    send_pair(2, 1, order[planes - 2])
    send_pair(2, 1, order[planes - 1])
    gather_pair(2, 0)
    hidden_rows(2, start, 2 * quarter)
    for j in range(planes):
        down_rows(2, start, 2 * quarter, order[j])
        send_core(2, 1 - member, 0, order[j])
        if j > 1:
            send_pair(2, 0, order[j - 2])
    down_rows(2, member * rows, rows, order[1])
    for j in range(2):
        send_pair(2, 0, order[planes - 2 + j])
    for j in range(2, planes):
        down_rows(2, member * rows, rows, order[j])
    for part in (1, 0):
        core_parts(2, member, part)
    stores = [None, None]
    for part in (1, 0):
        wait_pair(2, part)
        settle(2, 5, 0.5, current, result, None, part)
        there = pl.ds(aligned(part * 2 * quarter + core * quarter, 16), quarter)
        send(
            result.at[local_rows(part), pl.ds(aligned((1 - core) * width, 128), width)],
            out.at[there, :], out_send, (part,), out_recv.at[part], core_peer,
        )
        store = pltpu.make_async_copy(
            result.at[local_rows(part), pl.ds(aligned(core * width, 128), width)],
            out.at[there, :], store_sem.at[part],
        )
        store.start()
        stores[part] = store
    for part in range(2):
        stores[part].wait()
        theirs = pl.ds(aligned(part * 2 * quarter + (1 - core) * quarter, 16), quarter)
        arrive(out.at[theirs, :], out_recv.at[part])
    for copy in pending.values():
        copy.wait_send()
    for s in range(2):
        tails(s, lambda copy: copy.wait_send())


def fits_kernel(mesh, stream, w_gate, w_down, w_inner, w_out):
    planes = mesh.shape["fs"] // 2
    return (
        mesh.shape["tp"] == 2
        and mesh.shape["rep"] == 2
        and mesh.shape["fs"] % 4 == 0
        and planes >= 4
        and w_gate.shape[0] == w_inner.shape[0] == w_out.shape[0] // 2
        and stream.shape[0] % 256 == 0
        and w_gate.shape[0] % 256 == 0
        and w_gate.shape[1] % 256 == 0
        and w_inner.shape[1] % 256 == 0
        and w_down.shape[1] % 128 == 0
    )


def fused(stream, norm_gains, w_gate, w_up, w_down, w_inner, w_bgate, w_cgate, conv_taps, w_out):
    count = lax.axis_size("fs")
    planes = count // 2
    rows, width = stream.shape
    model_width = 2 * width
    weight_rows, units = w_gate.shape[0], w_gate.shape[1] // 2
    channels, down_cols, out_cols = w_inner.shape[1] // 2, w_down.shape[1], w_out.shape[1]
    own_rows = rows // 2
    mix_width = 3 * channels + out_cols
    bf16, f32 = jnp.bfloat16, jnp.float32
    vmem, dma = pltpu.VMEM, pltpu.SemaphoreType.DMA
    anywhere = pl.BlockSpec(memory_space=pl.ANY)
    flops = 2 * 2 * rows * (6 * model_width * units + 4 * model_width * channels)
    return pl.pallas_call(
        functools.partial(layer_kernel, planes),
        out_shape=pltpu.VMEM((rows, width), bf16),
        in_specs=[anywhere] * 10,
        out_specs=pl.BlockSpec(memory_space=pltpu.VMEM),
        scratch_shapes=[
            vmem(norm_gains.shape, f32),
            vmem(conv_taps.shape, f32),
            vmem((weight_rows, 2 * mix_width), bf16),
            vmem((model_width, units), bf16),
            vmem((model_width, units), bf16),
            vmem((count, units, down_cols), bf16),
            vmem((model_width, mix_width), bf16),
            vmem((2 * rows, model_width), bf16),
            vmem((3, 2 * rows, model_width), bf16),
            vmem((2 * rows, units), bf16),
            vmem((3, 2 * rows, model_width), bf16),
            vmem((3, 2, own_rows, model_width), bf16),
            vmem((3, own_rows, model_width), bf16),
            vmem((3, own_rows, model_width), bf16),
            vmem((own_rows, model_width), bf16),
            vmem((2, 8 + rows, channels), f32),
            vmem((2 * rows, 3 * channels), f32),
            vmem((2 * rows, channels), bf16),
            vmem((own_rows, model_width), bf16),
            dma((5,)),
            dma((10,)),
            dma((2, 6, planes)),
            dma((4, 6, planes)),
            dma((3,)),
            dma((3,)),
            dma((2, 2, planes)),
            dma((3, 2, 2, planes)),
            dma((2, planes)),
            dma((3, 2, planes)),
            dma((3, 2)),
            dma((3, 3, 2)),
            dma((2,)),
            dma((2,)),
            dma((2,)),
            dma((2,)),
            dma((2,)),
        ],
        cost_estimate=pl.CostEstimate(
            flops=flops, bytes_accessed=4 * w_gate.size * 2, transcendentals=4 * rows * units
        ),
        compiler_params=pltpu.CompilerParams(
            collective_id=0, has_side_effects=True, vmem_limit_bytes=60 * 1024 * 1024
        ),
        name="layer",
    )(stream, norm_gains, w_gate, w_up, w_down, w_inner, w_bgate, w_cgate, conv_taps, w_out)


def solution(mesh):
    def body(stream, norm_gains, w_gate, w_up, w_down, w_inner, w_bgate, w_cgate, conv_taps, w_out):
        arguments = (stream, norm_gains, w_gate, w_up, w_down, w_inner, w_bgate, w_cgate, conv_taps, w_out)
        if fits_kernel(mesh, stream, w_gate, w_down, w_inner, w_out):
            return fused(*arguments)
        return shards(*arguments)

    return jax.shard_map(
        body,
        mesh=mesh,
        in_specs=(
            P(("rep", "fs"), "tp"),
            P(),
            P("fs", "tp"),
            P("fs", "tp"),
            P("tp", "fs"),
            P("fs", "tp"),
            P("fs", "tp"),
            P("fs", "tp"),
            P(None, "tp"),
            P("tp", "fs"),
        ),
        out_specs=P(("rep", "fs"), "tp"),
        check_vma=False,
    )
```

```python
import functools

import jax
import jax.numpy as jnp
from jax import lax
from jax.experimental import pallas as pl
from jax.experimental.pallas import tpu as pltpu
from jax.sharding import PartitionSpec as P

TAPS = 3
EPSILON = 1e-06


def ring_order(count):
    return list(range(0, count, 2)) + list(range(1, count, 2))[::-1]


def swap(x, axis):
    return lax.ppermute(x, axis, [(0, 1), (1, 0)])


def copy_blocks(count, size, starts, source, target):
    for i in range(count):
        begin = pl.multiple_of(starts[i] * size, size)
        target[:, i * size : (i + 1) * size] = source[:, pl.ds(begin, size)]


def permuted(x, starts, size):
    return pl.pallas_call(
        functools.partial(copy_blocks, len(starts), size),
        in_specs=[
            pl.BlockSpec(memory_space=pltpu.SMEM),
            pl.BlockSpec(memory_space=pltpu.VMEM),
        ],
        out_specs=pl.BlockSpec(memory_space=pltpu.VMEM),
        out_shape=jax.ShapeDtypeStruct(x.shape, x.dtype),
        cost_estimate=pl.CostEstimate(flops=0, bytes_accessed=2 * x.size * x.dtype.itemsize, transcendentals=0),
        compiler_params=pltpu.CompilerParams(vmem_limit_bytes=3 * x.size * x.dtype.itemsize),
    )(jnp.stack(starts), x)


class Ring:
    def __init__(self, own, after=None):
        count = lax.axis_size("fs")
        order = ring_order(count)
        onward = [(order[i], order[(i + 1) % count]) for i in range(count)]
        back = [(b, a) for a, b in onward]
        half = count // 2
        first, second = own, own
        if after is not None:
            first, _ = lax.optimization_barrier((own, after[0]))
            second, _ = lax.optimization_barrier((own, after[1]))
        rows = own.shape[0] // 2
        self.shards = {0: own}
        self.arrived = self.early = (own, own)
        for step in range(1, half):
            first = lax.ppermute(first, "fs", onward)
            second = lax.ppermute(second, "fs", back)
            self.shards[step] = first
            self.shards[count - step] = second
            self.arrived = (first, second)
            if step == 1:
                self.early = self.arrived
        self.last = (
            lax.ppermute(first[:rows], "fs", onward),
            lax.ppermute(second[rows:], "fs", back),
        )
        self.shards[half] = jnp.concatenate(self.last, axis=0)
        self.sequence = [0]
        for step in range(1, half):
            self.sequence += [step, count - step]
        self.sequence += [half]

    def lined_up(self, axis):
        return jnp.concatenate([self.shards[d] for d in range(len(self.shards))], axis=axis)


def shards(stream, norm_gains, w_gate, w_up, w_down, w_inner, w_bgate, w_cgate, conv_taps, w_out):
    count, tp = lax.axis_size("fs"), lax.axis_size("tp")
    tp_index, rep_index, fs_index = lax.axis_index("tp"), lax.axis_index("rep"), lax.axis_index("fs")
    rows, width = stream.shape
    model_width = width * tp
    order = ring_order(count)
    places = [order.index(i) for i in range(count)]
    place = jnp.array(places, jnp.int32)[fs_index]
    origin = [
        jnp.array(order, jnp.int32)[lax.rem(place - d + count, count)] for d in range(count)
    ]

    behind = [
        lax.rem(place - places[i] + count, count) for i in range(count)
    ]

    def blocks(x, starts):
        size = x.shape[1] // count
        if size % 128 == 0:
            return permuted(x, starts, size)
        return jnp.concatenate(
            [lax.dynamic_slice_in_dim(x, start * size, size, 1) for start in starts], axis=1
        )

    def rep_part(w, axis):
        size = w.shape[axis] // lax.axis_size("rep")
        return lax.dynamic_slice_in_dim(w, rep_index * size, size, axis)

    def whole_features(x):
        if tp != 2:
            return lax.all_gather(x, "tp", axis=1, tiled=True)
        other = swap(x, "tp")
        mine = tp_index == 0
        return jnp.concatenate([jnp.where(mine, x, other), jnp.where(mine, other, x)], axis=1)

    def own_features(x):
        return lax.dynamic_slice_in_dim(x, tp_index * width, width, 1)

    def feature_sum(partials):
        rounded = blocks(partials.astype(jnp.bfloat16), behind)
        if tp != 2:
            return lax.psum_scatter(rounded, "tp", scatter_dimension=1, tiled=True).astype(jnp.float32)
        theirs = lax.dynamic_slice_in_dim(rounded, (1 - tp_index) * width, width, 1)
        received = swap(theirs, "tp").astype(jnp.float32)
        return own_features(rounded).astype(jnp.float32) + received

    def norm_own(current, row):
        values = current.astype(jnp.float32)
        scaled = values * lax.rsqrt(jnp.mean(values * values, axis=1, keepdims=True) + EPSILON)
        return (scaled * norm_gains[row]).astype(jnp.bfloat16)

    def norm_other(normed):
        return whole_features(swap(own_features(normed), "rep"))

    def settle(current, own_sum, other_sum, row, weight):
        received = swap(other_sum.astype(jnp.bfloat16), "rep").astype(jnp.float32)
        branch = whole_features(own_sum + received)
        scaled = branch * lax.rsqrt(jnp.mean(branch * branch, axis=1, keepdims=True) + EPSILON)
        return (current.astype(jnp.float32) + weight * (scaled * norm_gains[row])).astype(
            jnp.bfloat16
        )

    def dot(a, b):
        return jnp.dot(a, b, preferred_element_type=jnp.float32)

    def activate(gate_vals, upward):
        return (jax.nn.silu(gate_vals) * upward).astype(jnp.bfloat16)

    current = whole_features(stream)
    normed = norm_own(current, 0)
    normed = jnp.concatenate([normed, norm_other(normed)], axis=0)

    gate_ring = Ring(rep_part(w_gate, 1))
    up_ring = Ring(rep_part(w_up, 1))
    down_own = rep_part(w_down, 0)
    down_ring = Ring(down_own, gate_ring.arrived)
    mix_own = jnp.concatenate([rep_part(w, 1) for w in (w_inner, w_bgate, w_cgate)], axis=1)
    out_own = rep_part(w_out, 0)
    mix_width = mix_own.shape[1]
    mix_ring = Ring(
        jnp.concatenate([mix_own, out_own.reshape(mix_own.shape[0], -1)], axis=1), down_ring.early
    )

    def by_shards(ring):
        size = ring.shards[0].shape[0]
        total = None
        for d in ring.sequence:
            term = dot(lax.dynamic_slice_in_dim(normed, origin[d] * size, size, 1), ring.shards[d])
            total = term if total is None else total + term
        return total

    hidden = activate(by_shards(gate_ring), by_shards(up_ring))
    down_blocks = {d: dot(hidden, down_ring.shards[d]).astype(jnp.bfloat16) for d in down_ring.sequence}
    sums = feature_sum(jnp.concatenate([down_blocks[d] for d in range(count)], axis=1))
    first = settle(current, sums[:rows], sums[rows:], 1, 0.5)

    mix_whole = mix_ring.lined_up(0)[:, :mix_width]
    out_whole = jnp.concatenate(
        [mix_ring.shards[d][:, mix_width:].reshape(out_own.shape) for d in range(count)], axis=1
    )
    channels = mix_width // 3
    taps = rep_part(conv_taps, 1)

    def mix_in(normed_mix):
        product = dot(blocks(normed_mix, origin), mix_whole)
        inner, bgate, cgate = (product[:, i * channels : (i + 1) * channels] for i in range(3))
        return cgate * inner, bgate

    def mix_out(conv_input, bgate, earlier):
        padded = jnp.concatenate([earlier, conv_input], axis=0)
        conv = taps[0] * padded[0:rows]
        for tap in range(1, TAPS):
            conv = conv + taps[tap] * padded[tap : tap + rows]
        return feature_sum(dot((bgate * conv).astype(jnp.bfloat16), out_whole))

    normed_mix = norm_own(first, 2)
    other_mix = norm_other(normed_mix)
    own_in, own_bgate = mix_in(normed_mix)
    other_in, other_bgate = mix_in(other_mix)
    tails = jnp.concatenate([own_in[rows - (TAPS - 1) :], other_in[rows - (TAPS - 1) :]], axis=0)
    earlier = lax.ppermute(tails, "fs", [(i, i + 1) for i in range(count - 1)])
    other_sum = mix_out(other_in, other_bgate, earlier[TAPS - 1 :])
    own_sum = mix_out(own_in, own_bgate, earlier[: TAPS - 1])
    second = settle(first, own_sum, other_sum, 3, 1.0)

    gate_whole, up_whole = gate_ring.lined_up(0), up_ring.lined_up(0)
    down_whole = down_ring.lined_up(1)

    def units(normed_rows):
        lined = blocks(normed_rows, origin)
        return activate(dot(lined, gate_whole), dot(lined, up_whole))

    normed = norm_own(second, 4)
    other_normed = norm_other(normed)
    own_units = units(normed)
    other_sum = feature_sum(dot(units(other_normed), down_whole))
    own_sum = feature_sum(dot(own_units, down_whole))
    return own_features(settle(second, own_sum, other_sum, 5, 0.5))


MESH = pl.DeviceIdType.MESH
GATE, UP, DOWN, MIX, OUT = range(5)
Z, X, Y, PART_A, PART_B, Z_OTHER = range(6)
DIRECT = ((8, 0), (4, 0), (8, 0), (8, 0), (8, 0))
BY_Y = (3, 3, 3, 3, 3)
TILE = 512


def aligned(value, to):
    return pl.multiple_of(value, to)


def layer_kernel(
    planes,
    stream, all_gains, w_gate, w_up, w_down, w_inner, w_bgate, w_cgate, all_taps, w_out, out,
    gains, taps, w_mix,
    gate_buf, up_buf, down_buf, mix_buf, out_buf, raw, normed, hidden, partials, from_core, summed,
    from_pair, current, conv_in, mix_sum, gated, result,
    local_sem, pack_sem, piece_send, piece_recv, raw_send, raw_recv, core_send, core_recv,
    pair_send, pair_recv, gather_send, gather_recv, halo_send, halo_recv, out_send, out_recv, store_sem,
):
    x, place, core = lax.axis_index("rep"), lax.axis_index("fs"), lax.axis_index("tp")
    z, y = place // 2, place % 2
    pair, member = z // 2, z % 2
    pairs = planes // 2
    rows, width = stream.shape
    quarter = rows // 4
    model_width = 2 * width
    units, channels, mix_width = gate_buf.shape[1], gated.shape[1], mix_buf.shape[1]
    out_cols = out_buf.shape[1]
    weight_rows = w_gate.shape[0]
    down_cols = w_down.shape[1]
    plane_cols = 2 * down_cols
    buffers = (gate_buf, up_buf, down_buf, mix_buf, out_buf)
    halves = (weight_rows // 2, weight_rows // 2, units // 2, weight_rows // 2, channels // 2)

    def device(to_x, to_z, to_y, to_core):
        return (to_x, to_z * 2 + to_y, to_core)

    order = [2 * ((pair + j // 2) % pairs) + (member + j) % 2 for j in range(planes)]
    ranks = {id(of_z): j for j, of_z in enumerate(order)}
    partner = order[1]
    core_peer = device(x, z, y, 1 - core)
    pair_peer = device(x, partner, y, core)
    x_peer, y_peer = device(1 - x, z, y, core), device(x, z, 1 - y, core)

    pending = {}

    def send(source, target, sems, slot, recv_sem, to):
        key = (id(sems),) + slot
        if key in pending:
            pending[key].wait_send()
        send_sem = sems.at[slot]
        copy = pltpu.make_async_remote_copy(
            src_ref=source, dst_ref=target, send_sem=send_sem, recv_sem=recv_sem,
            device_id=to, device_id_type=MESH,
        )
        copy.start()
        pending[key] = copy

    def arrive(target, recv_sem):
        pltpu.make_async_remote_copy(
            src_ref=target, dst_ref=target, send_sem=raw_send.at[0], recv_sem=recv_sem,
            device_id=core_peer, device_id_type=MESH,
        ).wait_recv()

    def piece(kind, of_z, of_y, of_x, begin=0, end=None):
        half = halves[kind]
        count = (half if end is None else end) - begin
        if kind == DOWN:
            return down_buf.at[of_z * 2 + of_y, pl.ds(aligned(of_x * half + begin, 16), count), :]
        start = ((of_z * 2 + of_y) * 2 + of_x) * half + begin
        return buffers[kind].at[pl.ds(aligned(start, 16), count), :]

    def own_source(kind, side, start, count):
        if kind == DOWN:
            return w_down.at[pl.ds(aligned(side * units + start, 16), count), :]
        if kind == OUT:
            return w_out.at[pl.ds(aligned(side * channels + start, 16), count), :]
        cols = mix_width if kind == MIX else units
        source = (w_gate, w_up, None, w_mix)[kind]
        return source.at[pl.ds(aligned(start, 16), count), pl.ds(aligned(side * cols, 128), cols)]

    def piece_copy(source, target, kind, route, j, of_z, to):
        send(source, target, piece_send, (kind % 3, route, j), piece_recv.at[kind, route, of_z], to)

    def wait_piece(target, kind, route, of_z):
        arrive(target, piece_recv.at[kind, route, of_z])

    def eighths(half, count):
        return min(half, (half * count // 8 + 15) // 16 * 16)

    def direct(kind, j):
        return eighths(halves[kind], DIRECT[kind][0 if j == 1 else 1])

    def split(kind):
        return halves[kind] - eighths(halves[kind], BY_Y[kind])

    def send_planes(kind, j):
        to, half = order[j], halves[kind]
        piece_copy(
            own_source(kind, to % 2, x * half, half), piece(kind, z, y, x),
            kind, Z, j, z, device(x, to, y, core),
        )

    def send_direct(kind, j):
        to, count = order[j], direct(kind, j)
        if count == 0:
            return
        piece_copy(
            own_source(kind, to % 2, (1 - x) * halves[kind], count), piece(kind, z, y, 1 - x, 0, count),
            kind, Z_OTHER, j, z, device(x, to, y, core),
        )

    def own_part(kind, i):
        half = halves[kind]
        return (0, half // 4, half // 2)[i], (half // 4, half // 2, half)[i]

    def send_own(kind):
        for i, route in enumerate((Y, PART_A, Z)):
            begin, end = own_part(kind, i)
            piece_copy(
                own_source(kind, member, x * halves[kind] + begin, end - begin),
                piece(kind, z, y, x, begin, end), kind, route, 0, z, y_peer,
            )

    def pass_own(kind, i):
        part = piece(kind, z, 1 - y, x, *own_part(kind, i))
        wait_piece(part, kind, (Y, PART_A, Z)[i], z)
        piece_copy(part, part, kind, (X, PART_B, Z_OTHER)[i], 0, z, x_peer)

    def spread(kind, j):
        of = order[j]
        whole = piece(kind, of, y, x)
        wait_piece(whole, kind, Z, of)
        piece_copy(whole, whole, kind, Y, j, of, y_peer)
        if direct(kind, j) < halves[kind]:
            rest = piece(kind, of, y, x, direct(kind, j), None)
            piece_copy(rest, rest, kind, X, j, of, x_peer)

    def relay(kind, j):
        of = order[j]
        if direct(kind, j) == halves[kind]:
            wait_piece(piece(kind, of, y, 1 - x), kind, Z_OTHER, of)
        else:
            wait_piece(piece(kind, of, y, 1 - x, direct(kind, j), None), kind, X, of)
        part = piece(kind, of, y, 1 - x, split(kind), None)
        piece_copy(part, part, kind, PART_A, j, of, y_peer)
        wait_piece(piece(kind, of, 1 - y, x), kind, Y, of)
        part = piece(kind, of, 1 - y, x, 0, split(kind))
        piece_copy(part, part, kind, PART_B, j, of, x_peer)

    def local_copy(kind):
        count = units if kind == DOWN else weight_rows
        if kind == DOWN:
            target = down_buf.at[z * 2 + y]
        else:
            target = buffers[kind].at[pl.ds(aligned((z * 2 + y) * weight_rows, 16), count), :]
        return pltpu.make_async_copy(own_source(kind, member, 0, count), target, local_sem.at[kind])

    def complete(kind, j):
        of = order[j]
        if j == 0:
            local_copy(kind).wait()
            for i, route in enumerate((X, PART_B, Z_OTHER)):
                wait_piece(piece(kind, z, 1 - y, 1 - x, *own_part(kind, i)), kind, route, z)
        else:
            if 0 < direct(kind, j) < halves[kind]:
                wait_piece(piece(kind, of, y, 1 - x, 0, direct(kind, j)), kind, Z_OTHER, of)
            wait_piece(piece(kind, of, 1 - y, 1 - x, split(kind), None), kind, PART_A, of)
            wait_piece(piece(kind, of, 1 - y, 1 - x, 0, split(kind)), kind, PART_B, of)

    own_raw = raw.at[pl.ds(aligned(member * rows, 16), rows), pl.ds(aligned(core * width, 128), width)]
    packs = []
    for side in range(2):
        base = side * mix_width
        for n, weight in enumerate((w_inner, w_bgate, w_cgate)):
            packs.append((
                weight.at[:, side * channels : (side + 1) * channels],
                w_mix.at[:, base + n * channels : base + (n + 1) * channels],
            ))
    packs += [(all_gains, gains), (all_taps, taps)]
    packs = [pltpu.make_async_copy(a, b, pack_sem.at[n]) for n, (a, b) in enumerate(packs)]
    for copy in packs:
        copy.start()
    raw_copy = pltpu.make_async_copy(stream, own_raw, local_sem.at[5])
    raw_copy.start()
    for kind in (GATE, UP, DOWN, OUT):
        local_copy(kind).start()

    first_segment = (y == 0) & (pair == 0)

    @pl.when(first_segment)
    def _():
        conv_in[0, 0:8, :] = jnp.zeros((8, channels), jnp.float32)

    barrier = pltpu.get_barrier_semaphore()
    greeted = [core_peer, x_peer, y_peer]
    greeted += [device(x, order[j], y, core) for j in range(1, planes)]
    greeted += [device(x, (z + s) % planes, 1 - y, core) for s in sorted({2, planes - 2})]
    for peer in greeted:
        pl.semaphore_signal(barrier, inc=1, device_id=peer, device_id_type=MESH)
    pl.semaphore_wait(barrier, len(greeted))

    others = range(1, planes)
    send_own(GATE)
    for j in others:
        send_planes(GATE, j)
    send_own(UP)
    send_own(DOWN)
    send(stream, own_raw, raw_send, (0,), raw_recv.at[0], core_peer)
    for j in others:
        send_direct(GATE, j)
    for copy in packs:
        copy.wait()
    local_copy(MIX).start()

    def rms(values):
        return values * lax.rsqrt(jnp.mean(values * values, axis=1, keepdims=True) + EPSILON)

    step_rows = 16

    def norm_all():
        @pl.loop(0, 2 * rows // step_rows)
        def _(i):
            at = pl.ds(aligned(i * step_rows, 16), step_rows)
            values = raw[at, :].astype(jnp.float32)
            normed[0, at, :] = (rms(values) * gains[0:1, :]).astype(jnp.bfloat16)

    def dot(a, b):
        return jnp.dot(a, b, preferred_element_type=jnp.float32)

    tile = TILE

    def hidden_tiles(which, start, row_count, first, last):
        at = pl.ds(aligned(start, 128), row_count)

        def columns(begin, count):
            cols = pl.ds(aligned(begin, 128), count)
            gate = dot(normed[which, at, :], gate_buf[:, cols])
            up = dot(normed[which, at, :], up_buf[:, cols])
            hidden[at, cols] = (gate / (1.0 + jnp.exp(-gate)) * up).astype(jnp.bfloat16)

        whole = min(last, units // tile)

        @pl.loop(first, whole)
        def _(n):
            columns(n * tile, tile)

        if whole < last:
            columns(whole * tile, units - whole * tile)

    tiles = pl.cdiv(units, tile)

    def hidden_rows(which, start, row_count):
        hidden_tiles(which, start, row_count, 0, tiles)

    def down_rows(phase, start, row_count, of_z):
        at = pl.ds(aligned(start, 128), row_count)

        for s in range(2):
            cols = pl.ds(aligned((of_z * 2 + s) * down_cols, 128), down_cols)
            partials[phase, at, cols] = dot(hidden[at, :], down_buf[of_z * 2 + s]).astype(jnp.bfloat16)

    def owned(of_member, of_core, part):
        return of_member * rows + part * 2 * quarter + of_core * quarter

    def owned_rows(of_member, of_core, part):
        return pl.ds(aligned(owned(of_member, of_core, part), 16), quarter)

    def local_rows(part):
        return pl.ds(part * quarter, quarter)

    def plane_of(of_z):
        return pl.ds(aligned(of_z * plane_cols, 128), plane_cols)

    def send_core(phase, of_member, part, of_z):
        send(
            partials.at[phase, owned_rows(of_member, 1 - core, part), plane_of(of_z)],
            from_core.at[phase, of_member, local_rows(part), plane_of(of_z)],
            core_send, (int(of_member is not member), part, ranks[id(of_z)]),
            core_recv.at[phase, of_member, part, of_z], core_peer,
        )

    def wait_core(phase, of_member, part, of_z):
        arrive(
            from_core.at[phase, of_member, local_rows(part), plane_of(of_z)],
            core_recv.at[phase, of_member, part, of_z],
        )

    def send_pair(phase, part, of_z):
        wait_core(phase, 1 - member, part, of_z)
        at, cols = local_rows(part), plane_of(of_z)
        mine = partials[phase, owned_rows(1 - member, core, part), cols].astype(jnp.float32)
        theirs = from_core[phase, 1 - member, at, cols].astype(jnp.float32)
        summed[phase, at, cols] = (mine + theirs).astype(jnp.bfloat16)
        send(
            summed.at[phase, at, cols], from_pair.at[phase, at, cols],
            pair_send, (part, ranks[id(of_z)]), pair_recv.at[phase, part, of_z], pair_peer,
        )

    def wait_pair(phase, part):
        for of_z in order:
            wait_core(phase, member, part, of_z)
            arrive(
                from_pair.at[phase, local_rows(part), plane_of(of_z)],
                pair_recv.at[phase, part, of_z],
            )

    def settle(phase, gain, weight, source, target, next_gain, part):
        @pl.loop(0, quarter // step_rows)
        def _(i):
            at = pl.ds(aligned(part * quarter + i * step_rows, 16), step_rows)
            mine = pl.ds(aligned(owned(member, core, part) + i * step_rows, 16), step_rows)
            branch = (
                partials[phase, mine, :].astype(jnp.float32)
                + from_core[phase, member, at, :].astype(jnp.float32)
                + from_pair[phase, at, :].astype(jnp.float32)
            )
            before = source[mine if phase == 0 else at, :]
            after = before.astype(jnp.float32) + weight * (rms(branch) * gains[gain : gain + 1, :])
            rounded = after.astype(jnp.bfloat16)
            target[at, :] = rounded
            if next_gain is not None:
                scaled = rms(rounded.astype(jnp.float32)) * gains[next_gain : next_gain + 1, :]
                normed[phase + 1, mine, :] = scaled.astype(jnp.bfloat16)

    def gather_ref(which, of_member, of_core, part):
        return normed.at[which, owned_rows(of_member, of_core, part), :]

    def gather_start(which, part):
        mine = gather_ref(which, member, core, part)
        send(mine, mine, gather_send, (1, part), gather_recv.at[which, 1, part], pair_peer)
        send(mine, mine, gather_send, (0, part), gather_recv.at[which, 0, part], core_peer)

    def gather_own(which, part):
        arrive(
            gather_ref(which, member, 1 - core, part),
            gather_recv.at[which, 0, part],
        )

    def gather_pass(which, part):
        theirs = gather_ref(which, 1 - member, core, part)
        arrive(theirs, gather_recv.at[which, 1, part])
        send(theirs, theirs, gather_send, (2, part), gather_recv.at[which, 2, part], core_peer)

    def gather_pair(which, part):
        arrive(
            gather_ref(which, 1 - member, 1 - core, part),
            gather_recv.at[which, 2, part],
        )

    head = 8

    def mix_in(s, begin, count, js):
        at = pl.ds(aligned(s * rows + begin, 128), count)
        deep = 2 * weight_rows
        total = None if 0 in js else mix_sum[at, :]
        for j in js:
            along = pl.ds(aligned(order[j] * deep, 128), deep)
            term = dot(normed[1, at, along], mix_buf[along, :])
            total = term if total is None else total + term
        mix_sum[at, :] = total
        if planes - 1 in js:
            conv_in[s, head + begin : head + begin + count, :] = (
                total[:, 2 * channels : 3 * channels] * total[:, 0:channels]
            )

    def halo(source, target, to):
        return pltpu.make_async_remote_copy(
            src_ref=conv_in.at[source, rows : rows + head, :],
            dst_ref=conv_in.at[target, 0:head, :],
            send_sem=halo_send.at[source], recv_sem=halo_recv.at[target],
            device_id=to, device_id_type=MESH,
        )

    def near_tail(s):
        return halo(s, y + s * (1 - y), y_peer)

    def far_tail(s):
        return halo(s, 0, device(x, (z + 2) % planes, 0, core))

    def tails(s, act):
        @pl.when((s == 0) | (y == 0))
        def _():
            act(near_tail(s))

        @pl.when((s == 1) & (y == 1) & (pair < pairs - 1))
        def _():
            act(far_tail(s))

    def mix_gate(s, part):
        if part == 0:
            @pl.when(jnp.logical_not(first_segment & (s == 0)))
            def _():
                halo(s, s, y_peer).wait_recv()

        count = 2 * quarter
        total = None
        for tap in range(TAPS):
            begin = head - TAPS + 1 + tap + part * count
            shifted = conv_in[s, begin : begin + count, :]
            scale = taps[tap : tap + 1, pl.ds(aligned(member * channels, 128), channels)]
            total = scale * shifted if total is None else total + scale * shifted
        at = pl.ds(aligned(s * rows + part * count, 128), count)
        bgate = mix_sum[at, channels : 2 * channels]
        gated[at, :] = (bgate * total).astype(jnp.bfloat16)

    def mix_out(s, part, of_z):
        at = pl.ds(aligned(s * rows + part * 2 * quarter, 128), 2 * quarter)

        for n in range(2):
            index = of_z * 2 + n
            cols = pl.ds(aligned(index * out_cols, 128), out_cols)
            weight = out_buf[pl.ds(aligned(index * channels, 128), channels), :]
            partials[1, at, cols] = dot(gated[at, :], weight).astype(jnp.bfloat16)

    def core_parts(phase, of_member, part):
        for of_z in order:
            send_core(phase, of_member, part, of_z)

    for kind in (GATE, UP):
        for i in range(3):
            pass_own(kind, i)
    for j in others:
        spread(GATE, j)
        send_planes(UP, j)
        if j <= 3:
            pass_own(DOWN, j - 1)
    send(stream, own_raw, raw_send, (1,), raw_recv.at[1], pair_peer)
    for j in others:
        send_direct(UP, j)
    for j in others:
        relay(GATE, j)
    for j in others:
        spread(UP, j)
        send_planes(DOWN, j)
    for j in others:
        send_direct(DOWN, j)
    relay(UP, 1)
    raw_copy.wait()

    def raw_at(of_member, of_core):
        return raw.at[
            pl.ds(aligned(of_member * rows, 16), rows), pl.ds(aligned(of_core * width, 128), width)
        ]

    arrive(raw_at(member, 1 - core), raw_recv.at[0])
    pair_raw = raw_at(1 - member, core)
    arrive(pair_raw, raw_recv.at[1])
    send(pair_raw, pair_raw, raw_send, (2,), raw_recv.at[2], core_peer)
    for j in range(2, planes):
        relay(UP, j)
    for j in others:
        spread(DOWN, j)
        send_planes(MIX, j)
    for j in others:
        send_direct(MIX, j)
    for j in others:
        send_planes(OUT, j)
    for j in others:
        send_direct(OUT, j)
    arrive(raw_at(1 - member, 1 - core), raw_recv.at[2])
    norm_all()
    for kind in (GATE, UP):
        for j in range(planes):
            complete(kind, j)
    for j in others:
        hidden_tiles(0, 0, 2 * rows, tiles * (j - 1) // (planes - 1), tiles * j // (planes - 1))
        relay(DOWN, j)
    send_own(MIX)
    for j in range(planes):
        if j > 0:
            spread(MIX, j)
        complete(DOWN, j)

        @pl.loop(0, 2)
        def _(r):
            down_rows(0, r * rows, rows, order[j])

        for of_member in (1 - member, member):
            for part in (1, 0):
                send_core(0, of_member, part, order[j])
        if j > 0:
            for part in (1, 0):
                send_pair(0, part, order[j - 1])
    for part in (1, 0):
        send_pair(0, part, order[planes - 1])
    for i in range(3):
        pass_own(MIX, i)
    for part in (1, 0):
        wait_pair(0, part)
        settle(0, 1, 0.5, raw, current, 2, part)
        gather_start(1, part)
    for j in others:
        relay(MIX, j)
    send_own(OUT)
    for j in others:
        spread(OUT, j)
    last = planes - 1
    half_rows = 2 * quarter
    gather_own(1, 1)
    gather_own(1, 0)
    for j in range(last):
        complete(MIX, j)
        mix_in(member, 0, rows, (j,))
    for i in range(3):
        pass_own(OUT, i)
    gather_pass(1, 1)
    relay(OUT, 1)
    gather_pair(1, 1)
    mix_in(1 - member, half_rows, half_rows, range(last))
    gather_pass(1, 0)
    relay(OUT, 2)
    complete(MIX, last)
    mix_in(1 - member, half_rows, half_rows, (last,))
    tails(1 - member, lambda copy: copy.start())
    mix_in(member, 0, rows, (last,))
    tails(member, lambda copy: copy.start())
    for j in range(3, planes):
        relay(OUT, j)
    gather_pair(1, 0)
    mix_in(1 - member, 0, half_rows, range(planes))
    mix_gate(1 - member, 1)
    for j, of_z in enumerate(order):
        complete(OUT, j)
        mix_out(1 - member, 1, of_z)
        send_core(1, 1 - member, 1, of_z)
    mix_gate(1 - member, 0)
    for of_z in order:
        mix_out(1 - member, 0, of_z)
        send_core(1, 1 - member, 0, of_z)
        send_pair(1, 1, of_z)
    mix_gate(member, 1)
    for of_z in order:
        mix_out(member, 1, of_z)
        send_core(1, member, 1, of_z)
        send_pair(1, 0, of_z)
    mix_gate(member, 0)
    for of_z in order:
        mix_out(member, 0, of_z)
        send_core(1, member, 0, of_z)
    for part in (1, 0):
        wait_pair(1, part)
        settle(1, 3, 1.0, current, current, 4, part)
        gather_start(2, part)
        gather_own(2, part)
        hidden_rows(2, member * rows + part * 2 * quarter, 2 * quarter)
    gather_pass(2, 1)
    down_rows(2, member * rows, rows, order[0])
    gather_pair(2, 1)
    start = (1 - member) * rows
    hidden_rows(2, start + 2 * quarter, 2 * quarter)
    for j in range(planes):
        down_rows(2, start + 2 * quarter, 2 * quarter, order[j])
        send_core(2, 1 - member, 1, order[j])
        if j > 1:
            send_pair(2, 1, order[j - 2])
    gather_pass(2, 0)
    send_pair(2, 1, order[planes - 2])
    send_pair(2, 1, order[planes - 1])
    gather_pair(2, 0)
    hidden_rows(2, start, 2 * quarter)
    for j in range(planes):
        down_rows(2, start, 2 * quarter, order[j])
        send_core(2, 1 - member, 0, order[j])
        if j > 1:
            send_pair(2, 0, order[j - 2])
    down_rows(2, member * rows, rows, order[1])
    for j in range(2):
        send_pair(2, 0, order[planes - 2 + j])
    for j in range(2, planes):
        down_rows(2, member * rows, rows, order[j])
    for part in (1, 0):
        core_parts(2, member, part)
    stores = [None, None]
    for part in (1, 0):
        wait_pair(2, part)
        settle(2, 5, 0.5, current, result, None, part)
        there = pl.ds(aligned(part * 2 * quarter + core * quarter, 16), quarter)
        send(
            result.at[local_rows(part), pl.ds(aligned((1 - core) * width, 128), width)],
            out.at[there, :], out_send, (part,), out_recv.at[part], core_peer,
        )
        store = pltpu.make_async_copy(
            result.at[local_rows(part), pl.ds(aligned(core * width, 128), width)],
            out.at[there, :], store_sem.at[part],
        )
        store.start()
        stores[part] = store
    for part in range(2):
        stores[part].wait()
        theirs = pl.ds(aligned(part * 2 * quarter + (1 - core) * quarter, 16), quarter)
        arrive(out.at[theirs, :], out_recv.at[part])
    for copy in pending.values():
        copy.wait_send()
    for s in range(2):
        tails(s, lambda copy: copy.wait_send())


def fits_kernel(mesh, stream, w_gate, w_down, w_inner, w_out):
    planes = mesh.shape["fs"] // 2
    return (
        mesh.shape["tp"] == 2
        and mesh.shape["rep"] == 2
        and mesh.shape["fs"] % 4 == 0
        and planes >= 4
        and w_gate.shape[0] == w_inner.shape[0] == w_out.shape[0] // 2
        and stream.shape[0] % 256 == 0
        and w_gate.shape[0] % 256 == 0
        and w_gate.shape[1] % 256 == 0
        and w_inner.shape[1] % 256 == 0
        and w_down.shape[1] % 128 == 0
    )


def fused(stream, norm_gains, w_gate, w_up, w_down, w_inner, w_bgate, w_cgate, conv_taps, w_out):
    count = lax.axis_size("fs")
    planes = count // 2
    rows, width = stream.shape
    model_width = 2 * width
    weight_rows, units = w_gate.shape[0], w_gate.shape[1] // 2
    channels, down_cols, out_cols = w_inner.shape[1] // 2, w_down.shape[1], w_out.shape[1]
    own_rows = rows // 2
    mix_width = 3 * channels
    bf16, f32 = jnp.bfloat16, jnp.float32
    vmem, dma = pltpu.VMEM, pltpu.SemaphoreType.DMA
    anywhere = pl.BlockSpec(memory_space=pl.ANY)
    flops = 2 * 2 * rows * (6 * model_width * units + 4 * model_width * channels)
    return pl.pallas_call(
        functools.partial(layer_kernel, planes),
        out_shape=pltpu.VMEM((rows, width), bf16),
        in_specs=[anywhere] * 10,
        out_specs=pl.BlockSpec(memory_space=pltpu.VMEM),
        scratch_shapes=[
            vmem(norm_gains.shape, f32),
            vmem(conv_taps.shape, f32),
            vmem((weight_rows, 2 * mix_width), bf16),
            vmem((model_width, units), bf16),
            vmem((model_width, units), bf16),
            vmem((count, units, down_cols), bf16),
            vmem((model_width, mix_width), bf16),
            vmem((count * channels, out_cols), bf16),
            vmem((2 * rows, model_width), bf16),
            vmem((3, 2 * rows, model_width), bf16),
            vmem((2 * rows, units), bf16),
            vmem((3, 2 * rows, model_width), bf16),
            vmem((3, 2, own_rows, model_width), bf16),
            vmem((3, own_rows, model_width), bf16),
            vmem((3, own_rows, model_width), bf16),
            vmem((own_rows, model_width), bf16),
            vmem((2, 8 + rows, channels), f32),
            vmem((2 * rows, 3 * channels), f32),
            vmem((2 * rows, channels), bf16),
            vmem((own_rows, model_width), bf16),
            dma((6,)),
            dma((8,)),
            dma((3, 6, planes)),
            dma((5, 6, planes)),
            dma((3,)),
            dma((3,)),
            dma((2, 2, planes)),
            dma((3, 2, 2, planes)),
            dma((2, planes)),
            dma((3, 2, planes)),
            dma((3, 2)),
            dma((3, 3, 2)),
            dma((2,)),
            dma((2,)),
            dma((2,)),
            dma((2,)),
            dma((2,)),
        ],
        cost_estimate=pl.CostEstimate(
            flops=flops, bytes_accessed=4 * w_gate.size * 2, transcendentals=4 * rows * units
        ),
        compiler_params=pltpu.CompilerParams(
            collective_id=0, has_side_effects=True, vmem_limit_bytes=60 * 1024 * 1024
        ),
        name="layer",
    )(stream, norm_gains, w_gate, w_up, w_down, w_inner, w_bgate, w_cgate, conv_taps, w_out)


def solution(mesh):
    def body(stream, norm_gains, w_gate, w_up, w_down, w_inner, w_bgate, w_cgate, conv_taps, w_out):
        arguments = (stream, norm_gains, w_gate, w_up, w_down, w_inner, w_bgate, w_cgate, conv_taps, w_out)
        if fits_kernel(mesh, stream, w_gate, w_down, w_inner, w_out):
            return fused(*arguments)
        return shards(*arguments)

    return jax.shard_map(
        body,
        mesh=mesh,
        in_specs=(
            P(("rep", "fs"), "tp"),
            P(),
            P("fs", "tp"),
            P("fs", "tp"),
            P("tp", "fs"),
            P("fs", "tp"),
            P("fs", "tp"),
            P("fs", "tp"),
            P(None, "tp"),
            P("tp", "fs"),
        ),
        out_specs=P(("rep", "fs"), "tp"),
        check_vma=False,
    )
```

```python
import functools

import jax
import jax.numpy as jnp
from jax import lax
from jax.experimental import pallas as pl
from jax.experimental.pallas import tpu as pltpu
from jax.sharding import PartitionSpec as P

TAPS = 3
EPSILON = 1e-06


def ring_order(count):
    return list(range(0, count, 2)) + list(range(1, count, 2))[::-1]


def swap(x, axis):
    return lax.ppermute(x, axis, [(0, 1), (1, 0)])


def copy_blocks(count, size, starts, source, target):
    for i in range(count):
        begin = pl.multiple_of(starts[i] * size, size)
        target[:, i * size : (i + 1) * size] = source[:, pl.ds(begin, size)]


def permuted(x, starts, size):
    return pl.pallas_call(
        functools.partial(copy_blocks, len(starts), size),
        in_specs=[
            pl.BlockSpec(memory_space=pltpu.SMEM),
            pl.BlockSpec(memory_space=pltpu.VMEM),
        ],
        out_specs=pl.BlockSpec(memory_space=pltpu.VMEM),
        out_shape=jax.ShapeDtypeStruct(x.shape, x.dtype),
        cost_estimate=pl.CostEstimate(flops=0, bytes_accessed=2 * x.size * x.dtype.itemsize, transcendentals=0),
        compiler_params=pltpu.CompilerParams(vmem_limit_bytes=3 * x.size * x.dtype.itemsize),
    )(jnp.stack(starts), x)


class Ring:
    def __init__(self, own, after=None):
        count = lax.axis_size("fs")
        order = ring_order(count)
        onward = [(order[i], order[(i + 1) % count]) for i in range(count)]
        back = [(b, a) for a, b in onward]
        half = count // 2
        first, second = own, own
        if after is not None:
            first, _ = lax.optimization_barrier((own, after[0]))
            second, _ = lax.optimization_barrier((own, after[1]))
        rows = own.shape[0] // 2
        self.shards = {0: own}
        self.arrived = self.early = (own, own)
        for step in range(1, half):
            first = lax.ppermute(first, "fs", onward)
            second = lax.ppermute(second, "fs", back)
            self.shards[step] = first
            self.shards[count - step] = second
            self.arrived = (first, second)
            if step == 1:
                self.early = self.arrived
        self.last = (
            lax.ppermute(first[:rows], "fs", onward),
            lax.ppermute(second[rows:], "fs", back),
        )
        self.shards[half] = jnp.concatenate(self.last, axis=0)
        self.sequence = [0]
        for step in range(1, half):
            self.sequence += [step, count - step]
        self.sequence += [half]

    def lined_up(self, axis):
        return jnp.concatenate([self.shards[d] for d in range(len(self.shards))], axis=axis)


def shards(stream, norm_gains, w_gate, w_up, w_down, w_inner, w_bgate, w_cgate, conv_taps, w_out):
    count, tp = lax.axis_size("fs"), lax.axis_size("tp")
    tp_index, rep_index, fs_index = lax.axis_index("tp"), lax.axis_index("rep"), lax.axis_index("fs")
    rows, width = stream.shape
    model_width = width * tp
    order = ring_order(count)
    places = [order.index(i) for i in range(count)]
    place = jnp.array(places, jnp.int32)[fs_index]
    origin = [
        jnp.array(order, jnp.int32)[lax.rem(place - d + count, count)] for d in range(count)
    ]

    behind = [
        lax.rem(place - places[i] + count, count) for i in range(count)
    ]

    def blocks(x, starts):
        size = x.shape[1] // count
        if size % 128 == 0:
            return permuted(x, starts, size)
        return jnp.concatenate(
            [lax.dynamic_slice_in_dim(x, start * size, size, 1) for start in starts], axis=1
        )

    def rep_part(w, axis):
        size = w.shape[axis] // lax.axis_size("rep")
        return lax.dynamic_slice_in_dim(w, rep_index * size, size, axis)

    def whole_features(x):
        if tp != 2:
            return lax.all_gather(x, "tp", axis=1, tiled=True)
        other = swap(x, "tp")
        mine = tp_index == 0
        return jnp.concatenate([jnp.where(mine, x, other), jnp.where(mine, other, x)], axis=1)

    def own_features(x):
        return lax.dynamic_slice_in_dim(x, tp_index * width, width, 1)

    def feature_sum(partials):
        rounded = blocks(partials.astype(jnp.bfloat16), behind)
        if tp != 2:
            return lax.psum_scatter(rounded, "tp", scatter_dimension=1, tiled=True).astype(jnp.float32)
        theirs = lax.dynamic_slice_in_dim(rounded, (1 - tp_index) * width, width, 1)
        received = swap(theirs, "tp").astype(jnp.float32)
        return own_features(rounded).astype(jnp.float32) + received

    def norm_own(current, row):
        values = current.astype(jnp.float32)
        scaled = values * lax.rsqrt(jnp.mean(values * values, axis=1, keepdims=True) + EPSILON)
        return (scaled * norm_gains[row]).astype(jnp.bfloat16)

    def norm_other(normed):
        return whole_features(swap(own_features(normed), "rep"))

    def settle(current, own_sum, other_sum, row, weight):
        received = swap(other_sum.astype(jnp.bfloat16), "rep").astype(jnp.float32)
        branch = whole_features(own_sum + received)
        scaled = branch * lax.rsqrt(jnp.mean(branch * branch, axis=1, keepdims=True) + EPSILON)
        return (current.astype(jnp.float32) + weight * (scaled * norm_gains[row])).astype(
            jnp.bfloat16
        )

    def dot(a, b):
        return jnp.dot(a, b, preferred_element_type=jnp.float32)

    def activate(gate_vals, upward):
        return (jax.nn.silu(gate_vals) * upward).astype(jnp.bfloat16)

    current = whole_features(stream)
    normed = norm_own(current, 0)
    normed = jnp.concatenate([normed, norm_other(normed)], axis=0)

    gate_ring = Ring(rep_part(w_gate, 1))
    up_ring = Ring(rep_part(w_up, 1))
    down_own = rep_part(w_down, 0)
    down_ring = Ring(down_own, gate_ring.arrived)
    mix_own = jnp.concatenate([rep_part(w, 1) for w in (w_inner, w_bgate, w_cgate)], axis=1)
    out_own = rep_part(w_out, 0)
    mix_width = mix_own.shape[1]
    mix_ring = Ring(
        jnp.concatenate([mix_own, out_own.reshape(mix_own.shape[0], -1)], axis=1), down_ring.early
    )

    def by_shards(ring):
        size = ring.shards[0].shape[0]
        total = None
        for d in ring.sequence:
            term = dot(lax.dynamic_slice_in_dim(normed, origin[d] * size, size, 1), ring.shards[d])
            total = term if total is None else total + term
        return total

    hidden = activate(by_shards(gate_ring), by_shards(up_ring))
    down_blocks = {d: dot(hidden, down_ring.shards[d]).astype(jnp.bfloat16) for d in down_ring.sequence}
    sums = feature_sum(jnp.concatenate([down_blocks[d] for d in range(count)], axis=1))
    first = settle(current, sums[:rows], sums[rows:], 1, 0.5)

    mix_whole = mix_ring.lined_up(0)[:, :mix_width]
    out_whole = jnp.concatenate(
        [mix_ring.shards[d][:, mix_width:].reshape(out_own.shape) for d in range(count)], axis=1
    )
    channels = mix_width // 3
    taps = rep_part(conv_taps, 1)

    def mix_in(normed_mix):
        product = dot(blocks(normed_mix, origin), mix_whole)
        inner, bgate, cgate = (product[:, i * channels : (i + 1) * channels] for i in range(3))
        return cgate * inner, bgate

    def mix_out(conv_input, bgate, earlier):
        padded = jnp.concatenate([earlier, conv_input], axis=0)
        conv = taps[0] * padded[0:rows]
        for tap in range(1, TAPS):
            conv = conv + taps[tap] * padded[tap : tap + rows]
        return feature_sum(dot((bgate * conv).astype(jnp.bfloat16), out_whole))

    normed_mix = norm_own(first, 2)
    other_mix = norm_other(normed_mix)
    own_in, own_bgate = mix_in(normed_mix)
    other_in, other_bgate = mix_in(other_mix)
    tails = jnp.concatenate([own_in[rows - (TAPS - 1) :], other_in[rows - (TAPS - 1) :]], axis=0)
    earlier = lax.ppermute(tails, "fs", [(i, i + 1) for i in range(count - 1)])
    other_sum = mix_out(other_in, other_bgate, earlier[TAPS - 1 :])
    own_sum = mix_out(own_in, own_bgate, earlier[: TAPS - 1])
    second = settle(first, own_sum, other_sum, 3, 1.0)

    gate_whole, up_whole = gate_ring.lined_up(0), up_ring.lined_up(0)
    down_whole = down_ring.lined_up(1)

    def units(normed_rows):
        lined = blocks(normed_rows, origin)
        return activate(dot(lined, gate_whole), dot(lined, up_whole))

    normed = norm_own(second, 4)
    other_normed = norm_other(normed)
    own_units = units(normed)
    other_sum = feature_sum(dot(units(other_normed), down_whole))
    own_sum = feature_sum(dot(own_units, down_whole))
    return own_features(settle(second, own_sum, other_sum, 5, 0.5))


MESH = pl.DeviceIdType.MESH
GATE, UP, DOWN, MIX, OUT = range(5)
Z, X, Y, PART_A, PART_B, Z_OTHER = range(6)
DIRECT = ((8, 0), (4, 0), (8, 0), (8, 0), (8, 0))
BY_Y = (3, 3, 3, 3, 3)
TILE = 512


def aligned(value, to):
    return pl.multiple_of(value, to)


def layer_kernel(
    planes,
    stream, all_gains, w_gate, w_up, w_down, w_inner, w_bgate, w_cgate, all_taps, w_out, out,
    gains, taps, w_mix,
    gate_buf, up_buf, down_buf, mix_buf, out_buf, raw, normed, hidden, partials, from_core, summed,
    from_pair, current, conv_in, mix_sum, gated, result,
    local_sem, pack_sem, piece_send, piece_recv, raw_send, raw_recv, core_send, core_recv,
    pair_send, pair_recv, gather_send, gather_recv, halo_send, halo_recv, out_send, out_recv, store_sem,
):
    x, place, core = lax.axis_index("rep"), lax.axis_index("fs"), lax.axis_index("tp")
    z, y = place // 2, place % 2
    pair, member = z // 2, z % 2
    pairs = planes // 2
    rows, width = stream.shape
    quarter = rows // 4
    model_width = 2 * width
    units, channels, mix_width = gate_buf.shape[1], gated.shape[1], mix_buf.shape[1]
    out_cols = out_buf.shape[1]
    weight_rows = w_gate.shape[0]
    down_cols = w_down.shape[1]
    plane_cols = 2 * down_cols
    buffers = (gate_buf, up_buf, down_buf, mix_buf, out_buf)
    halves = (weight_rows // 2, weight_rows // 2, units // 2, weight_rows // 2, channels // 2)

    def device(to_x, to_z, to_y, to_core):
        return (to_x, to_z * 2 + to_y, to_core)

    order = [2 * ((pair + j // 2) % pairs) + (member + j) % 2 for j in range(planes)]
    ranks = {id(of_z): j for j, of_z in enumerate(order)}
    partner = order[1]
    core_peer = device(x, z, y, 1 - core)
    pair_peer = device(x, partner, y, core)
    x_peer, y_peer = device(1 - x, z, y, core), device(x, z, 1 - y, core)

    pending = {}

    def send(source, target, sems, slot, recv_sem, to):
        key = (id(sems),) + slot
        if key in pending:
            pending[key].wait_send()
        send_sem = sems.at[slot]
        copy = pltpu.make_async_remote_copy(
            src_ref=source, dst_ref=target, send_sem=send_sem, recv_sem=recv_sem,
            device_id=to, device_id_type=MESH,
        )
        copy.start()
        pending[key] = copy

    def arrive(target, recv_sem):
        pltpu.make_async_remote_copy(
            src_ref=target, dst_ref=target, send_sem=raw_send.at[0], recv_sem=recv_sem,
            device_id=core_peer, device_id_type=MESH,
        ).wait_recv()

    def piece(kind, of_z, of_y, of_x, begin=0, end=None):
        half = halves[kind]
        count = (half if end is None else end) - begin
        if kind == DOWN:
            return down_buf.at[of_z * 2 + of_y, pl.ds(aligned(of_x * half + begin, 16), count), :]
        start = ((of_z * 2 + of_y) * 2 + of_x) * half + begin
        return buffers[kind].at[pl.ds(aligned(start, 16), count), :]

    def own_source(kind, side, start, count):
        if kind == DOWN:
            return w_down.at[pl.ds(aligned(side * units + start, 16), count), :]
        if kind == OUT:
            return w_out.at[pl.ds(aligned(side * channels + start, 16), count), :]
        cols = mix_width if kind == MIX else units
        source = (w_gate, w_up, None, w_mix)[kind]
        return source.at[pl.ds(aligned(start, 16), count), pl.ds(aligned(side * cols, 128), cols)]

    def piece_copy(source, target, kind, route, j, of_z, to):
        send(source, target, piece_send, (kind % 3, route, j), piece_recv.at[kind, route, of_z], to)

    def wait_piece(target, kind, route, of_z):
        arrive(target, piece_recv.at[kind, route, of_z])

    def eighths(half, count):
        return min(half, (half * count // 8 + 15) // 16 * 16)

    def direct(kind, j):
        return eighths(halves[kind], DIRECT[kind][0 if j == 1 else 1])

    def split(kind):
        return halves[kind] - eighths(halves[kind], BY_Y[kind])

    def send_planes(kind, j):
        to, half = order[j], halves[kind]
        piece_copy(
            own_source(kind, to % 2, x * half, half), piece(kind, z, y, x),
            kind, Z, j, z, device(x, to, y, core),
        )

    def send_direct(kind, j):
        to, count = order[j], direct(kind, j)
        if count == 0:
            return
        piece_copy(
            own_source(kind, to % 2, (1 - x) * halves[kind], count), piece(kind, z, y, 1 - x, 0, count),
            kind, Z_OTHER, j, z, device(x, to, y, core),
        )

    def own_part(kind, i):
        half = halves[kind]
        return (0, half // 4, half // 2)[i], (half // 4, half // 2, half)[i]

    def send_own(kind):
        for i, route in enumerate((Y, PART_A, Z)):
            begin, end = own_part(kind, i)
            piece_copy(
                own_source(kind, member, x * halves[kind] + begin, end - begin),
                piece(kind, z, y, x, begin, end), kind, route, 0, z, y_peer,
            )

    def pass_own(kind, i):
        part = piece(kind, z, 1 - y, x, *own_part(kind, i))
        wait_piece(part, kind, (Y, PART_A, Z)[i], z)
        piece_copy(part, part, kind, (X, PART_B, Z_OTHER)[i], 0, z, x_peer)

    def spread(kind, j):
        of = order[j]
        whole = piece(kind, of, y, x)
        wait_piece(whole, kind, Z, of)
        piece_copy(whole, whole, kind, Y, j, of, y_peer)
        if direct(kind, j) < halves[kind]:
            rest = piece(kind, of, y, x, direct(kind, j), None)
            piece_copy(rest, rest, kind, X, j, of, x_peer)

    def relay(kind, j):
        of = order[j]
        if direct(kind, j) == halves[kind]:
            wait_piece(piece(kind, of, y, 1 - x), kind, Z_OTHER, of)
        else:
            wait_piece(piece(kind, of, y, 1 - x, direct(kind, j), None), kind, X, of)
        part = piece(kind, of, y, 1 - x, split(kind), None)
        piece_copy(part, part, kind, PART_A, j, of, y_peer)
        wait_piece(piece(kind, of, 1 - y, x), kind, Y, of)
        part = piece(kind, of, 1 - y, x, 0, split(kind))
        piece_copy(part, part, kind, PART_B, j, of, x_peer)

    def local_copy(kind):
        count = units if kind == DOWN else weight_rows
        if kind == DOWN:
            target = down_buf.at[z * 2 + y]
        else:
            target = buffers[kind].at[pl.ds(aligned((z * 2 + y) * weight_rows, 16), count), :]
        return pltpu.make_async_copy(own_source(kind, member, 0, count), target, local_sem.at[kind])

    def complete(kind, j):
        of = order[j]
        if j == 0:
            local_copy(kind).wait()
            for i, route in enumerate((X, PART_B, Z_OTHER)):
                wait_piece(piece(kind, z, 1 - y, 1 - x, *own_part(kind, i)), kind, route, z)
        else:
            if 0 < direct(kind, j) < halves[kind]:
                wait_piece(piece(kind, of, y, 1 - x, 0, direct(kind, j)), kind, Z_OTHER, of)
            wait_piece(piece(kind, of, 1 - y, 1 - x, split(kind), None), kind, PART_A, of)
            wait_piece(piece(kind, of, 1 - y, 1 - x, 0, split(kind)), kind, PART_B, of)

    own_raw = raw.at[pl.ds(aligned(member * rows, 16), rows), pl.ds(aligned(core * width, 128), width)]
    packs = []
    for side in range(2):
        base = side * mix_width
        for n, weight in enumerate((w_inner, w_bgate, w_cgate)):
            packs.append((
                weight.at[:, side * channels : (side + 1) * channels],
                w_mix.at[:, base + n * channels : base + (n + 1) * channels],
            ))
    packs += [(all_gains, gains), (all_taps, taps)]
    packs = [pltpu.make_async_copy(a, b, pack_sem.at[n]) for n, (a, b) in enumerate(packs)]
    for copy in packs:
        copy.start()
    raw_copy = pltpu.make_async_copy(stream, own_raw, local_sem.at[5])
    raw_copy.start()
    for kind in (GATE, UP, DOWN, OUT):
        local_copy(kind).start()

    first_segment = (y == 0) & (pair == 0)

    @pl.when(first_segment)
    def _():
        conv_in[0, 0:8, :] = jnp.zeros((8, channels), jnp.float32)

    barrier = pltpu.get_barrier_semaphore()
    greeted = [core_peer, x_peer, y_peer]
    greeted += [device(x, order[j], y, core) for j in range(1, planes)]
    greeted += [device(x, (z + s) % planes, 1 - y, core) for s in sorted({2, planes - 2})]
    for peer in greeted:
        pl.semaphore_signal(barrier, inc=1, device_id=peer, device_id_type=MESH)
    pl.semaphore_wait(barrier, len(greeted))

    others = range(1, planes)
    send_own(GATE)
    for j in others:
        send_planes(GATE, j)
    send_own(UP)
    send_own(DOWN)
    send(stream, own_raw, raw_send, (0,), raw_recv.at[0], core_peer)
    for j in others:
        send_direct(GATE, j)
    for copy in packs:
        copy.wait()
    local_copy(MIX).start()

    def rms(values):
        return values * lax.rsqrt(jnp.mean(values * values, axis=1, keepdims=True) + EPSILON)

    step_rows = 16

    def norm_all():
        @pl.loop(0, 2 * rows // step_rows)
        def _(i):
            at = pl.ds(aligned(i * step_rows, 16), step_rows)
            values = raw[at, :].astype(jnp.float32)
            normed[0, at, :] = (rms(values) * gains[0:1, :]).astype(jnp.bfloat16)

    def dot(a, b):
        return jnp.dot(a, b, preferred_element_type=jnp.float32)

    tile = TILE

    def hidden_tiles(which, start, row_count, first, last):
        at = pl.ds(aligned(start, 128), row_count)

        def columns(begin, count):
            cols = pl.ds(aligned(begin, 128), count)
            gate = dot(normed[which, at, :], gate_buf[:, cols])
            up = dot(normed[which, at, :], up_buf[:, cols])
            hidden[at, cols] = (gate / (1.0 + jnp.exp(-gate)) * up).astype(jnp.bfloat16)

        whole = min(last, units // tile)

        @pl.loop(first, whole)
        def _(n):
            columns(n * tile, tile)

        if whole < last:
            columns(whole * tile, units - whole * tile)

    tiles = pl.cdiv(units, tile)

    def hidden_rows(which, start, row_count):
        hidden_tiles(which, start, row_count, 0, tiles)

    def down_rows(phase, start, row_count, of_z):
        at = pl.ds(aligned(start, 128), row_count)

        for s in range(2):
            cols = pl.ds(aligned((of_z * 2 + s) * down_cols, 128), down_cols)
            partials[phase, at, cols] = dot(hidden[at, :], down_buf[of_z * 2 + s]).astype(jnp.bfloat16)

    def owned(of_member, of_core, part):
        return of_member * rows + part * 2 * quarter + of_core * quarter

    def owned_rows(of_member, of_core, part):
        return pl.ds(aligned(owned(of_member, of_core, part), 16), quarter)

    def local_rows(part):
        return pl.ds(part * quarter, quarter)

    def plane_of(of_z):
        return pl.ds(aligned(of_z * plane_cols, 128), plane_cols)

    def send_core(phase, of_member, part, of_z):
        send(
            partials.at[phase, owned_rows(of_member, 1 - core, part), plane_of(of_z)],
            from_core.at[phase, of_member, local_rows(part), plane_of(of_z)],
            core_send, (int(of_member is not member), part, ranks[id(of_z)]),
            core_recv.at[phase, of_member, part, of_z], core_peer,
        )

    def wait_core(phase, of_member, part, of_z):
        arrive(
            from_core.at[phase, of_member, local_rows(part), plane_of(of_z)],
            core_recv.at[phase, of_member, part, of_z],
        )

    def send_pair(phase, part, of_z):
        wait_core(phase, 1 - member, part, of_z)
        at, cols = local_rows(part), plane_of(of_z)
        mine = partials[phase, owned_rows(1 - member, core, part), cols].astype(jnp.float32)
        theirs = from_core[phase, 1 - member, at, cols].astype(jnp.float32)
        summed[phase, at, cols] = (mine + theirs).astype(jnp.bfloat16)
        send(
            summed.at[phase, at, cols], from_pair.at[phase, at, cols],
            pair_send, (part, ranks[id(of_z)]), pair_recv.at[phase, part, of_z], pair_peer,
        )

    def wait_pair(phase, part):
        for of_z in order:
            wait_core(phase, member, part, of_z)
            arrive(
                from_pair.at[phase, local_rows(part), plane_of(of_z)],
                pair_recv.at[phase, part, of_z],
            )

    def settle(phase, gain, weight, source, target, next_gain, part):
        @pl.loop(0, quarter // step_rows)
        def _(i):
            at = pl.ds(aligned(part * quarter + i * step_rows, 16), step_rows)
            mine = pl.ds(aligned(owned(member, core, part) + i * step_rows, 16), step_rows)
            branch = (
                partials[phase, mine, :].astype(jnp.float32)
                + from_core[phase, member, at, :].astype(jnp.float32)
                + from_pair[phase, at, :].astype(jnp.float32)
            )
            before = source[mine if phase == 0 else at, :]
            after = before.astype(jnp.float32) + weight * (rms(branch) * gains[gain : gain + 1, :])
            rounded = after.astype(jnp.bfloat16)
            target[at, :] = rounded
            if next_gain is not None:
                scaled = rms(rounded.astype(jnp.float32)) * gains[next_gain : next_gain + 1, :]
                normed[phase + 1, mine, :] = scaled.astype(jnp.bfloat16)

    def gather_ref(which, of_member, of_core, part):
        return normed.at[which, owned_rows(of_member, of_core, part), :]

    def gather_start(which, part):
        mine = gather_ref(which, member, core, part)
        send(mine, mine, gather_send, (1, part), gather_recv.at[which, 1, part], pair_peer)
        send(mine, mine, gather_send, (0, part), gather_recv.at[which, 0, part], core_peer)

    def gather_own(which, part):
        arrive(
            gather_ref(which, member, 1 - core, part),
            gather_recv.at[which, 0, part],
        )

    def gather_pass(which, part):
        theirs = gather_ref(which, 1 - member, core, part)
        arrive(theirs, gather_recv.at[which, 1, part])
        send(theirs, theirs, gather_send, (2, part), gather_recv.at[which, 2, part], core_peer)

    def gather_pair(which, part):
        arrive(
            gather_ref(which, 1 - member, 1 - core, part),
            gather_recv.at[which, 2, part],
        )

    head = 8

    def mix_in(s, begin, count, js):
        at = pl.ds(aligned(s * rows + begin, 128), count)
        deep = 2 * weight_rows
        total = None if 0 in js else mix_sum[at, :]
        for j in js:
            along = pl.ds(aligned(order[j] * deep, 128), deep)
            term = dot(normed[1, at, along], mix_buf[along, :])
            total = term if total is None else total + term
        mix_sum[at, :] = total
        if planes - 1 in js:
            conv_in[s, head + begin : head + begin + count, :] = (
                total[:, 2 * channels : 3 * channels] * total[:, 0:channels]
            )

    def halo(source, target, to):
        return pltpu.make_async_remote_copy(
            src_ref=conv_in.at[source, rows : rows + head, :],
            dst_ref=conv_in.at[target, 0:head, :],
            send_sem=halo_send.at[source], recv_sem=halo_recv.at[target],
            device_id=to, device_id_type=MESH,
        )

    def near_tail(s):
        return halo(s, y + s * (1 - y), y_peer)

    def far_tail(s):
        return halo(s, 0, device(x, (z + 2) % planes, 0, core))

    def tails(s, act):
        @pl.when((s == 0) | (y == 0))
        def _():
            act(near_tail(s))

        @pl.when((s == 1) & (y == 1) & (pair < pairs - 1))
        def _():
            act(far_tail(s))

    def mix_gate(s, part):
        if part == 0:
            @pl.when(jnp.logical_not(first_segment & (s == 0)))
            def _():
                halo(s, s, y_peer).wait_recv()

        count = 2 * quarter
        total = None
        for tap in range(TAPS):
            begin = head - TAPS + 1 + tap + part * count
            shifted = conv_in[s, begin : begin + count, :]
            scale = taps[tap : tap + 1, pl.ds(aligned(member * channels, 128), channels)]
            total = scale * shifted if total is None else total + scale * shifted
        at = pl.ds(aligned(s * rows + part * count, 128), count)
        bgate = mix_sum[at, channels : 2 * channels]
        gated[at, :] = (bgate * total).astype(jnp.bfloat16)

    def mix_out(s, part, of_z):
        at = pl.ds(aligned(s * rows + part * 2 * quarter, 128), 2 * quarter)

        for n in range(2):
            index = of_z * 2 + n
            cols = pl.ds(aligned(index * out_cols, 128), out_cols)
            weight = out_buf[pl.ds(aligned(index * channels, 128), channels), :]
            partials[1, at, cols] = dot(gated[at, :], weight).astype(jnp.bfloat16)

    def core_parts(phase, of_member, part):
        for of_z in order:
            send_core(phase, of_member, part, of_z)

    for kind in (GATE, UP):
        for i in range(3):
            pass_own(kind, i)
    for j in others:
        spread(GATE, j)
        send_planes(UP, j)
        if j <= 3:
            pass_own(DOWN, j - 1)
    send(stream, own_raw, raw_send, (1,), raw_recv.at[1], pair_peer)
    for j in others:
        send_direct(UP, j)
    for j in others:
        relay(GATE, j)
    for j in others:
        spread(UP, j)
        send_planes(DOWN, j)
    for j in others:
        send_direct(DOWN, j)
    relay(UP, 1)
    raw_copy.wait()

    def raw_at(of_member, of_core):
        return raw.at[
            pl.ds(aligned(of_member * rows, 16), rows), pl.ds(aligned(of_core * width, 128), width)
        ]

    arrive(raw_at(member, 1 - core), raw_recv.at[0])
    pair_raw = raw_at(1 - member, core)
    arrive(pair_raw, raw_recv.at[1])
    send(pair_raw, pair_raw, raw_send, (2,), raw_recv.at[2], core_peer)
    for j in range(2, planes):
        relay(UP, j)
    for j in others:
        spread(DOWN, j)
        send_planes(MIX, j)
    for j in others:
        send_direct(MIX, j)
    for j in others:
        send_planes(OUT, j)
    for j in others:
        send_direct(OUT, j)
    arrive(raw_at(1 - member, 1 - core), raw_recv.at[2])
    norm_all()
    for kind in (GATE, UP):
        for j in range(planes):
            complete(kind, j)
    for j in others:
        hidden_tiles(0, 0, 2 * rows, tiles * (j - 1) // (planes - 1), tiles * j // (planes - 1))
        relay(DOWN, j)
    send_own(MIX)
    for j in range(planes):
        if j > 0:
            spread(MIX, j)
        complete(DOWN, j)

        @pl.loop(0, 2)
        def _(r):
            down_rows(0, r * rows, rows, order[j])

        for of_member in (1 - member, member):
            for part in (1, 0):
                send_core(0, of_member, part, order[j])
        if j > 0:
            for part in (1, 0):
                send_pair(0, part, order[j - 1])
    for part in (1, 0):
        send_pair(0, part, order[planes - 1])
    for i in range(3):
        pass_own(MIX, i)
    for part in (1, 0):
        wait_pair(0, part)
        settle(0, 1, 0.5, raw, current, 2, part)
        gather_start(1, part)
    for j in others:
        relay(MIX, j)
    send_own(OUT)
    for j in others:
        spread(OUT, j)
    last = planes - 1
    half_rows = 2 * quarter
    gather_own(1, 1)
    gather_own(1, 0)
    for j in range(last):
        complete(MIX, j)
        mix_in(member, 0, rows, (j,))
    for i in range(3):
        pass_own(OUT, i)
    gather_pass(1, 1)
    relay(OUT, 1)
    gather_pair(1, 1)
    mix_in(1 - member, half_rows, half_rows, range(last))
    gather_pass(1, 0)
    relay(OUT, 2)
    complete(MIX, last)
    mix_in(1 - member, half_rows, half_rows, (last,))
    tails(1 - member, lambda copy: copy.start())
    mix_in(member, 0, rows, (last,))
    tails(member, lambda copy: copy.start())
    for j in range(3, planes):
        relay(OUT, j)
    gather_pair(1, 0)
    mix_in(1 - member, 0, half_rows, range(planes))
    mix_gate(1 - member, 1)
    for j, of_z in enumerate(order):
        complete(OUT, j)
        mix_out(1 - member, 1, of_z)
        send_core(1, 1 - member, 1, of_z)
        if j > 1:
            send_pair(1, 1, order[j - 2])
    mix_gate(1 - member, 0)
    for j, of_z in enumerate(order):
        mix_out(1 - member, 0, of_z)
        send_core(1, 1 - member, 0, of_z)
        if j in (1, 3):
            send_pair(1, 1, order[planes - 2 + j // 2])
    mix_gate(member, 1)
    for of_z in order:
        mix_out(member, 1, of_z)
        send_core(1, member, 1, of_z)
        send_pair(1, 0, of_z)
    mix_gate(member, 0)
    for of_z in order:
        mix_out(member, 0, of_z)
        send_core(1, member, 0, of_z)
    for part in (1, 0):
        wait_pair(1, part)
        settle(1, 3, 1.0, current, current, 4, part)
        gather_start(2, part)
        gather_own(2, part)
        hidden_rows(2, member * rows + part * 2 * quarter, 2 * quarter)
    gather_pass(2, 1)
    down_rows(2, member * rows, rows, order[0])
    gather_pair(2, 1)
    start = (1 - member) * rows
    hidden_rows(2, start + 2 * quarter, 2 * quarter)
    for j in range(planes):
        down_rows(2, start + 2 * quarter, 2 * quarter, order[j])
        send_core(2, 1 - member, 1, order[j])
        if j > 1:
            send_pair(2, 1, order[j - 2])
    gather_pass(2, 0)
    send_pair(2, 1, order[planes - 2])
    send_pair(2, 1, order[planes - 1])
    gather_pair(2, 0)
    hidden_rows(2, start, 2 * quarter)
    for j in range(planes):
        down_rows(2, start, 2 * quarter, order[j])
        send_core(2, 1 - member, 0, order[j])
        if j > 1:
            send_pair(2, 0, order[j - 2])
    down_rows(2, member * rows, rows, order[1])
    for j in range(2):
        send_pair(2, 0, order[planes - 2 + j])
    for j in range(2, planes):
        down_rows(2, member * rows, rows, order[j])
    for part in (1, 0):
        core_parts(2, member, part)
    stores = [None, None]
    for part in (1, 0):
        wait_pair(2, part)
        settle(2, 5, 0.5, current, result, None, part)
        there = pl.ds(aligned(part * 2 * quarter + core * quarter, 16), quarter)
        send(
            result.at[local_rows(part), pl.ds(aligned((1 - core) * width, 128), width)],
            out.at[there, :], out_send, (part,), out_recv.at[part], core_peer,
        )
        store = pltpu.make_async_copy(
            result.at[local_rows(part), pl.ds(aligned(core * width, 128), width)],
            out.at[there, :], store_sem.at[part],
        )
        store.start()
        stores[part] = store
    for part in range(2):
        stores[part].wait()
        theirs = pl.ds(aligned(part * 2 * quarter + (1 - core) * quarter, 16), quarter)
        arrive(out.at[theirs, :], out_recv.at[part])
    for copy in pending.values():
        copy.wait_send()
    for s in range(2):
        tails(s, lambda copy: copy.wait_send())


def fits_kernel(mesh, stream, w_gate, w_down, w_inner, w_out):
    planes = mesh.shape["fs"] // 2
    return (
        mesh.shape["tp"] == 2
        and mesh.shape["rep"] == 2
        and mesh.shape["fs"] % 4 == 0
        and planes >= 4
        and w_gate.shape[0] == w_inner.shape[0] == w_out.shape[0] // 2
        and stream.shape[0] % 256 == 0
        and w_gate.shape[0] % 256 == 0
        and w_gate.shape[1] % 256 == 0
        and w_inner.shape[1] % 256 == 0
        and w_down.shape[1] % 128 == 0
    )


def fused(stream, norm_gains, w_gate, w_up, w_down, w_inner, w_bgate, w_cgate, conv_taps, w_out):
    count = lax.axis_size("fs")
    planes = count // 2
    rows, width = stream.shape
    model_width = 2 * width
    weight_rows, units = w_gate.shape[0], w_gate.shape[1] // 2
    channels, down_cols, out_cols = w_inner.shape[1] // 2, w_down.shape[1], w_out.shape[1]
    own_rows = rows // 2
    mix_width = 3 * channels
    bf16, f32 = jnp.bfloat16, jnp.float32
    vmem, dma = pltpu.VMEM, pltpu.SemaphoreType.DMA
    anywhere = pl.BlockSpec(memory_space=pl.ANY)
    flops = 2 * 2 * rows * (6 * model_width * units + 4 * model_width * channels)
    return pl.pallas_call(
        functools.partial(layer_kernel, planes),
        out_shape=pltpu.VMEM((rows, width), bf16),
        in_specs=[anywhere] * 10,
        out_specs=pl.BlockSpec(memory_space=pltpu.VMEM),
        scratch_shapes=[
            vmem(norm_gains.shape, f32),
            vmem(conv_taps.shape, f32),
            vmem((weight_rows, 2 * mix_width), bf16),
            vmem((model_width, units), bf16),
            vmem((model_width, units), bf16),
            vmem((count, units, down_cols), bf16),
            vmem((model_width, mix_width), bf16),
            vmem((count * channels, out_cols), bf16),
            vmem((2 * rows, model_width), bf16),
            vmem((3, 2 * rows, model_width), bf16),
            vmem((2 * rows, units), bf16),
            vmem((3, 2 * rows, model_width), bf16),
            vmem((3, 2, own_rows, model_width), bf16),
            vmem((3, own_rows, model_width), bf16),
            vmem((3, own_rows, model_width), bf16),
            vmem((own_rows, model_width), bf16),
            vmem((2, 8 + rows, channels), f32),
            vmem((2 * rows, 3 * channels), f32),
            vmem((2 * rows, channels), bf16),
            vmem((own_rows, model_width), bf16),
            dma((6,)),
            dma((8,)),
            dma((3, 6, planes)),
            dma((5, 6, planes)),
            dma((3,)),
            dma((3,)),
            dma((2, 2, planes)),
            dma((3, 2, 2, planes)),
            dma((2, planes)),
            dma((3, 2, planes)),
            dma((3, 2)),
            dma((3, 3, 2)),
            dma((2,)),
            dma((2,)),
            dma((2,)),
            dma((2,)),
            dma((2,)),
        ],
        cost_estimate=pl.CostEstimate(
            flops=flops, bytes_accessed=4 * w_gate.size * 2, transcendentals=4 * rows * units
        ),
        compiler_params=pltpu.CompilerParams(
            collective_id=0, has_side_effects=True, vmem_limit_bytes=60 * 1024 * 1024
        ),
        name="layer",
    )(stream, norm_gains, w_gate, w_up, w_down, w_inner, w_bgate, w_cgate, conv_taps, w_out)


def solution(mesh):
    def body(stream, norm_gains, w_gate, w_up, w_down, w_inner, w_bgate, w_cgate, conv_taps, w_out):
        arguments = (stream, norm_gains, w_gate, w_up, w_down, w_inner, w_bgate, w_cgate, conv_taps, w_out)
        if fits_kernel(mesh, stream, w_gate, w_down, w_inner, w_out):
            return fused(*arguments)
        return shards(*arguments)

    return jax.shard_map(
        body,
        mesh=mesh,
        in_specs=(
            P(("rep", "fs"), "tp"),
            P(),
            P("fs", "tp"),
            P("fs", "tp"),
            P("tp", "fs"),
            P("fs", "tp"),
            P("fs", "tp"),
            P("fs", "tp"),
            P(None, "tp"),
            P("tp", "fs"),
        ),
        out_specs=P(("rep", "fs"), "tp"),
        check_vma=False,
    )
```
